32 devices in a mesh: sp: 4 (over y, x), dp: 8 (over z, core).
Axes of the slice: x: 2, y: 2, z: 4, core: 2. Of those that a mesh axis runs over, the one named last changes fastest.
Arguments:
- tokens: bfloat16 [8, 640, 2048], P('dp', 'sp'), may hold values from -42 to 42
- query_weight: bfloat16 [2048, 1024], P('dp'), may hold values from -1 to 1
- key_weight: bfloat16 [2048, 1024], P('dp'), may hold values from -1 to 1
- values: bfloat16 [8, 640, 1024], P('dp', 'sp'), may hold values from -6 to 6
- lambdas: float32 [16], replicated, may hold values from 0.3 to 0.8
- out_grad: bfloat16 [8, 640, 1024], P('dp', 'sp'), may hold values from -6 to 6
Outputs:
- tokens_grad: bfloat16 [8, 640, 2048], P('dp', 'sp')
- values_grad: bfloat16 [8, 640, 1024], P('dp', 'sp')
- query_weight_grad: float32 [2048, 1024], P('dp')
- key_weight_grad: float32 [2048, 1024], P('dp')
The draws below stay inside these ranges and needn't reach their ends.
All inputs are finite; a program needn't handle non-finite values.
Results may differ from the reference program's by a relative error of at most 0.029.
The reference program's roundings to bfloat16 on the way count: a program that leaves them out, or rounds other values in their place, can miss the bound.
Values may be sent and summed in bfloat16 or wider, within the bound.
A program may use at most 128 MiB of HBM per device.

```python
import math
import jax
import jax.numpy as jnp
from jax import lax

D = 2048
HEADS = 16
DQK = 32
SEQLEN = 640
BATCH = 8
QCOLS = 1024
VCOLS = 1024


def weight_normals(key):
    first_draw = jax.random.normal(jax.random.fold_in(key, 11), (D, QCOLS), jnp.float32)
    second_draw = jax.random.normal(jax.random.fold_in(key, 12), (D, QCOLS), jnp.float32)
    return (first_draw, second_draw)


def draw_query_weight(key, part):
    first_draw, second_draw = weight_normals(key)
    return (jnp.clip(first_draw, -6.0, 6.0) * math.sqrt(3.0 / D)).astype(jnp.bfloat16)


def draw_key_weight(key, part):
    first_draw, second_draw = weight_normals(key)
    blended = second_draw
    return (jnp.clip(blended, -6.0, 6.0) * math.sqrt(1.0 / D)).astype(jnp.bfloat16)


def draw_tokens(key, part):
    base_draw = jnp.clip(jax.random.normal(jax.random.fold_in(key, 21), (BATCH, SEQLEN, D), jnp.float32), -6.0, 6.0)
    return base_draw.astype(jnp.bfloat16)


def levels(rng, dims, split, smallest, largest):
    factor_of, own = 1.0, jax.random.fold_in(rng, 6)
    for dim, shards_of in split:
        draws = jnp.exp(jax.random.uniform(jax.random.fold_in(own, dim), (shards_of,), jnp.float32, smallest / len(split), largest / len(split)))
        factor_of = factor_of * jnp.repeat(draws, dims[dim] // shards_of).reshape([-1 if axis == dim else 1 for axis in range(len(dims))])
    return factor_of


def gaussian(own_key, shape, scale, reach, pieces=(), kind=jnp.bfloat16):
    level = levels(own_key, shape, pieces, -0.22, 0.18) if pieces else 1.0
    entries = jax.random.normal(own_key, shape, jnp.float32) * scale * level
    return jnp.minimum(jnp.maximum(entries, -reach), reach).astype(kind)


def setup_inputs(seed: int = 0) -> dict:
    arg_keys = jax.random.split(jax.random.key(seed), 7)
    tokens = draw_tokens(jax.random.fold_in(arg_keys[6], 71), 0)
    query_weight = draw_query_weight(jax.random.fold_in(arg_keys[6], 71), 0)
    key_weight = draw_key_weight(jax.random.fold_in(arg_keys[6], 71), 0)
    values = gaussian(arg_keys[3], (BATCH, SEQLEN, VCOLS), 1.0, 6.0, ((0, 8), (1, 4)))
    lambdas = jnp.clip(jax.random.uniform(arg_keys[4], (HEADS,), jnp.float32, 0.3, 0.8), 0.3, 0.8)
    out_grad = gaussian(arg_keys[5], (BATCH, SEQLEN, VCOLS), 1.0, 6.0, ((0, 8), (1, 4)))
    return dict(tokens=tokens, query_weight=query_weight, key_weight=key_weight, values=values, lambdas=lambdas, out_grad=out_grad)


NORM_EPS = 0.1
THETA = 10000.0

def rotation_tables(positions, vec_width):
    half_width = vec_width // 2
    freqs = jnp.exp(-math.log(THETA) * jnp.arange(half_width, dtype=jnp.float32) / half_width)
    angles = positions.astype(jnp.float32)[:, None] * freqs[None, :]
    return (jnp.cos(angles), jnp.sin(angles))

def rotate(field, cosine, sine_table, vec_width, sign_value):
    full_shape = field.shape
    grouped = field.reshape(full_shape[:-1] + (full_shape[-1] // vec_width, 2, vec_width // 2))
    first_half = grouped[..., 0, :]
    second_half = grouped[..., 1, :]
    cos_cols = cosine[:, None, :]
    sin_cols = sign_value * sine_table[:, None, :]
    turned = jnp.stack([first_half * cos_cols - second_half * sin_cols, second_half * cos_cols + first_half * sin_cols], axis=-2)
    return turned.reshape(full_shape)

def pair_product(pattern, first_op, second_op):
    return jnp.einsum(pattern, first_op.astype(jnp.float32), second_op.astype(jnp.float32))

def head_backward(query_rot, key_rot, value_rows, grad_rows, lambda_here, cosine, sine_table):
    seq_length = query_rot.shape[0]
    head_count = lambda_here.shape[0]
    qk_width = query_rot.shape[1] // (2 * head_count)
    value_width = value_rows.shape[1] // head_count
    block_rows = math.gcd(seq_length, 512)
    block_count = seq_length // block_rows
    inv_root = 1.0 / math.sqrt(qk_width)
    query_split = query_rot.reshape(block_count, block_rows, head_count, 2, qk_width)
    key_split = key_rot.reshape(seq_length, head_count, 2, qk_width)
    value_split = value_rows.reshape(seq_length, head_count, value_width)
    grad_split = grad_rows.reshape(block_count, block_rows, head_count, value_width)
    lambda_col = lambda_here[:, None, None]
    key_positions = jnp.arange(seq_length, dtype=jnp.int32)

    def block_step(carried, inputs):
        key_sum, value_sum = carried
        query_part, grad_part, block_start = inputs
        scores = pair_product('qhmd,khmd->hmqk', query_part, key_split) * inv_root
        query_positions = block_start + jnp.arange(block_rows, dtype=jnp.int32)
        causal_mask = key_positions[None, :] <= query_positions[:, None]
        scores = jnp.where(causal_mask, scores, -jnp.inf)
        row_max = lax.optimization_barrier(jnp.max(scores, axis=-1, keepdims=True))
        exp_scores = jnp.exp(scores - row_max)
        prob_maps = exp_scores / lax.optimization_barrier(jnp.sum(exp_scores, axis=-1, keepdims=True))
        weights = (prob_maps[:, 0] - lambda_col * prob_maps[:, 1]).astype(jnp.bfloat16)
        mixed_out = pair_product('hqk,khe->qhe', weights, value_split)
        norm_scale = lax.rsqrt(lax.optimization_barrier(jnp.mean(mixed_out * mixed_out, axis=-1, keepdims=True)) + NORM_EPS)
        grad_float = grad_part.astype(jnp.float32)
        mixed_grad = (norm_scale * grad_float - norm_scale * norm_scale * norm_scale * mixed_out * lax.optimization_barrier(jnp.mean(grad_float * mixed_out, axis=-1, keepdims=True))).astype(jnp.bfloat16)
        weight_grad = pair_product('qhe,khe->hqk', mixed_grad, value_split)
        value_sum = value_sum + pair_product('hqk,qhe->khe', weights, mixed_grad)
        first_grad = prob_maps[:, 0] * (weight_grad - lax.optimization_barrier(jnp.sum(weight_grad * prob_maps[:, 0], axis=-1, keepdims=True)))
        second_grad = -lambda_col * prob_maps[:, 1] * (weight_grad - lax.optimization_barrier(jnp.sum(weight_grad * prob_maps[:, 1], axis=-1, keepdims=True)))
        score_grad = (jnp.stack([first_grad, second_grad], axis=1) * inv_root).astype(jnp.bfloat16)
        query_grad = pair_product('hmqk,khmd->qhmd', score_grad, key_split)
        key_sum = key_sum + pair_product('hmqk,qhmd->khmd', score_grad, query_part)
        return ((key_sum, value_sum), query_grad)
    zero_init = (jnp.zeros((seq_length, head_count, 2, qk_width), jnp.float32), jnp.zeros((seq_length, head_count, value_width), jnp.float32))
    block_starts = jnp.arange(block_count, dtype=jnp.int32) * block_rows
    (key_sum, value_sum), query_blocks = lax.scan(block_step, zero_init, (query_split, grad_split, block_starts))
    query_turned = query_blocks.reshape(seq_length, head_count * 2 * qk_width)
    key_turned = key_sum.reshape(seq_length, head_count * 2 * qk_width)
    query_back = rotate(query_turned, cosine, sine_table, qk_width, -1.0).astype(jnp.bfloat16)
    key_back = rotate(key_turned, cosine, sine_table, qk_width, -1.0).astype(jnp.bfloat16)
    values_back = value_sum.reshape(seq_length, head_count * value_width).astype(jnp.bfloat16)
    return (query_back, key_back, values_back)

def reference(tokens, query_weight, key_weight, values, lambdas, out_grad):
    cosine, sine_table = rotation_tables(jnp.arange(SEQLEN, dtype=jnp.int32), DQK)
    query_float = query_weight.astype(jnp.float32)
    key_float = key_weight.astype(jnp.float32)

    def one_sequence(inputs):
        token_seq, value_seq, grad_seq = inputs
        token_float = token_seq.astype(jnp.float32)
        query_rot = rotate(jnp.dot(token_float, query_float), cosine, sine_table, DQK, 1.0).astype(jnp.bfloat16)
        key_rot = rotate(jnp.dot(token_float, key_float), cosine, sine_table, DQK, 1.0).astype(jnp.bfloat16)
        query_back, key_back, values_back = head_backward(query_rot, key_rot, value_seq, grad_seq, lambdas, cosine, sine_table)
        query_back_f = query_back.astype(jnp.float32)
        key_back_f = key_back.astype(jnp.float32)
        input_grad = (jnp.dot(query_back_f, query_float.T) + jnp.dot(key_back_f, key_float.T)).astype(jnp.bfloat16)
        query_part = jnp.dot(token_float.T, query_back_f)
        key_part = jnp.dot(token_float.T, key_back_f)
        return (input_grad, values_back, query_part, key_part)
    tokens_grad, values_grad, query_parts, key_parts = lax.map(one_sequence, (tokens, values, out_grad))
    factor = 1.0 / math.sqrt(BATCH * SEQLEN)
    return (tokens_grad, values_grad, lax.optimization_barrier(jnp.sum(query_parts, axis=0)) * factor, lax.optimization_barrier(jnp.sum(key_parts, axis=0)) * factor)
```

```python
import functools
import math

import jax
import jax.numpy as jnp
from jax import lax
from jax.experimental import pallas as pl
from jax.experimental.pallas import tpu as pltpu
from jax.sharding import PartitionSpec as P

DQK = 32
NORM_EPS = 0.1
THETA = 10000.0
F32 = jnp.float32
BF16 = jnp.bfloat16


def dot(a, b, ca=1, cb=0):
    return lax.dot_general(a, b, (((ca,), (cb,)), ((), ())), preferred_element_type=F32)


def rotation_tables(seq_length):
    half = DQK // 2
    freqs = jnp.exp(-math.log(THETA) * jnp.arange(half, dtype=F32) / half)
    angles = freqs[:, None] * jnp.arange(seq_length, dtype=jnp.int32).astype(F32)[None, :]
    return jnp.cos(angles), jnp.sin(angles)


def rotate_rows(x, cos, sin):
    half = DQK // 2
    parts = []
    for g in range(x.shape[0] // DQK):
        a = x[g * DQK : g * DQK + half]
        b = x[g * DQK + half : (g + 1) * DQK]
        parts += [a * cos - b * sin, b * cos + a * sin]
    return jnp.concatenate(parts, axis=0)


def attention_kernel(heads, lam_ref, cos_ref, sin_ref, qk_in, vog_ref, back_ref, rows_ref, dv_ref,
                     qk_ref, vt_s, ogt_s, dvt_s, dk_s):
    seq = cos_ref.shape[1]
    qc = qk_ref.shape[0] // 2
    hw = qc // heads
    ve = vog_ref.shape[2] // heads
    qk_ref[...] = qk_in[...].T
    inv_root = 1.0 / math.sqrt(DQK)
    vt_s[...] = vog_ref[0].T
    ogt_s[...] = vog_ref[1].T
    step = 256

    def one_head(h, _):
        lam = lam_ref[lax.axis_index("sp") * heads + h]
        cos, sin = cos_ref[...], sin_ref[...]
        qrow = pl.multiple_of(h * hw, hw)
        vrow = pl.multiple_of(h * ve, ve)
        qt = rotate_rows(qk_ref[pl.ds(qrow, hw), :], cos, sin).astype(BF16)
        kt = rotate_rows(qk_ref[pl.ds(qc + qrow, hw), :], cos, sin).astype(BF16)
        k = kt.T
        vt = vt_s[pl.ds(vrow, ve), :]
        v = vt.T
        zero_half = jnp.zeros((DQK, step), BF16)
        dk_s[...] = jnp.zeros_like(dk_s)
        dvt_s[pl.ds(vrow, ve), :] = jnp.zeros((ve, seq), F32)
        for t0 in range(0, seq, step):
            end = min(t0 + step, seq)
            tb = end - t0
            zh = zero_half[:, :tb]
            q_b = qt[:, t0:end]
            mask = lax.broadcasted_iota(jnp.int32, (tb, tb), 0) <= lax.broadcasted_iota(
                jnp.int32, (tb, tb), 1
            )
            probs = []
            for m in range(2):
                half_q = q_b[m * DQK : (m + 1) * DQK]
                rhs = jnp.concatenate([half_q, zh] if m == 0 else [zh, half_q], axis=0)
                s = dot(k[:end], rhs) * inv_root
                diag = jnp.where(mask, s[t0:], -jnp.inf)
                s = jnp.concatenate([s[:t0], diag], axis=0) if t0 else diag
                e = jnp.exp(s - jnp.max(s, axis=0, keepdims=True))
                probs.append(e * (1.0 / jnp.sum(e, axis=0, keepdims=True)))
            p1, p2 = probs
            mix = (p1 - lam * p2).astype(BF16)
            ho = dot(vt[:, :end], mix)
            inv = lax.rsqrt(jnp.mean(ho * ho, axis=0, keepdims=True) + NORM_EPS)
            og = ogt_s[pl.ds(vrow, ve), t0:end].astype(F32)
            ob = (inv * og - inv * inv * inv * ho * jnp.mean(og * ho, axis=0, keepdims=True)).astype(BF16)
            mg = dot(v[:end], ob) * inv_root
            g1 = (p1 * (mg - jnp.sum(mg * p1, axis=0, keepdims=True))).astype(BF16)
            g2 = ((-lam * p2) * (mg - jnp.sum(mg * p2, axis=0, keepdims=True))).astype(BF16)
            dvt_s[pl.ds(vrow, ve), :end] += dot(ob, mix, 1, 1)
            dq = jnp.concatenate([dot(kt[:DQK, :end], g1), dot(kt[DQK:, :end], g2)], axis=0)
            back_ref[pl.ds(qrow, hw), t0:end] = rotate_rows(dq, cos[:, t0:end], -sin[:, t0:end]).astype(BF16)
            dk_s[:DQK, :end] += dot(q_b[:DQK], g1, 1, 1)
            dk_s[DQK:, :end] += dot(q_b[DQK:], g2, 1, 1)
        back_ref[pl.ds(qc + qrow, hw), :] = rotate_rows(dk_s[...], cos, -sin).astype(BF16)
        return 0

    lax.fori_loop(0, heads, one_head, 0)
    dv_ref[...] = dvt_s[...].T.astype(BF16)
    rows_ref[...] = back_ref[...].T


def attention(qk, vog, lam, cos, sin, heads):
    seq, qk_cols = qk.shape
    vc = vog.shape[2]
    vm = pl.BlockSpec(memory_space=pltpu.VMEM)
    return pl.pallas_call(
        functools.partial(attention_kernel, heads),
        out_shape=(
            jax.ShapeDtypeStruct((qk_cols, seq), BF16),
            jax.ShapeDtypeStruct((seq, qk_cols), BF16),
            jax.ShapeDtypeStruct((seq, vc), BF16),
        ),
        in_specs=[pl.BlockSpec(memory_space=pltpu.SMEM)] + [vm] * 4,
        out_specs=(vm, vm, vm),
        scratch_shapes=[
            pltpu.VMEM((qk_cols, seq), F32),
            pltpu.VMEM((vc, seq), BF16),
            pltpu.VMEM((vc, seq), BF16),
            pltpu.VMEM((vc, seq), F32),
            pltpu.VMEM((qk_cols // heads // 2, seq), F32),
        ],
        compiler_params=pltpu.CompilerParams(vmem_limit_bytes=60 * 1024 * 1024),
        name="attn",
    )(lam, cos, sin, qk, vog)


def sender(src, dst, ssem, rsem, device):
    return pltpu.make_async_remote_copy(
        src_ref=src, dst_ref=dst, send_sem=ssem, recv_sem=rsem,
        device_id=device, device_id_type=pl.DeviceIdType.MESH,
    )


def places(sp, dp):
    me, mine = lax.axis_index("sp"), lax.axis_index("dp")
    z, core = mine // 2, lax.rem(mine, 2)
    nz = dp // 2
    if sp == 4:
        peers = [me + 1 - 2 * lax.rem(me, 2), lax.rem(me + 2, 4), 3 - me]
        froms = peers
    else:
        peers = [lax.rem(me + d, sp) for d in range(1, sp)]
        froms = [lax.rem(me + sp - d, sp) for d in range(1, sp)]
    z_to = [lax.rem(z + i, nz) * 2 for i in range(1, nz)]
    z_from = [lax.rem(z + nz - i, nz) * 2 for i in range(1, nz)]
    return me, mine, z, core, peers, froms, z_to, z_from


def greet(me, mine, core, peers, z_to):
    barrier = pltpu.get_barrier_semaphore()
    where = [(p, mine) for p in peers] + [(me, zt + core) for zt in z_to] + [(me, mine + 1 - 2 * core)]
    for device in where:
        pl.semaphore_signal(barrier, inc=1, device_id=device, device_id_type=pl.DeviceIdType.MESH)
    pl.semaphore_wait(barrier, len(where))


def gather_kernel(sp, dp, tok_ref, v_ref, og_ref, wq_ref, wk_ref, tok_all, vog_all, w_all, qk_ref,
                  vog_ref, tok_ss, tok_rs, vog_ss, vog_rs, w_ss, w_rs, sib_ss, sib_rs):
    me, mine, z, core, peers, froms, z_to, z_from = places(sp, dp)
    rows, wr = tok_ref.shape[0], wq_ref.shape[0]
    sib = (me, mine + 1 - 2 * core)

    def trow(i, start=0, size=rows):
        return pl.ds(pl.multiple_of(i * rows + start, 16), size)

    def wrow(i):
        return pl.ds(pl.multiple_of(i * wr, wr), wr)

    vc, qc = v_ref.shape[1] // sp, wq_ref.shape[1] // sp
    for s in range(sp):
        vog_ref[s, 0] = v_ref[:, s * vc : (s + 1) * vc]
        vog_ref[s, 1] = og_ref[:, s * vc : (s + 1) * vc]

        @pl.when(me == s)
        def _():
            w_all[wrow(mine), :qc] = wq_ref[:, s * qc : (s + 1) * qc]
            w_all[wrow(mine), qc:] = wk_ref[:, s * qc : (s + 1) * qc]

    tok_all[trow(me), :] = tok_ref[...]
    greet(me, mine, core, peers, z_to)
    w_ref = w_all.at[wrow(mine)]
    sends = []

    def go(copy):
        copy.start()
        sends.append(copy)
        return copy

    wz = [go(sender(w_ref, w_all.at[wrow(mine)], w_ss.at[i], w_rs.at[i], (me, zt + core)))
          for i, zt in enumerate(z_to)]
    ws = [go(sender(w_ref, w_all.at[wrow(mine)], sib_ss.at[0], sib_rs.at[0], sib))]
    half = rows // 2
    if sp == 4:
        def piece(p, h, k):
            r = trow(me, h * half, half)
            return go(sender(tok_ref.at[pl.ds(h * half, half)], tok_all.at[r], tok_ss.at[k], tok_rs.at[k], (p, mine)))

        x0, y1 = piece(peers[0], 0, 0), piece(peers[1], 1, 1)
        x1, y0 = piece(peers[0], 1, 2), piece(peers[1], 0, 3)
    else:
        tk = [go(sender(tok_ref, tok_all.at[trow(me)], tok_ss.at[i], tok_rs.at[i], (p, mine)))
              for i, p in enumerate(peers)]
    vg = [go(sender(vog_ref.at[p], vog_all.at[:, trow(me)], vog_ss.at[i], vog_rs.at[i], (p, mine)))
          for i, p in enumerate(peers)]
    vog_all[:, trow(me), :] = vog_ref[me]
    if sp == 4:
        x0.wait_recv()
        f0 = trow(peers[0], 0, half)
        d0 = go(sender(tok_all.at[f0], tok_all.at[f0], tok_ss.at[4], tok_rs.at[4], (peers[1], mine)))
        y1.wait_recv()
        f1 = trow(peers[1], half, half)
        d1 = go(sender(tok_all.at[f1], tok_all.at[f1], tok_ss.at[5], tok_rs.at[5], (peers[0], mine)))
        arrivals = [[x1], [y0], [d0, d1]]
    else:
        arrivals = [[c] for c in tk]
    for i, zf in enumerate(z_from):
        wz[i].wait_recv()
        r = wrow(zf + core)
        ws.append(go(sender(w_all.at[r], w_all.at[r], sib_ss.at[i + 1], sib_rs.at[i + 1], sib)))
    for c in ws:
        c.wait_recv()
    qk_ref[trow(me), :] = dot(tok_ref[...], w_all[...])
    for f, copies in zip(froms, arrivals):
        for c in copies:
            c.wait_recv()
        qk_ref[trow(f), :] = dot(tok_all[trow(f), :], w_all[...])
    for c in vg:
        c.wait_recv()
    for c in sends:
        c.wait_send()


def gather(tok, v, og, wq, wk, sp, dp):
    rows, width = tok.shape
    vc, wr, cols = v.shape[1] // sp, wq.shape[0], 2 * wq.shape[1] // sp
    vm = pl.BlockSpec(memory_space=pltpu.VMEM)
    dma = pltpu.SemaphoreType.DMA
    nt = 6 if sp == 4 else sp - 1
    nz = dp // 2
    return pl.pallas_call(
        functools.partial(gather_kernel, sp, dp),
        out_shape=(
            jax.ShapeDtypeStruct((rows * sp, width), BF16),
            jax.ShapeDtypeStruct((2, rows * sp, vc), BF16),
            jax.ShapeDtypeStruct((wr * dp, cols), BF16),
            jax.ShapeDtypeStruct((rows * sp, cols), F32),
        ),
        in_specs=[vm] * 5,
        out_specs=(vm,) * 4,
        scratch_shapes=[pltpu.VMEM((sp, 2, rows, vc), BF16), dma((nt,)), dma((nt,)), dma((sp - 1,)), dma((sp - 1,)),
                        dma((nz - 1,)), dma((nz - 1,)), dma((nz,)), dma((nz,))],
        compiler_params=pltpu.CompilerParams(
            vmem_limit_bytes=60 * 1024 * 1024, collective_id=0, has_side_effects=True
        ),
        name="gather",
    )(tok, v, og, wq, wk)


def scatter_kernel(sp, dp, back_t, back_m, tok_all, w_all, dv, tg_out, dv_out, qg, kg,
                   tbuf, trecv, tacc, dvr, sib_s, sib_r, wz_s, wz_r, wacc, wg_s, wg_r,
                   t_ss, t_rs, d_ss, d_rs, s_ss, s_rs, z_ss, z_rs, g_ss, g_rs):
    me, mine, z, core, peers, froms, z_to, z_from = places(sp, dp)
    nz = dp // 2
    rows, wr = tg_out.shape[0], qg.shape[0]
    vc = dv.shape[1]
    qc = w_all.shape[1] // 2
    sib = (me, mine + 1 - 2 * core)
    greet(me, mine, core, peers, z_to)
    sends = []

    def go(copy):
        copy.start()
        sends.append(copy)
        return copy

    def trow(i):
        return pl.ds(pl.multiple_of(i * rows, 16), rows)

    def weight_part(owner):
        return dot(back_t[...], tok_all[:, pl.ds(pl.multiple_of(owner * wr, wr), wr)])

    def token_part(p):
        return dot(back_m[trow(p), :], w_all[...], 1, 1)

    def send_tokens(i):
        tbuf[i] = token_part(peers[i]).astype(BF16)
        return go(sender(tbuf.at[i], trecv.at[i], t_ss.at[i], t_rs.at[i], (peers[i], mine)))

    targets = z_to + [z * 2]
    half = rows // 2
    lo, hi = pl.ds(0, half), pl.ds(half, half)
    tg = []

    def hop(i, dst, part, k, to):
        return go(sender(tbuf.at[i, part], trecv.at[dst, part], t_ss.at[k], t_rs.at[k], (peers[to], mine)))

    if sp == 4:
        tbuf[2] = token_part(peers[2]).astype(BF16)
        via_x, via_y = hop(2, 2, lo, 0, 0), hop(2, 2, hi, 1, 1)
    else:
        tg.append(send_tokens(0))
    sb = []
    for i, zt in enumerate(targets):
        sib_s[i] = weight_part(zt + 1 - core).astype(BF16)
        sb.append(go(sender(sib_s.at[i], sib_r.at[i], s_ss.at[i], s_rs.at[i], sib)))
    zs = []
    for i, zt in enumerate(targets):
        part = weight_part(zt + core)
        sb[i].wait_recv()
        part = part + sib_r[i].astype(F32)
        if i < nz - 1:
            wz_s[i] = part.astype(BF16)
            zs.append(go(sender(wz_s.at[i], wz_r.at[i], z_ss.at[i], z_rs.at[i], (me, zt + core))))
        else:
            wacc[...] = part
    if sp == 4:
        part = token_part(peers[0])
        tbuf[0, lo] = part[:half].astype(BF16)
        x_lo = hop(0, 0, lo, 2, 0)
        tacc[hi] = part[half:]
        part = token_part(peers[1])
        tbuf[1, hi] = part[half:].astype(BF16)
        y_hi = hop(1, 1, hi, 3, 1)
        tacc[lo] = part[:half]
        via_x.wait_recv()
        tbuf[1, lo] = (tacc[lo] + trecv[2, lo].astype(F32)).astype(BF16)
        y_lo = hop(1, 1, lo, 4, 1)
        via_y.wait_recv()
        tbuf[0, hi] = (tacc[hi] + trecv[2, hi].astype(F32)).astype(BF16)
        x_hi = hop(0, 0, hi, 5, 0)
        tg = [x_lo, x_hi, y_lo, y_hi]
    else:
        for i in range(1, sp - 1):
            tg.append(send_tokens(i))
    dvc = [go(sender(dv.at[trow(p)], dvr.at[me], d_ss.at[i], d_rs.at[i], (p, mine)))
           for i, p in enumerate(peers)]
    dvr[me] = dv[trow(me), :]
    tacc[...] = token_part(me)
    for i in range(nz - 1):
        zs[i].wait_recv()
        wacc[...] += wz_r[i].astype(F32)
    total = wacc[...].T.astype(BF16)
    wg_s[...] = total
    wg_r[me] = total
    wh = wr // 2
    if sp == 4:
        def piece(p, h, k):
            r = pl.ds(h * wh, wh)
            return go(sender(wg_s.at[r], wg_r.at[me, r], g_ss.at[k], g_rs.at[k], (p, mine)))

        def forward(f, h, k, p):
            r = pl.ds(h * wh, wh)
            return go(sender(wg_r.at[f, r], wg_r.at[f, r], g_ss.at[k], g_rs.at[k], (p, mine)))

        gx0, gy1 = piece(peers[0], 0, 0), piece(peers[1], 1, 1)
        gx1, gy0 = piece(peers[0], 1, 2), piece(peers[1], 0, 3)
        gx0.wait_recv()
        gd0 = forward(peers[0], 0, 4, peers[1])
        gy1.wait_recv()
        gd1 = forward(peers[1], 1, 5, peers[0])
        gs = [gx1, gy0, gd0, gd1]
    else:
        gs = [go(sender(wg_s, wg_r.at[me], g_ss.at[i], g_rs.at[i], (p, mine))) for i, p in enumerate(peers)]
    for c in tg:
        c.wait_recv()
    for i in range(2 if sp == 4 else sp - 1):
        tacc[...] += trecv[i].astype(F32)
    tg_out[...] = tacc[...].astype(BF16)
    for c in dvc:
        c.wait_recv()
    for s in range(sp):
        dv_out[:, s * vc : (s + 1) * vc] = dvr[s]
    for c in gs:
        c.wait_recv()
    for s in range(sp):
        qg[:, s * qc : (s + 1) * qc] = wg_r[s, :, :qc]
        kg[:, s * qc : (s + 1) * qc] = wg_r[s, :, qc:]
    for c in sends:
        c.wait_send()


def scatter(back_t, back_m, tok_all, w_all, dv, sp, dp):
    seq, width = tok_all.shape
    rows, wr = seq // sp, width // dp
    cols = w_all.shape[1]
    vc = dv.shape[1]
    nz = dp // 2
    vm = pl.BlockSpec(memory_space=pltpu.VMEM)
    dma = pltpu.SemaphoreType.DMA
    nt = 6 if sp == 4 else sp - 1
    return pl.pallas_call(
        functools.partial(scatter_kernel, sp, dp),
        out_shape=(
            jax.ShapeDtypeStruct((rows, width), BF16),
            jax.ShapeDtypeStruct((rows, vc * sp), BF16),
            jax.ShapeDtypeStruct((wr, cols // 2 * sp), BF16),
            jax.ShapeDtypeStruct((wr, cols // 2 * sp), BF16),
        ),
        in_specs=[vm] * 5,
        out_specs=(vm,) * 4,
        scratch_shapes=[
            pltpu.VMEM((sp - 1, rows, width), BF16),
            pltpu.VMEM((sp - 1, rows, width), BF16),
            pltpu.VMEM((rows, width), F32),
            pltpu.VMEM((sp, rows, vc), BF16),
            pltpu.VMEM((nz, cols, wr), BF16),
            pltpu.VMEM((nz, cols, wr), BF16),
            pltpu.VMEM((nz - 1, cols, wr), BF16),
            pltpu.VMEM((nz - 1, cols, wr), BF16),
            pltpu.VMEM((cols, wr), F32),
            pltpu.VMEM((wr, cols), BF16),
            pltpu.VMEM((sp, wr, cols), BF16),
            dma((nt,)), dma((nt,)), dma((sp - 1,)), dma((sp - 1,)), dma((nz,)), dma((nz,)),
            dma((nz - 1,)), dma((nz - 1,)), dma((nt,)), dma((nt,)),
        ],
        compiler_params=pltpu.CompilerParams(
            vmem_limit_bytes=62 * 1024 * 1024, collective_id=1, has_side_effects=True
        ),
        name="scatter",
    )(back_t, back_m, tok_all, w_all, dv)


def head_pair(h0, lam_ref, cos, sin, qk, vt_s, ogt_s, dvt_s, dk_s, bt_s):
    seq = cos.shape[1]
    hw = 2 * DQK
    ve = vt_s.shape[0] // 2
    inv_root = 1.0 / math.sqrt(DQK)
    step = 256
    zero_half = jnp.zeros((DQK, step), BF16)
    for hh in range(2):
        lam = lam_ref[h0 + hh]
        rows = slice(hh * hw, (hh + 1) * hw)
        vr = slice(hh * ve, (hh + 1) * ve)
        qt = rotate_rows(qk[0][rows], cos, sin).astype(BF16)
        kt = rotate_rows(qk[1][rows], cos, sin).astype(BF16)
        k = kt.T
        vt = vt_s[vr, :]
        v = vt.T
        for t0 in range(0, seq, step):
            end = min(t0 + step, seq)
            tb = end - t0
            zh = zero_half[:, :tb]
            q_b = qt[:, t0:end]
            mask = lax.broadcasted_iota(jnp.int32, (tb, tb), 0) <= lax.broadcasted_iota(
                jnp.int32, (tb, tb), 1
            )
            probs = []
            for m in range(2):
                half_q = q_b[m * DQK : (m + 1) * DQK]
                rhs = jnp.concatenate([half_q, zh] if m == 0 else [zh, half_q], axis=0)
                s = dot(k[:end], rhs) * inv_root
                diag = jnp.where(mask, s[t0:], -jnp.inf)
                s = jnp.concatenate([s[:t0], diag], axis=0) if t0 else diag
                e = jnp.exp(s - jnp.max(s, axis=0, keepdims=True))
                probs.append(e * (1.0 / jnp.sum(e, axis=0, keepdims=True)))
            p1, p2 = probs
            mix = (p1 - lam * p2).astype(BF16)
            ho = dot(vt[:, :end], mix)
            inv = lax.rsqrt(jnp.mean(ho * ho, axis=0, keepdims=True) + NORM_EPS)
            og = ogt_s[vr, t0:end].astype(F32)
            ob = (inv * og - inv * inv * inv * ho * jnp.mean(og * ho, axis=0, keepdims=True)).astype(BF16)
            mg = dot(v[:end], ob) * inv_root
            g1 = (p1 * (mg - jnp.sum(mg * p1, axis=0, keepdims=True))).astype(BF16)
            g2 = ((-lam * p2) * (mg - jnp.sum(mg * p2, axis=0, keepdims=True))).astype(BF16)
            dvd = dot(ob, mix, 1, 1)
            dkd = jnp.concatenate([dot(q_b[:DQK], g1, 1, 1), dot(q_b[DQK:], g2, 1, 1)], axis=0)
            if t0:
                dvd = jnp.concatenate([dvt_s[vr, :t0] + dvd[:, :t0], dvd[:, t0:]], axis=1)
                dkd = jnp.concatenate([dk_s[rows, :t0] + dkd[:, :t0], dkd[:, t0:]], axis=1)
            dvt_s[vr, :end] = dvd
            dk_s[rows, :end] = dkd
            dq = jnp.concatenate([dot(kt[:DQK, :end], g1), dot(kt[DQK:, :end], g2)], axis=0)
            bt_s[rows, t0:end] = rotate_rows(dq, cos[:, t0:end], -sin[:, t0:end]).astype(BF16)
        bt_s[2 * hw + hh * hw : 2 * hw + (hh + 1) * hw, :] = rotate_rows(dk_s[rows, :], cos, -sin).astype(BF16)


def fused_kernel(sp, dp, pairs, factor, lam_ref, cos_ref, sin_ref, tok_ref, v_ref, og_ref, wq_ref, wk_ref,
                 tg_out, dv_out, qg, kg,
                 tok_all, w1, w2, qk_s, vog_src, vog_all, vt_s, ogt_s, dvt_s, dk_s, bt_s, back_m, back_x,
                 dv_s, dvr, sib_s, sib_r, wz_s, wz_r, wacc, wg_r, tbuf, trecv,
                 tok_ss, tok_rs, vog_ss, vog_rs, z_ss, z_rs, s_ss, s_rs, bx_ss, bx_rs, dv_ss, dv_rs,
                 c_ss, c_rs, g_ss, g_rs, ag_ss, ag_rs, ty_ss, ty_rs):
    me, mine, z, core, peers, froms, z_to, z_from = places(sp, dp)
    nz = dp // 2
    rows, wr = tok_ref.shape[0], wq_ref.shape[0]
    half = rows // 2
    width = tok_ref.shape[1]
    pw = 128
    cw = pairs * pw
    sib = (me, mine + 1 - 2 * core)
    xp, yp = (peers[0], mine), (peers[1], mine)

    def trow(i, start=0, size=rows):
        return pl.ds(pl.multiple_of(i * rows + start, 16), size)

    def wrow(i):
        return pl.ds(pl.multiple_of(i * wr, wr), wr)

    def lanes(i, size):
        return pl.ds(pl.multiple_of(i * size, size), size)

    sends = []

    def go(copy, cond=None):
        if cond is None:
            copy.start()
        else:
            pl.when(cond)(copy.start)
        sends.append((copy, cond))
        return copy

    for w, who in ((w1, me), (w2, peers[0])):
        for j in range(pairs):
            src = lanes(who * pairs + j, pw)
            w[wrow(mine), 2 * j * pw : (2 * j + 1) * pw] = wq_ref[:, src]
            w[wrow(mine), (2 * j + 1) * pw : (2 * j + 2) * pw] = wk_ref[:, src]
    for s in range(sp):
        for j in range(pairs):
            c = (s * pairs + j) * pw
            vog_src[s, j, 0] = v_ref[:, c : c + pw]
            vog_src[s, j, 1] = og_ref[:, c : c + pw]
    tok_all[trow(me), :] = tok_ref[...]
    greet(me, mine, core, peers, z_to)

    def z_start(w, k):
        r = w.at[wrow(mine)]
        for n, d in enumerate((2, -2, 1, -1)):
            cond = (z + d < nz) if d > 0 else (z + d >= 0)
            go(sender(r, r, z_ss.at[k, n], z_rs.at[k, z], (me, (z + d) * 2 + core)), cond)
        go(sender(r, r, s_ss.at[k, z], s_rs.at[k, z], sib))

    far = lax.rem(z + 2, nz)
    order = [far, z + 1 - 2 * lax.rem(z, 2), nz - 1 - z]

    def z_step(w, k, i):
        src = order[i]
        r = w.at[wrow(2 * src + core)]
        sender(r, r, z_ss.at[k, 0], z_rs.at[k, src], sib).wait_recv()
        go(sender(r, r, s_ss.at[k, src], s_rs.at[k, src], sib))
        if i == 0:
            inner = jnp.logical_and(z > 0, z < nz - 1)
            go(sender(r, r, z_ss.at[k, 4], z_rs.at[k, src], (me, (z - 1) * (nz - 1) * 2 + core)), inner)

    def z_sib(w, k):
        for src in [z] + order:
            r = w.at[wrow(2 * src + 1 - core)]
            sender(r, r, s_ss.at[k, 0], s_rs.at[k, src], sib).wait_recv()

    def piece(p, h, k):
        r = trow(me, h * half, half)
        return go(sender(tok_ref.at[pl.ds(h * half, half)], tok_all.at[r], tok_ss.at[k], tok_rs.at[k], p))

    z_start(w1, 0)
    x0, y1 = piece(xp, 0, 0), piece(yp, 1, 1)
    x1, y0 = piece(xp, 1, 2), piece(yp, 0, 3)
    x0.wait_recv()
    f0 = trow(peers[0], 0, half)
    d0 = go(sender(tok_all.at[f0], tok_all.at[f0], tok_ss.at[4], tok_rs.at[4], yp))
    y1.wait_recv()
    f1 = trow(peers[1], half, half)
    d1 = go(sender(tok_all.at[f1], tok_all.at[f1], tok_ss.at[5], tok_rs.at[5], xp))
    for j in range(pairs):
        for i, p in enumerate(peers):
            go(sender(vog_src.at[p, j], vog_all.at[j, :, trow(me)], vog_ss.at[j, i], vog_rs.at[j, i], (p, mine)))
        vog_all[j, :, trow(me), :] = vog_src[me, j]
    for i in range(3):
        z_step(w1, 0, i)
    z_start(w2, 1)
    z_sib(w1, 0)
    qk_s[trow(me), :] = dot(tok_ref[...], w1[...])
    for f, copies in zip(froms, [[x1], [y0], [d0, d1]]):
        for c in copies:
            c.wait_recv()
        qk_s[trow(f), :] = dot(tok_all[trow(f), :], w1[...])

    targets = z_to + [z]
    cos, sin = cos_ref[...], sin_ref[...]

    def one_pair(j):
        qk = [qk_s[:, (2 * j + n) * pw : (2 * j + n + 1) * pw].T for n in range(2)]
        for i, p in enumerate(peers):
            r = vog_all.at[j, :, trow(p)]
            sender(vog_src.at[p, j], r, vog_ss.at[j, i], vog_rs.at[j, i], (p, mine)).wait_recv()
        vt_s[...] = vog_all[j, 0].T
        ogt_s[...] = vog_all[j, 1].T
        head_pair(me * 2 * pairs + 2 * j, lam_ref, cos, sin, qk, vt_s, ogt_s, dvt_s, dk_s, bt_s)
        back_m[j] = bt_s[...].T
        for b, p in enumerate((peers[0], peers[2])):
            go(sender(back_m.at[j, trow(p)], back_x.at[j, b], bx_ss.at[j, b], bx_rs.at[j, b], xp))
        dv_s[j] = dvt_s[...].T.astype(BF16)
        for i, p in enumerate(peers):
            go(sender(dv_s.at[j, trow(p)], dvr.at[me, j], dv_ss.at[j, i], dv_rs.at[j, i], (p, mine)))
        dvr[me, j] = dv_s[j, trow(me), :]

        def weight_part(owner):
            return dot(bt_s[...], tok_all[:, lanes(owner, wr)])

        for i, zt in enumerate(targets):
            zz = zt // 2 if i < nz - 1 else zt
            sib_s[j, i] = weight_part(2 * zz + 1 - core).astype(BF16)
            go(sender(sib_s.at[j, i], sib_r.at[j, i], c_ss.at[j, i], c_rs.at[j, i], sib))
        for i, zt in enumerate(targets):
            zz = zt // 2 if i < nz - 1 else zt
            part = weight_part(2 * zz + core)
            sender(sib_s.at[j, i], sib_r.at[j, i], c_ss.at[j, i], c_rs.at[j, i], sib).wait_recv()
            part = part + sib_r[j, i].astype(F32)
            if i < nz - 1:
                wz_s[j, i] = part.astype(BF16)
                go(sender(wz_s.at[j, i], wz_r.at[j, i], g_ss.at[j, i], g_rs.at[j, i], (me, zt + core)))
            else:
                wacc[j] = part

    for j in range(pairs):
        one_pair(j)
        if j == 0:
            z_step(w2, 1, 0)
            z_step(w2, 1, 1)
    z_step(w2, 1, 2)
    z_sib(w2, 1)

    nc = 4
    cols = width // nc

    def back_wait(b):
        for j in range(pairs):
            r = back_x.at[j, b]
            sender(r, r, bx_ss.at[j, b], bx_rs.at[j, b], xp).wait_recv()

    def token_part(who, b, c):
        n = slice(c * cols, (c + 1) * cols)
        out = None
        for j in range(pairs):
            k = slice(2 * j * pw, (2 * j + 2) * pw)
            for lhs, w in ((back_m[j, trow(who), :], w1), (back_x[j, b], w2)):
                part = dot(lhs, w[n, k], 1, 1)
                out = part if out is None else out + part
        return out

    back_wait(1)
    ty = []
    for c in range(nc):
        tbuf[c] = token_part(peers[1], 1, c).astype(BF16)
        ty.append(go(sender(tbuf.at[c], trecv.at[c], ty_ss.at[c], ty_rs.at[c], yp)))
    back_wait(0)

    for j in range(pairs):
        for i in range(nz - 1):
            r = wz_r.at[j, i]
            sender(r, r, g_ss.at[j, i], g_rs.at[j, i], sib).wait_recv()
            wacc[j] += wz_r[j, i].astype(F32)
        wg_r[me, j] = wacc[j].T.astype(BF16)
        mine_r = wg_r.at[me, j]
        go(sender(mine_r, mine_r, ag_ss.at[j, 0], ag_rs.at[j, 0], yp))
        go(sender(mine_r, mine_r, ag_ss.at[j, 1], ag_rs.at[j, 1], xp))
        r = wg_r.at[peers[1], j]
        sender(r, r, ag_ss.at[j, 0], ag_rs.at[j, 0], yp).wait_recv()
        go(sender(r, r, ag_ss.at[j, 2], ag_rs.at[j, 2], xp))
    for c in range(nc):
        part = token_part(me, 0, c)
        ty[c].wait_recv()
        tg_out[:, c * cols : (c + 1) * cols] = (part + trecv[c].astype(F32)).astype(BF16)
    for j in range(pairs):
        for i, p in enumerate(peers):
            r = dvr.at[p, j]
            sender(r, r, dv_ss.at[j, i], dv_rs.at[j, i], xp).wait_recv()
        for s in range(sp):
            c = (s * pairs + j) * pw
            dv_out[:, c : c + pw] = dvr[s, j]
    for j in range(pairs):
        for i, p in ((1, peers[0]), (2, peers[2])):
            r = wg_r.at[p, j]
            sender(r, r, ag_ss.at[j, i], ag_rs.at[j, i], xp).wait_recv()
        for s in range(sp):
            c = (s * pairs + j) * pw
            qg[:, c : c + pw] = wg_r[s, j, :, :pw].astype(F32) * factor
            kg[:, c : c + pw] = wg_r[s, j, :, pw:].astype(F32) * factor
    for c, cond in sends:
        if cond is None:
            c.wait_send()
        else:
            pl.when(cond)(c.wait_send)


def fused(tok, v, og, wq, wk, lam, cos, sin, sp, dp):
    rows, width = tok.shape
    seq = rows * sp
    wr = wq.shape[0]
    nz = dp // 2
    pw = 128
    pairs = v.shape[1] // (sp * pw)
    factor = 1.0 / math.sqrt(dp * seq)
    vm = pl.BlockSpec(memory_space=pltpu.VMEM)
    dma = pltpu.SemaphoreType.DMA
    V = pltpu.VMEM
    nc = 4
    return pl.pallas_call(
        functools.partial(fused_kernel, sp, dp, pairs, factor),
        out_shape=(
            jax.ShapeDtypeStruct((rows, width), BF16),
            jax.ShapeDtypeStruct((rows, v.shape[1]), BF16),
            jax.ShapeDtypeStruct((wr, wq.shape[1]), F32),
            jax.ShapeDtypeStruct((wr, wq.shape[1]), F32),
        ),
        in_specs=[pl.BlockSpec(memory_space=pltpu.SMEM)] + [vm] * 7,
        out_specs=(vm,) * 4,
        scratch_shapes=[
            V((seq, width), BF16), V((width, 2 * pairs * pw), BF16), V((width, 2 * pairs * pw), BF16),
            V((seq, 2 * pairs * pw), F32), V((sp, pairs, 2, rows, pw), BF16), V((pairs, 2, seq, pw), BF16),
            V((pw, seq), BF16), V((pw, seq), BF16), V((pw, seq), F32), V((pw, seq), F32), V((2 * pw, seq), BF16),
            V((pairs, seq, 2 * pw), BF16), V((pairs, 2, rows, 2 * pw), BF16),
            V((pairs, seq, pw), BF16), V((sp, pairs, rows, pw), BF16),
            V((pairs, nz, 2 * pw, wr), BF16), V((pairs, nz, 2 * pw, wr), BF16),
            V((pairs, nz - 1, 2 * pw, wr), BF16), V((pairs, nz - 1, 2 * pw, wr), BF16),
            V((pairs, 2 * pw, wr), F32), V((sp, pairs, wr, 2 * pw), BF16),
            V((nc, rows, width // nc), BF16), V((nc, rows, width // nc), BF16),
            dma((6,)), dma((6,)), dma((pairs, sp - 1)), dma((pairs, sp - 1)),
            dma((2, 5)), dma((2, nz)), dma((2, nz)), dma((2, nz)),
            dma((pairs, 2)), dma((pairs, 2)), dma((pairs, sp - 1)), dma((pairs, sp - 1)),
            dma((pairs, nz)), dma((pairs, nz)), dma((pairs, nz - 1)), dma((pairs, nz - 1)),
            dma((pairs, 3)), dma((pairs, 3)), dma((nc,)), dma((nc,)),
        ],
        compiler_params=pltpu.CompilerParams(
            vmem_limit_bytes=62 * 1024 * 1024, collective_id=2, has_side_effects=True
        ),
        name="fused",
    )(lam, cos, sin, tok, v, og, wq, wk)


def body(tokens, query_weight, key_weight, values, lambdas, out_grad):
    sp = lax.axis_size("sp")
    dp = lax.axis_size("dp")
    rows = tokens.shape[1]
    heads = lambdas.shape[0] // sp
    cos, sin = rotation_tables(rows * sp)
    head_vec = values.shape[2] // lambdas.shape[0]
    if sp == 4 and dp == 8 and heads % 2 == 0 and head_vec == 64 and rows * sp <= 640:
        tg, dv, qg, kg = fused(
            tokens[0], values[0], out_grad[0], query_weight, key_weight, lambdas, cos, sin, sp, dp
        )
        return tg[None], dv[None], qg, kg
    tok_all, vog_all, w_all, qk = gather(
        tokens[0], values[0], out_grad[0], query_weight, key_weight, sp, dp
    )
    back_t, back_m, dv = attention(qk, vog_all, lambdas, cos, sin, heads)
    tokens_grad, values_grad, qg, kg = scatter(back_t, back_m, tok_all, w_all, dv, sp, dp)
    factor = 1.0 / math.sqrt(dp * rows * sp)
    return tokens_grad[None], values_grad[None], qg.astype(F32) * factor, kg.astype(F32) * factor


def solution(mesh):
    x = P("dp", "sp", None)
    w = P("dp", None)
    return jax.shard_map(
        body, mesh=mesh, in_specs=(x, w, w, x, P(), x), out_specs=(x, x, w, w), check_vma=False
    )
```

```python
import functools
import math

import jax
import jax.numpy as jnp
import numpy as np
from jax import lax
from jax.experimental import pallas as pl
from jax.experimental.pallas import tpu as pltpu
from jax.sharding import PartitionSpec as P

DQK = 32
NORM_EPS = 0.1
THETA = 10000.0
F32 = jnp.float32
BF16 = jnp.bfloat16


def dot(a, b, ca=1, cb=0):
    return lax.dot_general(a, b, (((ca,), (cb,)), ((), ())), preferred_element_type=F32)


def rotation_tables(seq_length):
    half = DQK // 2
    freqs = jnp.exp(-math.log(THETA) * jnp.arange(half, dtype=F32) / half)
    angles = freqs[:, None] * jnp.arange(seq_length, dtype=jnp.int32).astype(F32)[None, :]
    return jnp.cos(angles), jnp.sin(angles)


def rotate_rows(x, cos, sin):
    half = DQK // 2
    parts = []
    for g in range(x.shape[0] // DQK):
        a = x[g * DQK : g * DQK + half]
        b = x[g * DQK + half : (g + 1) * DQK]
        parts += [a * cos - b * sin, b * cos + a * sin]
    return jnp.concatenate(parts, axis=0)


def attention_kernel(heads, lam_ref, cos_ref, sin_ref, qk_in, vog_ref, back_ref, rows_ref, dv_ref,
                     qk_ref, vt_s, ogt_s, dvt_s, dk_s):
    seq = cos_ref.shape[1]
    qc = qk_ref.shape[0] // 2
    hw = qc // heads
    ve = vog_ref.shape[2] // heads
    qk_ref[...] = qk_in[...].T
    inv_root = 1.0 / math.sqrt(DQK)
    vt_s[...] = vog_ref[0].T
    ogt_s[...] = vog_ref[1].T
    step = 256

    def one_head(h, _):
        lam = lam_ref[lax.axis_index("sp") * heads + h]
        cos, sin = cos_ref[...], sin_ref[...]
        qrow = pl.multiple_of(h * hw, hw)
        vrow = pl.multiple_of(h * ve, ve)
        qt = rotate_rows(qk_ref[pl.ds(qrow, hw), :], cos, sin).astype(BF16)
        kt = rotate_rows(qk_ref[pl.ds(qc + qrow, hw), :], cos, sin).astype(BF16)
        k = kt.T
        vt = vt_s[pl.ds(vrow, ve), :]
        v = vt.T
        zero_half = jnp.zeros((DQK, step), BF16)
        dk_s[...] = jnp.zeros_like(dk_s)
        dvt_s[pl.ds(vrow, ve), :] = jnp.zeros((ve, seq), F32)
        for t0 in range(0, seq, step):
            end = min(t0 + step, seq)
            tb = end - t0
            zh = zero_half[:, :tb]
            q_b = qt[:, t0:end]
            mask = lax.broadcasted_iota(jnp.int32, (tb, tb), 0) <= lax.broadcasted_iota(
                jnp.int32, (tb, tb), 1
            )
            probs = []
            for m in range(2):
                half_q = q_b[m * DQK : (m + 1) * DQK]
                rhs = jnp.concatenate([half_q, zh] if m == 0 else [zh, half_q], axis=0)
                s = dot(k[:end], rhs) * inv_root
                diag = jnp.where(mask, s[t0:], -jnp.inf)
                s = jnp.concatenate([s[:t0], diag], axis=0) if t0 else diag
                e = jnp.exp(s - jnp.max(s, axis=0, keepdims=True))
                probs.append(e * (1.0 / jnp.sum(e, axis=0, keepdims=True)))
            p1, p2 = probs
            mix = (p1 - lam * p2).astype(BF16)
            ho = dot(vt[:, :end], mix)
            inv = lax.rsqrt(jnp.mean(ho * ho, axis=0, keepdims=True) + NORM_EPS)
            og = ogt_s[pl.ds(vrow, ve), t0:end].astype(F32)
            ob = (inv * og - inv * inv * inv * ho * jnp.mean(og * ho, axis=0, keepdims=True)).astype(BF16)
            mg = dot(v[:end], ob) * inv_root
            g1 = (p1 * (mg - jnp.sum(mg * p1, axis=0, keepdims=True))).astype(BF16)
            g2 = ((-lam * p2) * (mg - jnp.sum(mg * p2, axis=0, keepdims=True))).astype(BF16)
            dvt_s[pl.ds(vrow, ve), :end] += dot(ob, mix, 1, 1)
            dq = jnp.concatenate([dot(kt[:DQK, :end], g1), dot(kt[DQK:, :end], g2)], axis=0)
            back_ref[pl.ds(qrow, hw), t0:end] = rotate_rows(dq, cos[:, t0:end], -sin[:, t0:end]).astype(BF16)
            dk_s[:DQK, :end] += dot(q_b[:DQK], g1, 1, 1)
            dk_s[DQK:, :end] += dot(q_b[DQK:], g2, 1, 1)
        back_ref[pl.ds(qc + qrow, hw), :] = rotate_rows(dk_s[...], cos, -sin).astype(BF16)
        return 0

    lax.fori_loop(0, heads, one_head, 0)
    dv_ref[...] = dvt_s[...].T.astype(BF16)
    rows_ref[...] = back_ref[...].T


def attention(qk, vog, lam, cos, sin, heads):
    seq, qk_cols = qk.shape
    vc = vog.shape[2]
    vm = pl.BlockSpec(memory_space=pltpu.VMEM)
    return pl.pallas_call(
        functools.partial(attention_kernel, heads),
        out_shape=(
            jax.ShapeDtypeStruct((qk_cols, seq), BF16),
            jax.ShapeDtypeStruct((seq, qk_cols), BF16),
            jax.ShapeDtypeStruct((seq, vc), BF16),
        ),
        in_specs=[pl.BlockSpec(memory_space=pltpu.SMEM)] + [vm] * 4,
        out_specs=(vm, vm, vm),
        scratch_shapes=[
            pltpu.VMEM((qk_cols, seq), F32),
            pltpu.VMEM((vc, seq), BF16),
            pltpu.VMEM((vc, seq), BF16),
            pltpu.VMEM((vc, seq), F32),
            pltpu.VMEM((qk_cols // heads // 2, seq), F32),
        ],
        compiler_params=pltpu.CompilerParams(vmem_limit_bytes=60 * 1024 * 1024),
        name="attn",
    )(lam, cos, sin, qk, vog)


def sender(src, dst, ssem, rsem, device):
    return pltpu.make_async_remote_copy(
        src_ref=src, dst_ref=dst, send_sem=ssem, recv_sem=rsem,
        device_id=device, device_id_type=pl.DeviceIdType.MESH,
    )


def places(sp, dp):
    me, mine = lax.axis_index("sp"), lax.axis_index("dp")
    z, core = mine // 2, lax.rem(mine, 2)
    nz = dp // 2
    if sp == 4:
        peers = [me + 1 - 2 * lax.rem(me, 2), lax.rem(me + 2, 4), 3 - me]
        froms = peers
    else:
        peers = [lax.rem(me + d, sp) for d in range(1, sp)]
        froms = [lax.rem(me + sp - d, sp) for d in range(1, sp)]
    z_to = [lax.rem(z + i, nz) * 2 for i in range(1, nz)]
    z_from = [lax.rem(z + nz - i, nz) * 2 for i in range(1, nz)]
    return me, mine, z, core, peers, froms, z_to, z_from


def greet(me, mine, core, peers, z_to):
    barrier = pltpu.get_barrier_semaphore()
    where = [(p, mine) for p in peers] + [(me, zt + core) for zt in z_to] + [(me, mine + 1 - 2 * core)]
    for device in where:
        pl.semaphore_signal(barrier, inc=1, device_id=device, device_id_type=pl.DeviceIdType.MESH)
    pl.semaphore_wait(barrier, len(where))


def gather_kernel(sp, dp, tok_ref, v_ref, og_ref, wq_ref, wk_ref, tok_all, vog_all, w_all, qk_ref,
                  vog_ref, tok_ss, tok_rs, vog_ss, vog_rs, w_ss, w_rs, sib_ss, sib_rs):
    me, mine, z, core, peers, froms, z_to, z_from = places(sp, dp)
    rows, wr = tok_ref.shape[0], wq_ref.shape[0]
    sib = (me, mine + 1 - 2 * core)

    def trow(i, start=0, size=rows):
        return pl.ds(pl.multiple_of(i * rows + start, 16), size)

    def wrow(i):
        return pl.ds(pl.multiple_of(i * wr, wr), wr)

    vc, qc = v_ref.shape[1] // sp, wq_ref.shape[1] // sp
    for s in range(sp):
        vog_ref[s, 0] = v_ref[:, s * vc : (s + 1) * vc]
        vog_ref[s, 1] = og_ref[:, s * vc : (s + 1) * vc]

        @pl.when(me == s)
        def _():
            w_all[wrow(mine), :qc] = wq_ref[:, s * qc : (s + 1) * qc]
            w_all[wrow(mine), qc:] = wk_ref[:, s * qc : (s + 1) * qc]

    tok_all[trow(me), :] = tok_ref[...]
    greet(me, mine, core, peers, z_to)
    w_ref = w_all.at[wrow(mine)]
    sends = []

    def go(copy):
        copy.start()
        sends.append(copy)
        return copy

    wz = [go(sender(w_ref, w_all.at[wrow(mine)], w_ss.at[i], w_rs.at[i], (me, zt + core)))
          for i, zt in enumerate(z_to)]
    ws = [go(sender(w_ref, w_all.at[wrow(mine)], sib_ss.at[0], sib_rs.at[0], sib))]
    half = rows // 2
    if sp == 4:
        def piece(p, h, k):
            r = trow(me, h * half, half)
            return go(sender(tok_ref.at[pl.ds(h * half, half)], tok_all.at[r], tok_ss.at[k], tok_rs.at[k], (p, mine)))

        x0, y1 = piece(peers[0], 0, 0), piece(peers[1], 1, 1)
        x1, y0 = piece(peers[0], 1, 2), piece(peers[1], 0, 3)
    else:
        tk = [go(sender(tok_ref, tok_all.at[trow(me)], tok_ss.at[i], tok_rs.at[i], (p, mine)))
              for i, p in enumerate(peers)]
    vg = [go(sender(vog_ref.at[p], vog_all.at[:, trow(me)], vog_ss.at[i], vog_rs.at[i], (p, mine)))
          for i, p in enumerate(peers)]
    vog_all[:, trow(me), :] = vog_ref[me]
    if sp == 4:
        x0.wait_recv()
        f0 = trow(peers[0], 0, half)
        d0 = go(sender(tok_all.at[f0], tok_all.at[f0], tok_ss.at[4], tok_rs.at[4], (peers[1], mine)))
        y1.wait_recv()
        f1 = trow(peers[1], half, half)
        d1 = go(sender(tok_all.at[f1], tok_all.at[f1], tok_ss.at[5], tok_rs.at[5], (peers[0], mine)))
        arrivals = [[x1], [y0], [d0, d1]]
    else:
        arrivals = [[c] for c in tk]
    for i, zf in enumerate(z_from):
        wz[i].wait_recv()
        r = wrow(zf + core)
        ws.append(go(sender(w_all.at[r], w_all.at[r], sib_ss.at[i + 1], sib_rs.at[i + 1], sib)))
    for c in ws:
        c.wait_recv()
    qk_ref[trow(me), :] = dot(tok_ref[...], w_all[...])
    for f, copies in zip(froms, arrivals):
        for c in copies:
            c.wait_recv()
        qk_ref[trow(f), :] = dot(tok_all[trow(f), :], w_all[...])
    for c in vg:
        c.wait_recv()
    for c in sends:
        c.wait_send()


def gather(tok, v, og, wq, wk, sp, dp):
    rows, width = tok.shape
    vc, wr, cols = v.shape[1] // sp, wq.shape[0], 2 * wq.shape[1] // sp
    vm = pl.BlockSpec(memory_space=pltpu.VMEM)
    dma = pltpu.SemaphoreType.DMA
    nt = 6 if sp == 4 else sp - 1
    nz = dp // 2
    return pl.pallas_call(
        functools.partial(gather_kernel, sp, dp),
        out_shape=(
            jax.ShapeDtypeStruct((rows * sp, width), BF16),
            jax.ShapeDtypeStruct((2, rows * sp, vc), BF16),
            jax.ShapeDtypeStruct((wr * dp, cols), BF16),
            jax.ShapeDtypeStruct((rows * sp, cols), F32),
        ),
        in_specs=[vm] * 5,
        out_specs=(vm,) * 4,
        scratch_shapes=[pltpu.VMEM((sp, 2, rows, vc), BF16), dma((nt,)), dma((nt,)), dma((sp - 1,)), dma((sp - 1,)),
                        dma((nz - 1,)), dma((nz - 1,)), dma((nz,)), dma((nz,))],
        compiler_params=pltpu.CompilerParams(
            vmem_limit_bytes=60 * 1024 * 1024, collective_id=0, has_side_effects=True
        ),
        name="gather",
    )(tok, v, og, wq, wk)


def scatter_kernel(sp, dp, back_t, back_m, tok_all, w_all, dv, tg_out, dv_out, qg, kg,
                   tbuf, trecv, tacc, dvr, sib_s, sib_r, wz_s, wz_r, wacc, wg_s, wg_r,
                   t_ss, t_rs, d_ss, d_rs, s_ss, s_rs, z_ss, z_rs, g_ss, g_rs):
    me, mine, z, core, peers, froms, z_to, z_from = places(sp, dp)
    nz = dp // 2
    rows, wr = tg_out.shape[0], qg.shape[0]
    vc = dv.shape[1]
    qc = w_all.shape[1] // 2
    sib = (me, mine + 1 - 2 * core)
    greet(me, mine, core, peers, z_to)
    sends = []

    def go(copy):
        copy.start()
        sends.append(copy)
        return copy

    def trow(i):
        return pl.ds(pl.multiple_of(i * rows, 16), rows)

    def weight_part(owner):
        return dot(back_t[...], tok_all[:, pl.ds(pl.multiple_of(owner * wr, wr), wr)])

    def token_part(p):
        return dot(back_m[trow(p), :], w_all[...], 1, 1)

    def send_tokens(i):
        tbuf[i] = token_part(peers[i]).astype(BF16)
        return go(sender(tbuf.at[i], trecv.at[i], t_ss.at[i], t_rs.at[i], (peers[i], mine)))

    targets = z_to + [z * 2]
    half = rows // 2
    lo, hi = pl.ds(0, half), pl.ds(half, half)
    tg = []

    def hop(i, dst, part, k, to):
        return go(sender(tbuf.at[i, part], trecv.at[dst, part], t_ss.at[k], t_rs.at[k], (peers[to], mine)))

    if sp == 4:
        tbuf[2] = token_part(peers[2]).astype(BF16)
        via_x, via_y = hop(2, 2, lo, 0, 0), hop(2, 2, hi, 1, 1)
    else:
        tg.append(send_tokens(0))
    sb = []
    for i, zt in enumerate(targets):
        sib_s[i] = weight_part(zt + 1 - core).astype(BF16)
        sb.append(go(sender(sib_s.at[i], sib_r.at[i], s_ss.at[i], s_rs.at[i], sib)))
    zs = []
    for i, zt in enumerate(targets):
        part = weight_part(zt + core)
        sb[i].wait_recv()
        part = part + sib_r[i].astype(F32)
        if i < nz - 1:
            wz_s[i] = part.astype(BF16)
            zs.append(go(sender(wz_s.at[i], wz_r.at[i], z_ss.at[i], z_rs.at[i], (me, zt + core))))
        else:
            wacc[...] = part
    if sp == 4:
        part = token_part(peers[0])
        tbuf[0, lo] = part[:half].astype(BF16)
        x_lo = hop(0, 0, lo, 2, 0)
        tacc[hi] = part[half:]
        part = token_part(peers[1])
        tbuf[1, hi] = part[half:].astype(BF16)
        y_hi = hop(1, 1, hi, 3, 1)
        tacc[lo] = part[:half]
        via_x.wait_recv()
        tbuf[1, lo] = (tacc[lo] + trecv[2, lo].astype(F32)).astype(BF16)
        y_lo = hop(1, 1, lo, 4, 1)
        via_y.wait_recv()
        tbuf[0, hi] = (tacc[hi] + trecv[2, hi].astype(F32)).astype(BF16)
        x_hi = hop(0, 0, hi, 5, 0)
        tg = [x_lo, x_hi, y_lo, y_hi]
    else:
        for i in range(1, sp - 1):
            tg.append(send_tokens(i))
    dvc = [go(sender(dv.at[trow(p)], dvr.at[me], d_ss.at[i], d_rs.at[i], (p, mine)))
           for i, p in enumerate(peers)]
    dvr[me] = dv[trow(me), :]
    tacc[...] = token_part(me)
    for i in range(nz - 1):
        zs[i].wait_recv()
        wacc[...] += wz_r[i].astype(F32)
    total = wacc[...].T.astype(BF16)
    wg_s[...] = total
    wg_r[me] = total
    wh = wr // 2
    if sp == 4:
        def piece(p, h, k):
            r = pl.ds(h * wh, wh)
            return go(sender(wg_s.at[r], wg_r.at[me, r], g_ss.at[k], g_rs.at[k], (p, mine)))

        def forward(f, h, k, p):
            r = pl.ds(h * wh, wh)
            return go(sender(wg_r.at[f, r], wg_r.at[f, r], g_ss.at[k], g_rs.at[k], (p, mine)))

        gx0, gy1 = piece(peers[0], 0, 0), piece(peers[1], 1, 1)
        gx1, gy0 = piece(peers[0], 1, 2), piece(peers[1], 0, 3)
        gx0.wait_recv()
        gd0 = forward(peers[0], 0, 4, peers[1])
        gy1.wait_recv()
        gd1 = forward(peers[1], 1, 5, peers[0])
        gs = [gx1, gy0, gd0, gd1]
    else:
        gs = [go(sender(wg_s, wg_r.at[me], g_ss.at[i], g_rs.at[i], (p, mine))) for i, p in enumerate(peers)]
    for c in tg:
        c.wait_recv()
    for i in range(2 if sp == 4 else sp - 1):
        tacc[...] += trecv[i].astype(F32)
    tg_out[...] = tacc[...].astype(BF16)
    for c in dvc:
        c.wait_recv()
    for s in range(sp):
        dv_out[:, s * vc : (s + 1) * vc] = dvr[s]
    for c in gs:
        c.wait_recv()
    for s in range(sp):
        qg[:, s * qc : (s + 1) * qc] = wg_r[s, :, :qc]
        kg[:, s * qc : (s + 1) * qc] = wg_r[s, :, qc:]
    for c in sends:
        c.wait_send()


def scatter(back_t, back_m, tok_all, w_all, dv, sp, dp):
    seq, width = tok_all.shape
    rows, wr = seq // sp, width // dp
    cols = w_all.shape[1]
    vc = dv.shape[1]
    nz = dp // 2
    vm = pl.BlockSpec(memory_space=pltpu.VMEM)
    dma = pltpu.SemaphoreType.DMA
    nt = 6 if sp == 4 else sp - 1
    return pl.pallas_call(
        functools.partial(scatter_kernel, sp, dp),
        out_shape=(
            jax.ShapeDtypeStruct((rows, width), BF16),
            jax.ShapeDtypeStruct((rows, vc * sp), BF16),
            jax.ShapeDtypeStruct((wr, cols // 2 * sp), BF16),
            jax.ShapeDtypeStruct((wr, cols // 2 * sp), BF16),
        ),
        in_specs=[vm] * 5,
        out_specs=(vm,) * 4,
        scratch_shapes=[
            pltpu.VMEM((sp - 1, rows, width), BF16),
            pltpu.VMEM((sp - 1, rows, width), BF16),
            pltpu.VMEM((rows, width), F32),
            pltpu.VMEM((sp, rows, vc), BF16),
            pltpu.VMEM((nz, cols, wr), BF16),
            pltpu.VMEM((nz, cols, wr), BF16),
            pltpu.VMEM((nz - 1, cols, wr), BF16),
            pltpu.VMEM((nz - 1, cols, wr), BF16),
            pltpu.VMEM((cols, wr), F32),
            pltpu.VMEM((wr, cols), BF16),
            pltpu.VMEM((sp, wr, cols), BF16),
            dma((nt,)), dma((nt,)), dma((sp - 1,)), dma((sp - 1,)), dma((nz,)), dma((nz,)),
            dma((nz - 1,)), dma((nz - 1,)), dma((nt,)), dma((nt,)),
        ],
        compiler_params=pltpu.CompilerParams(
            vmem_limit_bytes=62 * 1024 * 1024, collective_id=1, has_side_effects=True
        ),
        name="scatter",
    )(back_t, back_m, tok_all, w_all, dv)


def position_tables(seq_length):
    half = DQK // 2
    freqs = np.exp(np.float32(-math.log(THETA)) * np.arange(half, dtype=np.float32) / np.float32(half)).astype(np.float32)
    angles = freqs[:, None] * np.arange(seq_length, dtype=np.float32)[None, :]
    wide = angles.astype(np.float64)
    return jnp.asarray(np.concatenate([np.cos(wide), np.sin(wide)]).astype(np.float32))


def head_scores(hh, cos, sin, q, k_in, qt_s, kt_s, p_s, lam):
    seq = cos.shape[1]
    scale = math.log2(math.e) / math.sqrt(DQK)
    step = 256
    zero_half = jnp.zeros((DQK, step), BF16)
    qt = rotate_rows(q, cos, sin).astype(BF16)
    kt = rotate_rows(k_in, cos, sin).astype(BF16)
    qt_s[hh] = qt
    kt_s[hh] = kt
    k = kt.T
    for t0 in range(0, seq, step):
        end = min(t0 + step, seq)
        tb = end - t0
        zh = zero_half[:, :tb]
        q_b = qt[:, t0:end]
        mask = lax.broadcasted_iota(jnp.int32, (tb, tb), 0) <= lax.broadcasted_iota(jnp.int32, (tb, tb), 1)
        for m in range(2):
            half_q = q_b[m * DQK : (m + 1) * DQK]
            rhs = jnp.concatenate([half_q, zh] if m == 0 else [zh, half_q], axis=0)
            s = dot(k[:end], rhs)
            diag = jnp.where(mask, s[t0:], -jnp.inf)
            s = jnp.concatenate([s[:t0], diag], axis=0) if t0 else diag
            e = jnp.exp2((s - jnp.max(s, axis=0, keepdims=True)) * scale)
            r = 1.0 / jnp.sum(e, axis=0, keepdims=True)
            p_s[hh, m, :end, t0:end] = e * (r if m == 0 else r * -lam)


def head_back(hh, cos, sin, lam, qt_s, kt_s, p_s, vt_s, ogt_s, dvt_s, dk_s, bt_s):
    seq = cos.shape[1]
    hw = 2 * DQK
    ve = vt_s.shape[0] // 2
    inv_root = 1.0 / math.sqrt(DQK)
    step = 256
    rows = slice(hh * hw, (hh + 1) * hw)
    vr = slice(hh * ve, (hh + 1) * ve)
    qt, kt = qt_s[hh], kt_s[hh]
    vt = vt_s[vr, :]
    v = vt.T
    cb, sb = cos * inv_root, sin * -inv_root
    for t0 in range(0, seq, step):
        end = min(t0 + step, seq)
        q_b = qt[:, t0:end]
        p1, p2 = p_s[hh, 0, :end, t0:end], p_s[hh, 1, :end, t0:end]
        mix = (p1 + p2).astype(BF16)
        ho = dot(vt[:, :end], mix)
        inv = lax.rsqrt(jnp.mean(ho * ho, axis=0, keepdims=True) + NORM_EPS)
        og = ogt_s[vr, t0:end].astype(F32)
        ob = (inv * og - inv * inv * inv * ho * jnp.mean(og * ho, axis=0, keepdims=True)).astype(BF16)
        mg = dot(v[:end], ob)
        g1 = (p1 * (mg - jnp.sum(mg * p1, axis=0, keepdims=True))).astype(BF16)
        g2 = (p2 * (mg + jnp.sum(mg * p2, axis=0, keepdims=True) * (1.0 / lam))).astype(BF16)
        dvd = dot(ob, mix, 1, 1)
        dkd = jnp.concatenate([dot(q_b[:DQK], g1, 1, 1), dot(q_b[DQK:], g2, 1, 1)], axis=0)
        if t0:
            dvd = jnp.concatenate([dvt_s[vr, :t0] + dvd[:, :t0], dvd[:, t0:]], axis=1)
            dkd = jnp.concatenate([dk_s[rows, :t0] + dkd[:, :t0], dkd[:, t0:]], axis=1)
        dvt_s[vr, :end] = dvd
        dk_s[rows, :end] = dkd
        dq = jnp.concatenate([dot(kt[:DQK, :end], g1), dot(kt[DQK:, :end], g2)], axis=0)
        bt_s[rows, t0:end] = rotate_rows(dq, cb[:, t0:end], sb[:, t0:end]).astype(BF16)
    bt_s[2 * hw + hh * hw : 2 * hw + (hh + 1) * hw, :] = rotate_rows(dk_s[rows, :], cb, sb).astype(BF16)


def fused_kernel(sp, dp, pairs, lam_in, rot_in, tok_in, v_in, og_in, wq_in, wk_in,
                 tg_out, dvr, wg_r,
                 lam_ref, rot_ref, tok_all, w1, w2, qk_s, vog_src, vog_all, qt_s, kt_s, p_s,
                 vt_s, ogt_s, dvt_s, dk_s, bt_s, back_m, back_x,
                 dv_s, sib_s, sib_r, own_s, wz_s, wz_r, tbuf, trecv,
                 l_s, tok_ss, tok_rs, vog_ss, vog_rs, z_ss, z_rs, s_ss, s_rs, bx_ss, bx_rs, dv_ss, dv_rs,
                 c_ss, c_rs, g_ss, g_rs, ag_ss, ag_rs, ty_ss, ty_rs):
    me, mine, z, core, peers, froms, z_to, z_from = places(sp, dp)
    nz = dp // 2
    rows, wr = tok_in.shape[0], wq_in.shape[0]
    half = rows // 2
    pw = 128
    sib = (me, mine + 1 - 2 * core)
    xp, yp = (peers[0], mine), (peers[1], mine)

    def trow(i, start=0, size=rows):
        return pl.ds(pl.multiple_of(i * rows + start, 16), size)

    def wrow(i):
        return pl.ds(pl.multiple_of(i * wr, wr), wr)

    def lanes(i, size):
        return pl.ds(pl.multiple_of(i * size, size), size)

    sends = []

    def go(copy, cond=None):
        if cond is None:
            copy.start()
        else:
            pl.when(cond)(copy.start)
        sends.append((copy, cond))
        return copy

    barrier = pltpu.get_barrier_semaphore()
    where = [(p, mine) for p in peers] + [(me, zt + core) for zt in z_to] + [sib]
    for device in where:
        pl.semaphore_signal(barrier, inc=1, device_id=device, device_id_type=pl.DeviceIdType.MESH)

    count = [0]

    def load(src, dst):
        c = pltpu.make_async_copy(src, dst, l_s.at[count[0]])
        count[0] += 1
        c.start()
        return c

    def load_weights(w, who):
        out = []
        for j in range(pairs):
            src = lanes(who * pairs + j, pw)
            out.append(load(wq_in.at[:, src], w.at[wrow(mine), 2 * j * pw : (2 * j + 1) * pw]))
            out.append(load(wk_in.at[:, src], w.at[wrow(mine), (2 * j + 1) * pw : (2 * j + 2) * pw]))
        return out

    l_tok = [load(tok_in, tok_all.at[trow(me)])]
    l_w1 = load_weights(w1, me)
    l_vog = []
    for j in range(pairs):
        for n, src in enumerate((v_in, og_in)):
            for i, p in enumerate(peers):
                l_vog.append(load(src.at[:, lanes(p * pairs + j, pw)], vog_src.at[i, j, n]))
            l_vog.append(load(src.at[:, lanes(me * pairs + j, pw)], vog_all.at[j, n, trow(me)]))
    l_w2 = load_weights(w2, jnp.where(core == 0, peers[0], peers[1]))
    l_rot = [load(rot_in, rot_ref), load(lam_in, lam_ref)]

    def z_start(w, k):
        r = w.at[wrow(mine)]
        for n, d in enumerate((2, -2, 1, -1)):
            cond = (z + d < nz) if d > 0 else (z + d >= 0)
            go(sender(r, r, z_ss.at[k, n], z_rs.at[k, z], (me, (z + d) * 2 + core)), cond)
        go(sender(r, r, s_ss.at[k, z], s_rs.at[k, z], sib))

    far = lax.rem(z + 2, nz)
    order = [far, z + 1 - 2 * lax.rem(z, 2), nz - 1 - z]

    def z_step(w, k, i):
        src = order[i]
        r = w.at[wrow(2 * src + core)]
        sender(r, r, z_ss.at[k, 0], z_rs.at[k, src], sib).wait_recv()
        go(sender(r, r, s_ss.at[k, src], s_rs.at[k, src], sib))
        if i == 0:
            inner = jnp.logical_and(z > 0, z < nz - 1)
            go(sender(r, r, z_ss.at[k, 4], z_rs.at[k, src], (me, (z - 1) * (nz - 1) * 2 + core)), inner)

    def z_sib(w, k):
        for src in [z] + order:
            r = w.at[wrow(2 * src + 1 - core)]
            sender(r, r, s_ss.at[k, 0], s_rs.at[k, src], sib).wait_recv()

    def piece(p, h, k):
        r = trow(me, h * half, half)
        return go(sender(tok_all.at[r], tok_all.at[r], tok_ss.at[k], tok_rs.at[k], p))

    for c in l_tok:
        c.wait()
    pl.semaphore_wait(barrier, len(where))
    x0, y1 = piece(xp, 0, 0), piece(yp, 1, 1)
    x1, y0 = piece(xp, 1, 2), piece(yp, 0, 3)
    for c in l_w1:
        c.wait()
    z_start(w1, 0)
    for c in l_w2 + l_vog + l_rot:
        c.wait()
    x0.wait_recv()
    f0 = trow(peers[0], 0, half)
    d0 = go(sender(tok_all.at[f0], tok_all.at[f0], tok_ss.at[4], tok_rs.at[4], yp))
    y1.wait_recv()
    f1 = trow(peers[1], half, half)
    d1 = go(sender(tok_all.at[f1], tok_all.at[f1], tok_ss.at[5], tok_rs.at[5], xp))
    for j in range(pairs):
        for i, p in enumerate(peers):
            go(sender(vog_src.at[i, j], vog_all.at[j, :, trow(me)], vog_ss.at[j, i], vog_rs.at[j, i], (p, mine)))
    z_step(w1, 0, 0)
    z_start(w2, 1)
    z_step(w1, 0, 1)
    z_step(w1, 0, 2)
    z_sib(w1, 0)
    qk_s[trow(me), :] = dot(tok_all[trow(me), :], w1[...])
    for f, copies in zip(froms, [[x1], [y0], [d0, d1]]):
        for c in copies:
            c.wait_recv()
        qk_s[trow(f), :] = dot(tok_all[trow(f), :], w1[...])

    targets = [lax.rem(z + i, nz) for i in range(1, nz)] + [z]
    n16 = DQK // 2
    cos, sin = rot_ref[:n16, :], rot_ref[n16:, :]
    hw = 2 * DQK

    def one_pair(j):
        qk = [qk_s[:, (2 * j + n) * pw : (2 * j + n + 1) * pw].T for n in range(2)]
        lams = [lam_ref[(me * pairs + j) * 2 + hh] for hh in range(2)]
        for hh in range(2):
            r = slice(hh * hw, (hh + 1) * hw)
            head_scores(hh, cos, sin, qk[0][r], qk[1][r], qt_s, kt_s, p_s, lams[hh])
        for i, p in enumerate(peers):
            r = vog_all.at[j, :, trow(p)]
            sender(vog_src.at[i, j], r, vog_ss.at[j, i], vog_rs.at[j, i], (p, mine)).wait_recv()
        if j == 0:
            z_step(w2, 1, 0)
        vt_s[...] = vog_all[j, 0].T
        ogt_s[...] = vog_all[j, 1].T
        for hh in range(2):
            head_back(hh, cos, sin, lams[hh], qt_s, kt_s, p_s, vt_s, ogt_s, dvt_s, dk_s, bt_s)
        back_m[j] = bt_s[...].T
        for a, to in enumerate((0, 1)):
            for b, p in enumerate((peers[to], peers[2])):
                go(sender(back_m.at[j, trow(p)], back_x.at[a, j, b], bx_ss.at[a, j, b], bx_rs.at[a, j, b], (xp, yp)[to]))

        def weight_part(owner):
            return dot(bt_s[...], tok_all[:, lanes(owner, wr)])

        for i, zz in enumerate(targets):
            sib_s[j, i] = weight_part(2 * zz + 1 - core).astype(BF16)
        for i in range(nz):
            go(sender(sib_s.at[j, i], sib_r.at[j, i], c_ss.at[j, i], c_rs.at[j, i], sib))
        for i, zz in enumerate(targets):
            own_s[j, i] = weight_part(2 * zz + core)
        dv_s[j] = dvt_s[...].T.astype(BF16)
        for i, p in enumerate(peers):
            go(sender(dv_s.at[j, trow(p)], dvr.at[me, j], dv_ss.at[j, i], dv_rs.at[j, i], (p, mine)))
        dvr[me, j] = dv_s[j, trow(me), :]
        for i, zz in enumerate(targets):
            sender(sib_s.at[j, i], sib_r.at[j, i], c_ss.at[j, i], c_rs.at[j, i], sib).wait_recv()
            part = own_s[j, i] + sib_r[j, i].astype(F32)
            if i < nz - 1:
                wz_s[j, i] = part.astype(BF16)
            else:
                own_s[j, i] = part
        for i, zz in enumerate(targets[: nz - 1]):
            go(sender(wz_s.at[j, i], wz_r.at[j, i], g_ss.at[j, i], g_rs.at[j, i], (me, 2 * zz + core)))

    for j in range(pairs):
        one_pair(j)
        if j == 0:
            z_step(w2, 1, 1)
    z_step(w2, 1, 2)
    z_sib(w2, 1)

    def back_wait(a, b):
        for j in range(pairs):
            r = back_x.at[a, j, b]
            sender(r, r, bx_ss.at[a, j, b], bx_rs.at[a, j, b], sib).wait_recv()

    def token_part(who, a, b, c):
        n = slice((2 * c + a) * wr, (2 * c + a + 1) * wr)
        out = None
        for j in range(pairs):
            k = slice(2 * j * pw, (2 * j + 2) * pw)
            for lhs, w in ((back_m[j, trow(who), :], w1), (back_x[a, j, b], w2)):
                part = dot(lhs, w[n, k], 1, 1)
                out = part if out is None else out + part
        return out

    ty = []
    for a in range(2):
        back_wait(a, 1)
        for c in range(nz):
            tbuf[a, c] = token_part(peers[1 - a], a, 1, c).astype(BF16)
        for c in range(nz):
            ty.append(go(sender(tbuf.at[a, c], trecv.at[a, c], ty_ss.at[a, c], ty_rs.at[a, c], (yp, xp)[a])))

    def weights_end(j):
        total = own_s[j, nz - 1]
        for i in range(nz - 1):
            r = wz_r.at[j, i]
            sender(r, r, g_ss.at[j, i], g_rs.at[j, i], sib).wait_recv()
            total = total + wz_r[j, i].astype(F32)
        wg_r[me, j] = total.T.astype(BF16)
        r = wg_r.at[me, j]
        for i in (2, 0, 1):
            go(sender(r, r, ag_ss.at[j, i], ag_rs.at[j, i], (peers[i], mine)))

    for j in range(pairs):
        weights_end(j)
        if j == 0:
            for a in range(2):
                back_wait(a, 0)
                for c in range(nz):
                    part = token_part(me, a, 0, c)
                    ty[a * nz + c].wait_recv()
                    n = slice((2 * c + a) * wr, (2 * c + a + 1) * wr)
                    tg_out[:, n] = (part + trecv[a, c].astype(F32)).astype(BF16)
    for j in range(pairs):
        for i, p in enumerate(peers):
            r = dvr.at[p, j]
            sender(r, r, dv_ss.at[j, i], dv_rs.at[j, i], xp).wait_recv()
        for i, p in enumerate(peers):
            r = wg_r.at[p, j]
            sender(r, r, ag_ss.at[j, i], ag_rs.at[j, i], xp).wait_recv()
    for c, cond in sends:
        if cond is None:
            c.wait_send()
        else:
            pl.when(cond)(c.wait_send)


def finish_kernel(factor, tg, dvr, wg, tg_out, dv_out, qg_out, kg_out, dv_s, qg, kg, sem):
    sp, pairs, wr, cols = wg.shape
    pw = cols // 2
    copies = [pltpu.make_async_copy(tg, tg_out, sem.at[0])]
    copies[0].start()
    for s in range(sp):
        for j in range(pairs):
            n = slice((s * pairs + j) * pw, (s * pairs + j + 1) * pw)
            qg[:, n] = wg[s, j, :, :pw].astype(F32) * factor
    copies.append(pltpu.make_async_copy(qg, qg_out, sem.at[1]))
    copies[1].start()
    for s in range(sp):
        for j in range(pairs):
            n = slice((s * pairs + j) * pw, (s * pairs + j + 1) * pw)
            kg[:, n] = wg[s, j, :, pw:].astype(F32) * factor
    copies.append(pltpu.make_async_copy(kg, kg_out, sem.at[2]))
    copies[2].start()
    for s in range(sp):
        for j in range(pairs):
            n = slice((s * pairs + j) * pw, (s * pairs + j + 1) * pw)
            dv_s[:, n] = dvr[s, j]
    copies.append(pltpu.make_async_copy(dv_s, dv_out, sem.at[3]))
    copies[3].start()
    for c in copies:
        c.wait()


def fused(tok, v, og, wq, wk, lam, rot, sp, dp):
    rows, width = tok.shape
    seq = rows * sp
    wr = wq.shape[0]
    nz = dp // 2
    pw = 128
    pairs = v.shape[1] // (sp * pw)
    factor = 1.0 / math.sqrt(dp * seq)
    vm = pl.BlockSpec(memory_space=pltpu.VMEM)
    anywhere = pl.BlockSpec(memory_space=pl.ANY)
    dma = pltpu.SemaphoreType.DMA
    V = pltpu.VMEM
    tg, dvr, wg = pl.pallas_call(
        functools.partial(fused_kernel, sp, dp, pairs),
        out_shape=(
            V((rows, width), BF16),
            V((sp, pairs, rows, pw), BF16),
            V((sp, pairs, wr, 2 * pw), BF16),
        ),
        in_specs=[anywhere] * 7,
        out_specs=(vm,) * 3,
        scratch_shapes=[
            pltpu.SMEM(lam.shape, F32), V(rot.shape, F32),
            V((seq, width), BF16), V((width, 2 * pairs * pw), BF16), V((width, 2 * pairs * pw), BF16),
            V((seq, 2 * pairs * pw), F32), V((sp - 1, pairs, 2, rows, pw), BF16), V((pairs, 2, seq, pw), BF16),
            V((2, 2 * DQK, seq), BF16), V((2, 2 * DQK, seq), BF16), V((2, 2, seq, seq), F32),
            V((pw, seq), BF16), V((pw, seq), BF16), V((pw, seq), F32), V((pw, seq), F32), V((2 * pw, seq), BF16),
            V((pairs, seq, 2 * pw), BF16), V((2, pairs, 2, rows, 2 * pw), BF16),
            V((pairs, seq, pw), BF16),
            V((pairs, nz, 2 * pw, wr), BF16), V((pairs, nz, 2 * pw, wr), BF16), V((pairs, nz, 2 * pw, wr), F32),
            V((pairs, nz - 1, 2 * pw, wr), BF16), V((pairs, nz - 1, 2 * pw, wr), BF16),
            V((2, nz, rows, wr), BF16), V((2, nz, rows, wr), BF16),
            dma((3 + 8 * pairs + 2 * sp * pairs,)),
            dma((6,)), dma((6,)), dma((pairs, sp - 1)), dma((pairs, sp - 1)),
            dma((2, 5)), dma((2, nz)), dma((2, nz)), dma((2, nz)),
            dma((2, pairs, 2)), dma((2, pairs, 2)), dma((pairs, sp - 1)), dma((pairs, sp - 1)),
            dma((pairs, nz)), dma((pairs, nz)), dma((pairs, nz - 1)), dma((pairs, nz - 1)),
            dma((pairs, 3)), dma((pairs, 3)), dma((2, nz)), dma((2, nz)),
        ],
        compiler_params=pltpu.CompilerParams(
            vmem_limit_bytes=56 * 1024 * 1024, collective_id=2, has_side_effects=True
        ),
        name="fused",
    )(lam, rot, tok, v, og, wq, wk)
    return pl.pallas_call(
        functools.partial(finish_kernel, factor),
        out_shape=(
            jax.ShapeDtypeStruct((rows, width), BF16),
            jax.ShapeDtypeStruct((rows, v.shape[1]), BF16),
            jax.ShapeDtypeStruct((wr, wq.shape[1]), F32),
            jax.ShapeDtypeStruct((wr, wq.shape[1]), F32),
        ),
        in_specs=[vm] * 3,
        out_specs=(anywhere,) * 4,
        scratch_shapes=[V((rows, v.shape[1]), BF16), V((wr, wq.shape[1]), F32), V((wr, wq.shape[1]), F32), dma((4,))],
        compiler_params=pltpu.CompilerParams(vmem_limit_bytes=16 * 1024 * 1024),
        name="finish",
    )(tg, dvr, wg)


def body(tokens, query_weight, key_weight, values, lambdas, out_grad):
    sp = lax.axis_size("sp")
    dp = lax.axis_size("dp")
    rows = tokens.shape[1]
    heads = lambdas.shape[0] // sp
    head_vec = values.shape[2] // lambdas.shape[0]
    if sp == 4 and dp == 8 and heads % 2 == 0 and head_vec == 64 and rows * sp <= 640:
        tg, dv, qg, kg = fused(
            tokens[0], values[0], out_grad[0], query_weight, key_weight, lambdas,
            position_tables(rows * sp), sp, dp,
        )
        return tg[None], dv[None], qg, kg
    cos, sin = rotation_tables(rows * sp)
    tok_all, vog_all, w_all, qk = gather(
        tokens[0], values[0], out_grad[0], query_weight, key_weight, sp, dp
    )
    back_t, back_m, dv = attention(qk, vog_all, lambdas, cos, sin, heads)
    tokens_grad, values_grad, qg, kg = scatter(back_t, back_m, tok_all, w_all, dv, sp, dp)
    factor = 1.0 / math.sqrt(dp * rows * sp)
    return tokens_grad[None], values_grad[None], qg.astype(F32) * factor, kg.astype(F32) * factor


def solution(mesh):
    x = P("dp", "sp", None)
    w = P("dp", None)
    return jax.shard_map(
        body, mesh=mesh, in_specs=(x, w, w, x, P(), x), out_specs=(x, x, w, w), check_vma=False
    )
```

```python
import functools
import math

import jax
import jax.numpy as jnp
import numpy as np
from jax import lax
from jax.experimental import pallas as pl
from jax.experimental.pallas import tpu as pltpu
from jax.sharding import PartitionSpec as P

DQK = 32
NORM_EPS = 0.1
THETA = 10000.0
F32 = jnp.float32
BF16 = jnp.bfloat16


def dot(a, b, ca=1, cb=0):
    return lax.dot_general(a, b, (((ca,), (cb,)), ((), ())), preferred_element_type=F32)


def rotation_tables(seq_length):
    half = DQK // 2
    freqs = jnp.exp(-math.log(THETA) * jnp.arange(half, dtype=F32) / half)
    angles = freqs[:, None] * jnp.arange(seq_length, dtype=jnp.int32).astype(F32)[None, :]
    return jnp.cos(angles), jnp.sin(angles)


def rotate_rows(x, cos, sin):
    half = DQK // 2
    parts = []
    for g in range(x.shape[0] // DQK):
        a = x[g * DQK : g * DQK + half]
        b = x[g * DQK + half : (g + 1) * DQK]
        parts += [a * cos - b * sin, b * cos + a * sin]
    return jnp.concatenate(parts, axis=0)


def attention_kernel(heads, lam_ref, cos_ref, sin_ref, qk_in, vog_ref, back_ref, rows_ref, dv_ref,
                     qk_ref, vt_s, ogt_s, dvt_s, dk_s):
    seq = cos_ref.shape[1]
    qc = qk_ref.shape[0] // 2
    hw = qc // heads
    ve = vog_ref.shape[2] // heads
    qk_ref[...] = qk_in[...].T
    inv_root = 1.0 / math.sqrt(DQK)
    vt_s[...] = vog_ref[0].T
    ogt_s[...] = vog_ref[1].T
    step = 256

    def one_head(h, _):
        lam = lam_ref[lax.axis_index("sp") * heads + h]
        cos, sin = cos_ref[...], sin_ref[...]
        qrow = pl.multiple_of(h * hw, hw)
        vrow = pl.multiple_of(h * ve, ve)
        qt = rotate_rows(qk_ref[pl.ds(qrow, hw), :], cos, sin).astype(BF16)
        kt = rotate_rows(qk_ref[pl.ds(qc + qrow, hw), :], cos, sin).astype(BF16)
        k = kt.T
        vt = vt_s[pl.ds(vrow, ve), :]
        v = vt.T
        zero_half = jnp.zeros((DQK, step), BF16)
        dk_s[...] = jnp.zeros_like(dk_s)
        dvt_s[pl.ds(vrow, ve), :] = jnp.zeros((ve, seq), F32)
        for t0 in range(0, seq, step):
            end = min(t0 + step, seq)
            tb = end - t0
            zh = zero_half[:, :tb]
            q_b = qt[:, t0:end]
            mask = lax.broadcasted_iota(jnp.int32, (tb, tb), 0) <= lax.broadcasted_iota(
                jnp.int32, (tb, tb), 1
            )
            probs = []
            for m in range(2):
                half_q = q_b[m * DQK : (m + 1) * DQK]
                rhs = jnp.concatenate([half_q, zh] if m == 0 else [zh, half_q], axis=0)
                s = dot(k[:end], rhs) * inv_root
                diag = jnp.where(mask, s[t0:], -jnp.inf)
                s = jnp.concatenate([s[:t0], diag], axis=0) if t0 else diag
                e = jnp.exp(s - jnp.max(s, axis=0, keepdims=True))
                probs.append(e * (1.0 / jnp.sum(e, axis=0, keepdims=True)))
            p1, p2 = probs
            mix = (p1 - lam * p2).astype(BF16)
            ho = dot(vt[:, :end], mix)
            inv = lax.rsqrt(jnp.mean(ho * ho, axis=0, keepdims=True) + NORM_EPS)
            og = ogt_s[pl.ds(vrow, ve), t0:end].astype(F32)
            ob = (inv * og - inv * inv * inv * ho * jnp.mean(og * ho, axis=0, keepdims=True)).astype(BF16)
            mg = dot(v[:end], ob) * inv_root
            g1 = (p1 * (mg - jnp.sum(mg * p1, axis=0, keepdims=True))).astype(BF16)
            g2 = ((-lam * p2) * (mg - jnp.sum(mg * p2, axis=0, keepdims=True))).astype(BF16)
            dvt_s[pl.ds(vrow, ve), :end] += dot(ob, mix, 1, 1)
            dq = jnp.concatenate([dot(kt[:DQK, :end], g1), dot(kt[DQK:, :end], g2)], axis=0)
            back_ref[pl.ds(qrow, hw), t0:end] = rotate_rows(dq, cos[:, t0:end], -sin[:, t0:end]).astype(BF16)
            dk_s[:DQK, :end] += dot(q_b[:DQK], g1, 1, 1)
            dk_s[DQK:, :end] += dot(q_b[DQK:], g2, 1, 1)
        back_ref[pl.ds(qc + qrow, hw), :] = rotate_rows(dk_s[...], cos, -sin).astype(BF16)
        return 0

    lax.fori_loop(0, heads, one_head, 0)
    dv_ref[...] = dvt_s[...].T.astype(BF16)
    rows_ref[...] = back_ref[...].T


def attention(qk, vog, lam, cos, sin, heads):
    seq, qk_cols = qk.shape
    vc = vog.shape[2]
    vm = pl.BlockSpec(memory_space=pltpu.VMEM)
    return pl.pallas_call(
        functools.partial(attention_kernel, heads),
        out_shape=(
            jax.ShapeDtypeStruct((qk_cols, seq), BF16),
            jax.ShapeDtypeStruct((seq, qk_cols), BF16),
            jax.ShapeDtypeStruct((seq, vc), BF16),
        ),
        in_specs=[pl.BlockSpec(memory_space=pltpu.SMEM)] + [vm] * 4,
        out_specs=(vm, vm, vm),
        scratch_shapes=[
            pltpu.VMEM((qk_cols, seq), F32),
            pltpu.VMEM((vc, seq), BF16),
            pltpu.VMEM((vc, seq), BF16),
            pltpu.VMEM((vc, seq), F32),
            pltpu.VMEM((qk_cols // heads // 2, seq), F32),
        ],
        compiler_params=pltpu.CompilerParams(vmem_limit_bytes=60 * 1024 * 1024),
        name="attn",
    )(lam, cos, sin, qk, vog)


def sender(src, dst, ssem, rsem, device):
    return pltpu.make_async_remote_copy(
        src_ref=src, dst_ref=dst, send_sem=ssem, recv_sem=rsem,
        device_id=device, device_id_type=pl.DeviceIdType.MESH,
    )


def places(sp, dp):
    me, mine = lax.axis_index("sp"), lax.axis_index("dp")
    z, core = mine // 2, lax.rem(mine, 2)
    nz = dp // 2
    if sp == 4:
        peers = [me + 1 - 2 * lax.rem(me, 2), lax.rem(me + 2, 4), 3 - me]
        froms = peers
    else:
        peers = [lax.rem(me + d, sp) for d in range(1, sp)]
        froms = [lax.rem(me + sp - d, sp) for d in range(1, sp)]
    z_to = [lax.rem(z + i, nz) * 2 for i in range(1, nz)]
    z_from = [lax.rem(z + nz - i, nz) * 2 for i in range(1, nz)]
    return me, mine, z, core, peers, froms, z_to, z_from


def greet(me, mine, core, peers, z_to):
    barrier = pltpu.get_barrier_semaphore()
    where = [(p, mine) for p in peers] + [(me, zt + core) for zt in z_to] + [(me, mine + 1 - 2 * core)]
    for device in where:
        pl.semaphore_signal(barrier, inc=1, device_id=device, device_id_type=pl.DeviceIdType.MESH)
    pl.semaphore_wait(barrier, len(where))


def gather_kernel(sp, dp, tok_ref, v_ref, og_ref, wq_ref, wk_ref, tok_all, vog_all, w_all, qk_ref,
                  vog_ref, tok_ss, tok_rs, vog_ss, vog_rs, w_ss, w_rs, sib_ss, sib_rs):
    me, mine, z, core, peers, froms, z_to, z_from = places(sp, dp)
    rows, wr = tok_ref.shape[0], wq_ref.shape[0]
    sib = (me, mine + 1 - 2 * core)

    def trow(i, start=0, size=rows):
        return pl.ds(pl.multiple_of(i * rows + start, 16), size)

    def wrow(i):
        return pl.ds(pl.multiple_of(i * wr, wr), wr)

    vc, qc = v_ref.shape[1] // sp, wq_ref.shape[1] // sp
    for s in range(sp):
        vog_ref[s, 0] = v_ref[:, s * vc : (s + 1) * vc]
        vog_ref[s, 1] = og_ref[:, s * vc : (s + 1) * vc]

        @pl.when(me == s)
        def _():
            w_all[wrow(mine), :qc] = wq_ref[:, s * qc : (s + 1) * qc]
            w_all[wrow(mine), qc:] = wk_ref[:, s * qc : (s + 1) * qc]

    tok_all[trow(me), :] = tok_ref[...]
    greet(me, mine, core, peers, z_to)
    w_ref = w_all.at[wrow(mine)]
    sends = []

    def go(copy):
        copy.start()
        sends.append(copy)
        return copy

    wz = [go(sender(w_ref, w_all.at[wrow(mine)], w_ss.at[i], w_rs.at[i], (me, zt + core)))
          for i, zt in enumerate(z_to)]
    ws = [go(sender(w_ref, w_all.at[wrow(mine)], sib_ss.at[0], sib_rs.at[0], sib))]
    half = rows // 2
    if sp == 4:
        def piece(p, h, k):
            r = trow(me, h * half, half)
            return go(sender(tok_ref.at[pl.ds(h * half, half)], tok_all.at[r], tok_ss.at[k], tok_rs.at[k], (p, mine)))

        x0, y1 = piece(peers[0], 0, 0), piece(peers[1], 1, 1)
        x1, y0 = piece(peers[0], 1, 2), piece(peers[1], 0, 3)
    else:
        tk = [go(sender(tok_ref, tok_all.at[trow(me)], tok_ss.at[i], tok_rs.at[i], (p, mine)))
              for i, p in enumerate(peers)]
    vg = [go(sender(vog_ref.at[p], vog_all.at[:, trow(me)], vog_ss.at[i], vog_rs.at[i], (p, mine)))
          for i, p in enumerate(peers)]
    vog_all[:, trow(me), :] = vog_ref[me]
    if sp == 4:
        x0.wait_recv()
        f0 = trow(peers[0], 0, half)
        d0 = go(sender(tok_all.at[f0], tok_all.at[f0], tok_ss.at[4], tok_rs.at[4], (peers[1], mine)))
        y1.wait_recv()
        f1 = trow(peers[1], half, half)
        d1 = go(sender(tok_all.at[f1], tok_all.at[f1], tok_ss.at[5], tok_rs.at[5], (peers[0], mine)))
        arrivals = [[x1], [y0], [d0, d1]]
    else:
        arrivals = [[c] for c in tk]
    for i, zf in enumerate(z_from):
        wz[i].wait_recv()
        r = wrow(zf + core)
        ws.append(go(sender(w_all.at[r], w_all.at[r], sib_ss.at[i + 1], sib_rs.at[i + 1], sib)))
    for c in ws:
        c.wait_recv()
    qk_ref[trow(me), :] = dot(tok_ref[...], w_all[...])
    for f, copies in zip(froms, arrivals):
        for c in copies:
            c.wait_recv()
        qk_ref[trow(f), :] = dot(tok_all[trow(f), :], w_all[...])
    for c in vg:
        c.wait_recv()
    for c in sends:
        c.wait_send()


def gather(tok, v, og, wq, wk, sp, dp):
    rows, width = tok.shape
    vc, wr, cols = v.shape[1] // sp, wq.shape[0], 2 * wq.shape[1] // sp
    vm = pl.BlockSpec(memory_space=pltpu.VMEM)
    dma = pltpu.SemaphoreType.DMA
    nt = 6 if sp == 4 else sp - 1
    nz = dp // 2
    return pl.pallas_call(
        functools.partial(gather_kernel, sp, dp),
        out_shape=(
            jax.ShapeDtypeStruct((rows * sp, width), BF16),
            jax.ShapeDtypeStruct((2, rows * sp, vc), BF16),
            jax.ShapeDtypeStruct((wr * dp, cols), BF16),
            jax.ShapeDtypeStruct((rows * sp, cols), F32),
        ),
        in_specs=[vm] * 5,
        out_specs=(vm,) * 4,
        scratch_shapes=[pltpu.VMEM((sp, 2, rows, vc), BF16), dma((nt,)), dma((nt,)), dma((sp - 1,)), dma((sp - 1,)),
                        dma((nz - 1,)), dma((nz - 1,)), dma((nz,)), dma((nz,))],
        compiler_params=pltpu.CompilerParams(
            vmem_limit_bytes=60 * 1024 * 1024, collective_id=0, has_side_effects=True
        ),
        name="gather",
    )(tok, v, og, wq, wk)


def scatter_kernel(sp, dp, back_t, back_m, tok_all, w_all, dv, tg_out, dv_out, qg, kg,
                   tbuf, trecv, tacc, dvr, sib_s, sib_r, wz_s, wz_r, wacc, wg_s, wg_r,
                   t_ss, t_rs, d_ss, d_rs, s_ss, s_rs, z_ss, z_rs, g_ss, g_rs):
    me, mine, z, core, peers, froms, z_to, z_from = places(sp, dp)
    nz = dp // 2
    rows, wr = tg_out.shape[0], qg.shape[0]
    vc = dv.shape[1]
    qc = w_all.shape[1] // 2
    sib = (me, mine + 1 - 2 * core)
    greet(me, mine, core, peers, z_to)
    sends = []

    def go(copy):
        copy.start()
        sends.append(copy)
        return copy

    def trow(i):
        return pl.ds(pl.multiple_of(i * rows, 16), rows)

    def weight_part(owner):
        return dot(back_t[...], tok_all[:, pl.ds(pl.multiple_of(owner * wr, wr), wr)])

    def token_part(p):
        return dot(back_m[trow(p), :], w_all[...], 1, 1)

    def send_tokens(i):
        tbuf[i] = token_part(peers[i]).astype(BF16)
        return go(sender(tbuf.at[i], trecv.at[i], t_ss.at[i], t_rs.at[i], (peers[i], mine)))

    targets = z_to + [z * 2]
    half = rows // 2
    lo, hi = pl.ds(0, half), pl.ds(half, half)
    tg = []

    def hop(i, dst, part, k, to):
        return go(sender(tbuf.at[i, part], trecv.at[dst, part], t_ss.at[k], t_rs.at[k], (peers[to], mine)))

    if sp == 4:
        tbuf[2] = token_part(peers[2]).astype(BF16)
        via_x, via_y = hop(2, 2, lo, 0, 0), hop(2, 2, hi, 1, 1)
    else:
        tg.append(send_tokens(0))
    sb = []
    for i, zt in enumerate(targets):
        sib_s[i] = weight_part(zt + 1 - core).astype(BF16)
        sb.append(go(sender(sib_s.at[i], sib_r.at[i], s_ss.at[i], s_rs.at[i], sib)))
    zs = []
    for i, zt in enumerate(targets):
        part = weight_part(zt + core)
        sb[i].wait_recv()
        part = part + sib_r[i].astype(F32)
        if i < nz - 1:
            wz_s[i] = part.astype(BF16)
            zs.append(go(sender(wz_s.at[i], wz_r.at[i], z_ss.at[i], z_rs.at[i], (me, zt + core))))
        else:
            wacc[...] = part
    if sp == 4:
        part = token_part(peers[0])
        tbuf[0, lo] = part[:half].astype(BF16)
        x_lo = hop(0, 0, lo, 2, 0)
        tacc[hi] = part[half:]
        part = token_part(peers[1])
        tbuf[1, hi] = part[half:].astype(BF16)
        y_hi = hop(1, 1, hi, 3, 1)
        tacc[lo] = part[:half]
        via_x.wait_recv()
        tbuf[1, lo] = (tacc[lo] + trecv[2, lo].astype(F32)).astype(BF16)
        y_lo = hop(1, 1, lo, 4, 1)
        via_y.wait_recv()
        tbuf[0, hi] = (tacc[hi] + trecv[2, hi].astype(F32)).astype(BF16)
        x_hi = hop(0, 0, hi, 5, 0)
        tg = [x_lo, x_hi, y_lo, y_hi]
    else:
        for i in range(1, sp - 1):
            tg.append(send_tokens(i))
    dvc = [go(sender(dv.at[trow(p)], dvr.at[me], d_ss.at[i], d_rs.at[i], (p, mine)))
           for i, p in enumerate(peers)]
    dvr[me] = dv[trow(me), :]
    tacc[...] = token_part(me)
    for i in range(nz - 1):
        zs[i].wait_recv()
        wacc[...] += wz_r[i].astype(F32)
    total = wacc[...].T.astype(BF16)
    wg_s[...] = total
    wg_r[me] = total
    wh = wr // 2
    if sp == 4:
        def piece(p, h, k):
            r = pl.ds(h * wh, wh)
            return go(sender(wg_s.at[r], wg_r.at[me, r], g_ss.at[k], g_rs.at[k], (p, mine)))

        def forward(f, h, k, p):
            r = pl.ds(h * wh, wh)
            return go(sender(wg_r.at[f, r], wg_r.at[f, r], g_ss.at[k], g_rs.at[k], (p, mine)))

        gx0, gy1 = piece(peers[0], 0, 0), piece(peers[1], 1, 1)
        gx1, gy0 = piece(peers[0], 1, 2), piece(peers[1], 0, 3)
        gx0.wait_recv()
        gd0 = forward(peers[0], 0, 4, peers[1])
        gy1.wait_recv()
        gd1 = forward(peers[1], 1, 5, peers[0])
        gs = [gx1, gy0, gd0, gd1]
    else:
        gs = [go(sender(wg_s, wg_r.at[me], g_ss.at[i], g_rs.at[i], (p, mine))) for i, p in enumerate(peers)]
    for c in tg:
        c.wait_recv()
    for i in range(2 if sp == 4 else sp - 1):
        tacc[...] += trecv[i].astype(F32)
    tg_out[...] = tacc[...].astype(BF16)
    for c in dvc:
        c.wait_recv()
    for s in range(sp):
        dv_out[:, s * vc : (s + 1) * vc] = dvr[s]
    for c in gs:
        c.wait_recv()
    for s in range(sp):
        qg[:, s * qc : (s + 1) * qc] = wg_r[s, :, :qc]
        kg[:, s * qc : (s + 1) * qc] = wg_r[s, :, qc:]
    for c in sends:
        c.wait_send()


def scatter(back_t, back_m, tok_all, w_all, dv, sp, dp):
    seq, width = tok_all.shape
    rows, wr = seq // sp, width // dp
    cols = w_all.shape[1]
    vc = dv.shape[1]
    nz = dp // 2
    vm = pl.BlockSpec(memory_space=pltpu.VMEM)
    dma = pltpu.SemaphoreType.DMA
    nt = 6 if sp == 4 else sp - 1
    return pl.pallas_call(
        functools.partial(scatter_kernel, sp, dp),
        out_shape=(
            jax.ShapeDtypeStruct((rows, width), BF16),
            jax.ShapeDtypeStruct((rows, vc * sp), BF16),
            jax.ShapeDtypeStruct((wr, cols // 2 * sp), BF16),
            jax.ShapeDtypeStruct((wr, cols // 2 * sp), BF16),
        ),
        in_specs=[vm] * 5,
        out_specs=(vm,) * 4,
        scratch_shapes=[
            pltpu.VMEM((sp - 1, rows, width), BF16),
            pltpu.VMEM((sp - 1, rows, width), BF16),
            pltpu.VMEM((rows, width), F32),
            pltpu.VMEM((sp, rows, vc), BF16),
            pltpu.VMEM((nz, cols, wr), BF16),
            pltpu.VMEM((nz, cols, wr), BF16),
            pltpu.VMEM((nz - 1, cols, wr), BF16),
            pltpu.VMEM((nz - 1, cols, wr), BF16),
            pltpu.VMEM((cols, wr), F32),
            pltpu.VMEM((wr, cols), BF16),
            pltpu.VMEM((sp, wr, cols), BF16),
            dma((nt,)), dma((nt,)), dma((sp - 1,)), dma((sp - 1,)), dma((nz,)), dma((nz,)),
            dma((nz - 1,)), dma((nz - 1,)), dma((nt,)), dma((nt,)),
        ],
        compiler_params=pltpu.CompilerParams(
            vmem_limit_bytes=62 * 1024 * 1024, collective_id=1, has_side_effects=True
        ),
        name="scatter",
    )(back_t, back_m, tok_all, w_all, dv)


def position_tables(seq_length):
    half = DQK // 2
    freqs = np.exp(np.float32(-math.log(THETA)) * np.arange(half, dtype=np.float32) / np.float32(half)).astype(np.float32)
    angles = freqs[:, None] * np.arange(seq_length, dtype=np.float32)[None, :]
    wide = angles.astype(np.float64)
    return jnp.asarray(np.concatenate([np.cos(wide), np.sin(wide)]).astype(np.float32))


def head_scores(hh, cos, sin, q, k_in, qt_s, kt_s, p_s, lam):
    seq = cos.shape[1]
    scale = math.log2(math.e) / math.sqrt(DQK)
    step = 256
    zero_half = jnp.zeros((DQK, step), BF16)
    qt = rotate_rows(q, cos, sin).astype(BF16)
    kt = rotate_rows(k_in, cos, sin).astype(BF16)
    qt_s[hh] = qt
    kt_s[hh] = kt
    k = kt.T
    for t0 in range(0, seq, step):
        end = min(t0 + step, seq)
        tb = end - t0
        zh = zero_half[:, :tb]
        q_b = qt[:, t0:end]
        mask = lax.broadcasted_iota(jnp.int32, (tb, tb), 0) <= lax.broadcasted_iota(jnp.int32, (tb, tb), 1)
        for m in range(2):
            half_q = q_b[m * DQK : (m + 1) * DQK]
            rhs = jnp.concatenate([half_q, zh] if m == 0 else [zh, half_q], axis=0)
            s = dot(k[:end], rhs)
            diag = jnp.where(mask, s[t0:], -jnp.inf)
            s = jnp.concatenate([s[:t0], diag], axis=0) if t0 else diag
            e = jnp.exp2((s - jnp.max(s, axis=0, keepdims=True)) * scale)
            r = 1.0 / jnp.sum(e, axis=0, keepdims=True)
            p_s[hh, m, :end, t0:end] = e * (r if m == 0 else r * -lam)


def head_back(hh, h, cos, sin, lam, qt_s, kt_s, p_s, vt_s, ogt_s, dvt_s, dk_s, bt_s):
    seq = cos.shape[1]
    hw = 2 * DQK
    ve = vt_s.shape[0] // 2
    inv_root = 1.0 / math.sqrt(DQK)
    step = 256
    rows = slice(hh * hw, (hh + 1) * hw)
    vr = slice(hh * ve, (hh + 1) * ve)
    qt, kt = qt_s[h], kt_s[h]
    vt = vt_s[vr, :]
    v = vt.T
    cb, sb = cos * inv_root, sin * -inv_root
    for t0 in range(0, seq, step):
        end = min(t0 + step, seq)
        q_b = qt[:, t0:end]
        p1, p2 = p_s[h, 0, :end, t0:end], p_s[h, 1, :end, t0:end]
        mix = (p1 + p2).astype(BF16)
        ho = dot(vt[:, :end], mix)
        inv = lax.rsqrt(jnp.mean(ho * ho, axis=0, keepdims=True) + NORM_EPS)
        og = ogt_s[vr, t0:end].astype(F32)
        ob = (inv * og - inv * inv * inv * ho * jnp.mean(og * ho, axis=0, keepdims=True)).astype(BF16)
        mg = dot(v[:end], ob)
        g1 = (p1 * (mg - jnp.sum(mg * p1, axis=0, keepdims=True))).astype(BF16)
        g2 = (p2 * (mg + jnp.sum(mg * p2, axis=0, keepdims=True) * (1.0 / lam))).astype(BF16)
        dvd = dot(ob, mix, 1, 1)
        dkd = jnp.concatenate([dot(q_b[:DQK], g1, 1, 1), dot(q_b[DQK:], g2, 1, 1)], axis=0)
        if t0:
            dvd = jnp.concatenate([dvt_s[vr, :t0] + dvd[:, :t0], dvd[:, t0:]], axis=1)
            dkd = jnp.concatenate([dk_s[rows, :t0] + dkd[:, :t0], dkd[:, t0:]], axis=1)
        dvt_s[vr, :end] = dvd
        dk_s[rows, :end] = dkd
        dq = jnp.concatenate([dot(kt[:DQK, :end], g1), dot(kt[DQK:, :end], g2)], axis=0)
        bt_s[rows, t0:end] = rotate_rows(dq, cb[:, t0:end], sb[:, t0:end]).astype(BF16)
    bt_s[2 * hw + hh * hw : 2 * hw + (hh + 1) * hw, :] = rotate_rows(dk_s[rows, :], cb, sb).astype(BF16)


def fused_kernel(sp, dp, pairs, lam_in, rot_in, tok_in, v_in, og_in, wq_in, wk_in,
                 tg_out, dvr, wg_r,
                 lam_ref, rot_ref, tok_all, w1, w2, qk_s, vog_src, vog_all, qt_s, kt_s, p_s,
                 vt_s, ogt_s, dvt_s, dk_s, bt_s, back_m, back_x,
                 dv_s, sib_s, sib_r, own_s, wz_s, wz_r, wz_m, tbuf, trecv, tacc,
                 l_s, tok_ss, tok_rs, vog_ss, vog_rs, z_ss, z_rs, s_ss, s_rs, bx_ss, bx_rs, dv_ss, dv_rs,
                 c_ss, c_rs, g_ss, g_rs, m_rs, ag_ss, ag_rs, ty_ss, ty_rs):
    me, mine, z, core, peers, froms, z_to, z_from = places(sp, dp)
    nz = dp // 2
    rows, wr = tok_in.shape[0], wq_in.shape[0]
    half = rows // 2
    pw = 128
    sib = (me, mine + 1 - 2 * core)
    xp, yp = (peers[0], mine), (peers[1], mine)

    def trow(i, start=0, size=rows):
        return pl.ds(pl.multiple_of(i * rows + start, 16), size)

    def wrow(zz, c):
        return pl.ds(pl.multiple_of((c * nz + zz) * wr, wr), wr)

    def lanes(i, size):
        return pl.ds(pl.multiple_of(i * size, size), size)

    sends = []

    def go(copy, cond=None):
        if cond is None:
            copy.start()
        else:
            pl.when(cond)(copy.start)
        sends.append((copy, cond))
        return copy

    barrier = pltpu.get_barrier_semaphore()
    where = [(p, mine) for p in peers] + [(me, zt + core) for zt in z_to] + [sib]
    for device in where:
        pl.semaphore_signal(barrier, inc=1, device_id=device, device_id_type=pl.DeviceIdType.MESH)

    count = [0]

    def load(src, dst):
        c = pltpu.make_async_copy(src, dst, l_s.at[count[0]])
        count[0] += 1
        c.start()
        return c

    def load_weights(w, who):
        out = []
        for j in range(pairs):
            src = lanes(who * pairs + j, pw)
            out.append(load(wq_in.at[:, src], w.at[wrow(z, core), 2 * j * pw : (2 * j + 1) * pw]))
            out.append(load(wk_in.at[:, src], w.at[wrow(z, core), (2 * j + 1) * pw : (2 * j + 2) * pw]))
        return out

    l_tok = []
    for c in range(2):
        for zz in range(nz):
            n = slice((c * nz + zz) * wr, (c * nz + zz + 1) * wr)
            l_tok.append(load(tok_in.at[:, (2 * zz + c) * wr : (2 * zz + c + 1) * wr], tok_all.at[trow(me), n]))
    l_w1 = load_weights(w1, me)
    l_vog = []
    for j in range(pairs):
        for n, src in enumerate((v_in, og_in)):
            for i, p in enumerate(peers):
                l_vog.append(load(src.at[:, lanes(p * pairs + j, pw)], vog_src.at[i, j, n]))
            l_vog.append(load(src.at[:, lanes(me * pairs + j, pw)], vog_all.at[j, n, trow(me)]))
    l_w2 = load_weights(w2, jnp.where(core == 0, peers[0], peers[1]))
    l_rot = [load(rot_in, rot_ref), load(lam_in, lam_ref)]

    far = lax.rem(z + 2, nz)
    order = [far, z + 1 - 2 * lax.rem(z, 2), nz - 1 - z]
    inner = jnp.logical_and(z > 0, z < nz - 1)
    outer = jnp.logical_not(inner)

    def z_copy(w, k, n, src, to):
        r = w.at[wrow(src, core)]
        return sender(r, r, z_ss.at[k, n], z_rs.at[k, src], (me, 2 * to + core))

    def s_copy(w, k, src):
        r = w.at[wrow(src, core)]
        return sender(r, r, s_ss.at[k, src], s_rs.at[k, src], sib)

    def z_start():
        go(z_copy(w1, 0, 0, z, far))
        go(z_copy(w1, 0, 1, z, order[1]))
        go(z_copy(w1, 0, 2, z, order[2]), inner)
        go(s_copy(w1, 0, z))

    def z_step(i):
        z_copy(w1, 0, 0, order[i], z).wait_recv()
        go(s_copy(w1, 0, order[i]))
        if i == 0:
            go(z_copy(w1, 0, 3, far, order[1]), inner)

    aside = (1 - z // 2) * (nz - 1)
    near = [order[1], jnp.where(inner, order[2], far)]

    def other_start():
        go(z_copy(w2, 1, 0, z, far), inner)
        go(z_copy(w2, 1, 1, z, order[1]))
        go(z_copy(w2, 1, 2, z, order[2]), inner)
        go(s_copy(w2, 1, z))

    def other_aside():
        r = wrow(aside, core)
        to = (jnp.where(core == 0, peers[0], peers[1]), mine)
        return sender(w1.at[r], w2.at[r], z_ss.at[1, 3], z_rs.at[1, aside], to)

    def other_step(src):
        z_copy(w2, 1, 0, src, z).wait_recv()
        go(s_copy(w2, 1, src))

    def z_sib(w, k):
        for src in [z] + order:
            r = w.at[wrow(src, 1 - core)]
            sender(r, r, s_ss.at[k, 0], s_rs.at[k, src], sib).wait_recv()

    def piece(p, h, k):
        r = trow(me, h * half, half)
        return go(sender(tok_all.at[r], tok_all.at[r], tok_ss.at[k], tok_rs.at[k], p))

    for c in l_tok:
        c.wait()
    pl.semaphore_wait(barrier, len(where))
    x0, y1 = piece(xp, 0, 0), piece(yp, 1, 1)
    x1, y0 = piece(xp, 1, 2), piece(yp, 0, 3)
    for c in l_w1:
        c.wait()
    z_start()
    for c in l_w2 + l_vog + l_rot:
        c.wait()
    x0.wait_recv()
    f0 = trow(peers[0], 0, half)
    d0 = go(sender(tok_all.at[f0], tok_all.at[f0], tok_ss.at[4], tok_rs.at[4], yp))
    y1.wait_recv()
    f1 = trow(peers[1], half, half)
    d1 = go(sender(tok_all.at[f1], tok_all.at[f1], tok_ss.at[5], tok_rs.at[5], xp))

    def vog_start(j):
        for i in range(sp - 1):
            dst = vog_all.at[j, :, trow(me)]
            go(sender(vog_src.at[i, j], dst, vog_ss.at[j, i], vog_rs.at[j, i], (peers[i], mine)))

    vog_start(0)
    z_step(0)
    other_start()
    z_step(1)
    z_step(2)
    z_sib(w1, 0)
    qk_s[trow(me), :] = dot(tok_all[trow(me), :], w1[...])
    for f, copies in zip(froms, [[x1], [y0], [d0, d1]]):
        for c in copies:
            c.wait_recv()
        qk_s[trow(f), :] = dot(tok_all[trow(f), :], w1[...])

    n16 = DQK // 2
    cos, sin = rot_ref[:n16, :], rot_ref[n16:, :]
    hw = 2 * DQK

    lams = [lam_ref[me * pairs * 2 + h] for h in range(2 * pairs)]
    def scores(j):
        qk = [qk_s[:, (2 * j + n) * pw : (2 * j + n + 1) * pw].T for n in range(2)]
        for hh in range(2):
            r = slice(hh * hw, (hh + 1) * hw)
            h = 2 * j + hh
            head_scores(h, cos, sin, qk[0][r], qk[1][r], qt_s, kt_s, p_s, lams[h])

    def values_start(j):
        for i, p in enumerate(peers):
            go(sender(dv_s.at[j, trow(p)], dvr.at[me, j], dv_ss.at[j, i], dv_rs.at[j, i], (p, mine)))
        dvr[me, j] = dv_s[j, trow(me), :]

    def one_pair(j):
        for i, p in enumerate(peers):
            r = vog_all.at[j, :, trow(p)]
            sender(vog_src.at[i, j], r, vog_ss.at[j, i], vog_rs.at[j, i], (p, mine)).wait_recv()
        if j == 0:
            go(other_aside())
        vt_s[...] = vog_all[j, 0].T
        ogt_s[...] = vog_all[j, 1].T
        for hh in range(2):
            head_back(hh, 2 * j + hh, cos, sin, lams[2 * j + hh], qt_s, kt_s, p_s, vt_s, ogt_s, dvt_s, dk_s, bt_s)
        back_m[j] = bt_s[...].T
        for a, to in enumerate((0, 1)):
            for b, p in enumerate((peers[to], peers[2])):
                go(sender(back_m.at[j, trow(p)], back_x.at[a, j, b], bx_ss.at[a, j, b], bx_rs.at[a, j, b], (xp, yp)[to]))

        def weight_part(c):
            return dot(bt_s[...], tok_all[:, lanes(c, nz * wr)])

        part = weight_part(1 - core)
        for zz in range(nz):
            sib_s[j, zz] = part[:, zz * wr : (zz + 1) * wr].astype(BF16)
        for zz in range(nz):
            go(sender(sib_s.at[j, zz], sib_r.at[j, zz], c_ss.at[j, zz], c_rs.at[j, zz], sib))
        part = weight_part(core)
        for zz in range(nz):
            own_s[j, zz] = part[:, zz * wr : (zz + 1) * wr]
        dv_s[j] = dvt_s[...].T.astype(BF16)
        values_start(j)
        if j:
            merge(j - 1)
        for i in range(nz):
            sender(sib_s.at[j, i], sib_r.at[j, i], c_ss.at[j, i], c_rs.at[j, i], sib).wait_recv()
            own_s[j, i] = own_s[j, i] + sib_r[j, i].astype(F32)
        for i in range(nz - 1):
            wz_s[j, i] = own_s[j, order[i]].astype(BF16)
        go(sender(wz_s.at[j, 2], wz_m.at[j], g_ss.at[j, 2], m_rs.at[j], (me, 2 * order[1] + core)), outer)
        go(z_share(j, 0), outer)
        go(z_share(j, 2), inner)
        go(z_share(j, 1))

    def z_share(j, i):
        return sender(wz_s.at[j, i], wz_r.at[j, i], g_ss.at[j, i], g_rs.at[j, i], (me, 2 * order[i] + core))

    def merge(j):
        c = z_share(j, 0)

        @pl.when(inner)
        def _():
            sender(wz_m.at[j], wz_m.at[j], g_ss.at[j, 0], m_rs.at[j], sib).wait_recv()
            wz_s[j, 0] = (own_s[j, far] + wz_m[j].astype(F32)).astype(BF16)
            c.start()

        sends.append((c, inner))

    for j in range(pairs):
        scores(j)
        if j == 0:
            for jj in range(1, pairs):
                vog_start(jj)
        one_pair(j)
        if j == 0:
            other_step(near[0])

    def back_wait(a, j, b):
        r = back_x.at[a, j, b]
        sender(r, r, bx_ss.at[a, j, b], bx_rs.at[a, j, b], sib).wait_recv()

    def token_part(who, a, b, parts):
        n = slice(a * nz * wr, (a + 1) * nz * wr)
        out = None
        for j, own in parts:
            k = slice(2 * j * pw, (2 * j + 2) * pw)
            part = dot(back_m[j, trow(who), :], w1[n, k], 1, 1) if own else dot(back_x[a, j, b], w2[n, k], 1, 1)
            out = part if out is None else out + part
        return out

    early = [(j, True) for j in range(pairs)] + [(j, False) for j in range(pairs - 1)]
    late = [(pairs - 1, False)]
    other_step(near[1])
    other_step(aside)
    z_sib(w2, 1)
    for a in range(2):
        for b in range(2):
            for j in range(pairs - 1):
                back_wait(a, j, b)
    for a in range(2):
        tacc[a] = token_part(peers[1 - a], a, 1, early)
    ty = {}
    for a in range(2):
        back_wait(a, pairs - 1, 1)
        tbuf[a] = (tacc[a] + token_part(peers[1 - a], a, 1, late)).astype(BF16)
        for h in range(2):
            r = pl.ds(h * half, half)
            ty[a, h] = go(sender(tbuf.at[a, r], trecv.at[a, r], ty_ss.at[a, h], ty_rs.at[a, h], (yp, xp)[a]))

    def weights_end(j):
        @pl.when(inner)
        def _():
            z_share(j, 2).wait_recv()
            own_s[j, z] = own_s[j, z] + wz_r[j, 2].astype(F32)

        z_share(j, 0).wait_recv()
        z_share(j, 1).wait_recv()
        total = own_s[j, z] + wz_r[j, 0].astype(F32) + wz_r[j, 1].astype(F32)
        wg_r[me, j] = total.T.astype(BF16)
        for h, k, to in ((0, 0, xp), (1, 1, yp), (1, 2, xp), (0, 3, yp)):
            go(ag(me, j, h, k, to))

    wh = wr // 2

    def ag(owner, j, h, k, to):
        r = wg_r.at[owner, j, pl.ds(h * wh, wh)]
        return sender(r, r, ag_ss.at[j, k], ag_rs.at[j, k], to)

    def weights_relay(j):
        ag(peers[0], j, 0, 0, xp).wait_recv()
        go(ag(peers[0], j, 0, 4, yp))
        ag(peers[1], j, 1, 1, yp).wait_recv()
        go(ag(peers[1], j, 1, 5, xp))

    merge(pairs - 1)
    weights_end(0)
    for a in range(2):
        back_wait(a, pairs - 1, 0)
    for a in range(2):
        tacc[a] = token_part(me, a, 0, early + late)
    for j in range(1, pairs):
        weights_end(j)
    for h in range(2):
        for a in range(2):
            ty[a, h].wait_recv()
            r = slice(h * half, (h + 1) * half)
            total = (tacc[a, r] + trecv[a, r].astype(F32)).astype(BF16)
            for zz in range(nz):
                tg_out[r, (2 * zz + a) * wr : (2 * zz + a + 1) * wr] = total[:, zz * wr : (zz + 1) * wr]
    for j in range(pairs):
        weights_relay(j)
    for j in range(pairs):
        for i, p in enumerate(peers):
            r = dvr.at[p, j]
            sender(r, r, dv_ss.at[j, i], dv_rs.at[j, i], xp).wait_recv()
        for owner, h, k in ((peers[0], 1, 2), (peers[1], 0, 3), (peers[2], 0, 4), (peers[2], 1, 5)):
            ag(owner, j, h, k, xp).wait_recv()
    for c, cond in sends:
        if cond is None:
            c.wait_send()
        else:
            pl.when(cond)(c.wait_send)


def finish_kernel(factor, tg, dvr, wg, tg_out, dv_out, qg_out, kg_out, dv_s, qg, kg, sem):
    sp, pairs, wr, cols = wg.shape
    pw = cols // 2
    copies = [pltpu.make_async_copy(tg, tg_out, sem.at[0])]
    copies[0].start()
    for s in range(sp):
        for j in range(pairs):
            n = slice((s * pairs + j) * pw, (s * pairs + j + 1) * pw)
            qg[:, n] = wg[s, j, :, :pw].astype(F32) * factor
    copies.append(pltpu.make_async_copy(qg, qg_out, sem.at[1]))
    copies[1].start()
    for s in range(sp):
        for j in range(pairs):
            n = slice((s * pairs + j) * pw, (s * pairs + j + 1) * pw)
            kg[:, n] = wg[s, j, :, pw:].astype(F32) * factor
    copies.append(pltpu.make_async_copy(kg, kg_out, sem.at[2]))
    copies[2].start()
    for s in range(sp):
        for j in range(pairs):
            n = slice((s * pairs + j) * pw, (s * pairs + j + 1) * pw)
            dv_s[:, n] = dvr[s, j]
    copies.append(pltpu.make_async_copy(dv_s, dv_out, sem.at[3]))
    copies[3].start()
    for c in copies:
        c.wait()


def fused(tok, v, og, wq, wk, lam, rot, sp, dp):
    rows, width = tok.shape
    seq = rows * sp
    wr = wq.shape[0]
    nz = dp // 2
    pw = 128
    pairs = v.shape[1] // (sp * pw)
    factor = 1.0 / math.sqrt(dp * seq)
    vm = pl.BlockSpec(memory_space=pltpu.VMEM)
    anywhere = pl.BlockSpec(memory_space=pl.ANY)
    dma = pltpu.SemaphoreType.DMA
    V = pltpu.VMEM
    tg, dvr, wg = pl.pallas_call(
        functools.partial(fused_kernel, sp, dp, pairs),
        out_shape=(
            V((rows, width), BF16),
            V((sp, pairs, rows, pw), BF16),
            V((sp, pairs, wr, 2 * pw), BF16),
        ),
        in_specs=[anywhere] * 7,
        out_specs=(vm,) * 3,
        scratch_shapes=[
            pltpu.SMEM(lam.shape, F32), V(rot.shape, F32),
            V((seq, width), BF16), V((width, 2 * pairs * pw), BF16), V((width, 2 * pairs * pw), BF16),
            V((seq, 2 * pairs * pw), F32), V((sp - 1, pairs, 2, rows, pw), BF16), V((pairs, 2, seq, pw), BF16),
            V((2 * pairs, 2 * DQK, seq), BF16), V((2 * pairs, 2 * DQK, seq), BF16), V((2 * pairs, 2, seq, seq), F32),
            V((pw, seq), BF16), V((pw, seq), BF16), V((pw, seq), F32), V((pw, seq), F32), V((2 * pw, seq), BF16),
            V((pairs, seq, 2 * pw), BF16), V((2, pairs, 2, rows, 2 * pw), BF16),
            V((pairs, seq, pw), BF16),
            V((pairs, nz, 2 * pw, wr), BF16), V((pairs, nz, 2 * pw, wr), BF16), V((pairs, nz, 2 * pw, wr), F32),
            V((pairs, nz - 1, 2 * pw, wr), BF16), V((pairs, nz - 1, 2 * pw, wr), BF16), V((pairs, 2 * pw, wr), BF16),
            V((2, rows, nz * wr), BF16), V((2, rows, nz * wr), BF16), V((2, rows, nz * wr), F32),
            dma((2 + dp + 8 * pairs + 2 * sp * pairs,)),
            dma((6,)), dma((6,)), dma((pairs, sp - 1)), dma((pairs, sp - 1)),
            dma((2, 4)), dma((2, nz)), dma((2, nz)), dma((2, nz)),
            dma((2, pairs, 2)), dma((2, pairs, 2)), dma((pairs, sp - 1)), dma((pairs, sp - 1)),
            dma((pairs, nz)), dma((pairs, nz)), dma((pairs, nz - 1)), dma((pairs, nz - 1)), dma((pairs,)),
            dma((pairs, 6)), dma((pairs, 6)), dma((2, 2)), dma((2, 2)),
        ],
        compiler_params=pltpu.CompilerParams(
            vmem_limit_bytes=56 * 1024 * 1024, collective_id=2, has_side_effects=True
        ),
        name="fused",
    )(lam, rot, tok, v, og, wq, wk)
    return pl.pallas_call(
        functools.partial(finish_kernel, factor),
        out_shape=(
            jax.ShapeDtypeStruct((rows, width), BF16),
            jax.ShapeDtypeStruct((rows, v.shape[1]), BF16),
            jax.ShapeDtypeStruct((wr, wq.shape[1]), F32),
            jax.ShapeDtypeStruct((wr, wq.shape[1]), F32),
        ),
        in_specs=[vm] * 3,
        out_specs=(anywhere,) * 4,
        scratch_shapes=[V((rows, v.shape[1]), BF16), V((wr, wq.shape[1]), F32), V((wr, wq.shape[1]), F32), dma((4,))],
        compiler_params=pltpu.CompilerParams(vmem_limit_bytes=16 * 1024 * 1024),
        name="finish",
    )(tg, dvr, wg)


def body(tokens, query_weight, key_weight, values, lambdas, out_grad):
    sp = lax.axis_size("sp")
    dp = lax.axis_size("dp")
    rows = tokens.shape[1]
    heads = lambdas.shape[0] // sp
    head_vec = values.shape[2] // lambdas.shape[0]
    if sp == 4 and dp == 8 and heads % 2 == 0 and head_vec == 64 and rows * sp <= 640:
        tg, dv, qg, kg = fused(
            tokens[0], values[0], out_grad[0], query_weight, key_weight, lambdas,
            position_tables(rows * sp), sp, dp,
        )
        return tg[None], dv[None], qg, kg
    cos, sin = rotation_tables(rows * sp)
    tok_all, vog_all, w_all, qk = gather(
        tokens[0], values[0], out_grad[0], query_weight, key_weight, sp, dp
    )
    back_t, back_m, dv = attention(qk, vog_all, lambdas, cos, sin, heads)
    tokens_grad, values_grad, qg, kg = scatter(back_t, back_m, tok_all, w_all, dv, sp, dp)
    factor = 1.0 / math.sqrt(dp * rows * sp)
    return tokens_grad[None], values_grad[None], qg.astype(F32) * factor, kg.astype(F32) * factor


def solution(mesh):
    x = P("dp", "sp", None)
    w = P("dp", None)
    return jax.shard_map(
        body, mesh=mesh, in_specs=(x, w, w, x, P(), x), out_specs=(x, x, w, w), check_vma=False
    )
```

```python
import functools
import math

import jax
import jax.numpy as jnp
import numpy as np
from jax import lax
from jax.experimental import pallas as pl
from jax.experimental.pallas import tpu as pltpu
from jax.sharding import PartitionSpec as P

DQK = 32
NORM_EPS = 0.1
THETA = 10000.0
F32 = jnp.float32
BF16 = jnp.bfloat16


def dot(a, b, ca=1, cb=0):
    return lax.dot_general(a, b, (((ca,), (cb,)), ((), ())), preferred_element_type=F32)


def rotation_tables(seq_length):
    half = DQK // 2
    freqs = jnp.exp(-math.log(THETA) * jnp.arange(half, dtype=F32) / half)
    angles = freqs[:, None] * jnp.arange(seq_length, dtype=jnp.int32).astype(F32)[None, :]
    return jnp.cos(angles), jnp.sin(angles)


def rotate_rows(x, cos, sin):
    half = DQK // 2
    parts = []
    for g in range(x.shape[0] // DQK):
        a = x[g * DQK : g * DQK + half]
        b = x[g * DQK + half : (g + 1) * DQK]
        parts += [a * cos - b * sin, b * cos + a * sin]
    return jnp.concatenate(parts, axis=0)


def attention_kernel(heads, lam_ref, cos_ref, sin_ref, qk_in, vog_ref, back_ref, rows_ref, dv_ref,
                     qk_ref, vt_s, ogt_s, dvt_s, dk_s):
    seq = cos_ref.shape[1]
    qc = qk_ref.shape[0] // 2
    hw = qc // heads
    ve = vog_ref.shape[2] // heads
    qk_ref[...] = qk_in[...].T
    inv_root = 1.0 / math.sqrt(DQK)
    vt_s[...] = vog_ref[0].T
    ogt_s[...] = vog_ref[1].T
    step = 256

    def one_head(h, _):
        lam = lam_ref[lax.axis_index("sp") * heads + h]
        cos, sin = cos_ref[...], sin_ref[...]
        qrow = pl.multiple_of(h * hw, hw)
        vrow = pl.multiple_of(h * ve, ve)
        qt = rotate_rows(qk_ref[pl.ds(qrow, hw), :], cos, sin).astype(BF16)
        kt = rotate_rows(qk_ref[pl.ds(qc + qrow, hw), :], cos, sin).astype(BF16)
        k = kt.T
        vt = vt_s[pl.ds(vrow, ve), :]
        v = vt.T
        zero_half = jnp.zeros((DQK, step), BF16)
        dk_s[...] = jnp.zeros_like(dk_s)
        dvt_s[pl.ds(vrow, ve), :] = jnp.zeros((ve, seq), F32)
        for t0 in range(0, seq, step):
            end = min(t0 + step, seq)
            tb = end - t0
            zh = zero_half[:, :tb]
            q_b = qt[:, t0:end]
            mask = lax.broadcasted_iota(jnp.int32, (tb, tb), 0) <= lax.broadcasted_iota(
                jnp.int32, (tb, tb), 1
            )
            probs = []
            for m in range(2):
                half_q = q_b[m * DQK : (m + 1) * DQK]
                rhs = jnp.concatenate([half_q, zh] if m == 0 else [zh, half_q], axis=0)
                s = dot(k[:end], rhs) * inv_root
                diag = jnp.where(mask, s[t0:], -jnp.inf)
                s = jnp.concatenate([s[:t0], diag], axis=0) if t0 else diag
                e = jnp.exp(s - jnp.max(s, axis=0, keepdims=True))
                probs.append(e * (1.0 / jnp.sum(e, axis=0, keepdims=True)))
            p1, p2 = probs
            mix = (p1 - lam * p2).astype(BF16)
            ho = dot(vt[:, :end], mix)
            inv = lax.rsqrt(jnp.mean(ho * ho, axis=0, keepdims=True) + NORM_EPS)
            og = ogt_s[pl.ds(vrow, ve), t0:end].astype(F32)
            ob = (inv * og - inv * inv * inv * ho * jnp.mean(og * ho, axis=0, keepdims=True)).astype(BF16)
            mg = dot(v[:end], ob) * inv_root
            g1 = (p1 * (mg - jnp.sum(mg * p1, axis=0, keepdims=True))).astype(BF16)
            g2 = ((-lam * p2) * (mg - jnp.sum(mg * p2, axis=0, keepdims=True))).astype(BF16)
            dvt_s[pl.ds(vrow, ve), :end] += dot(ob, mix, 1, 1)
            dq = jnp.concatenate([dot(kt[:DQK, :end], g1), dot(kt[DQK:, :end], g2)], axis=0)
            back_ref[pl.ds(qrow, hw), t0:end] = rotate_rows(dq, cos[:, t0:end], -sin[:, t0:end]).astype(BF16)
            dk_s[:DQK, :end] += dot(q_b[:DQK], g1, 1, 1)
            dk_s[DQK:, :end] += dot(q_b[DQK:], g2, 1, 1)
        back_ref[pl.ds(qc + qrow, hw), :] = rotate_rows(dk_s[...], cos, -sin).astype(BF16)
        return 0

    lax.fori_loop(0, heads, one_head, 0)
    dv_ref[...] = dvt_s[...].T.astype(BF16)
    rows_ref[...] = back_ref[...].T


def attention(qk, vog, lam, cos, sin, heads):
    seq, qk_cols = qk.shape
    vc = vog.shape[2]
    vm = pl.BlockSpec(memory_space=pltpu.VMEM)
    return pl.pallas_call(
        functools.partial(attention_kernel, heads),
        out_shape=(
            jax.ShapeDtypeStruct((qk_cols, seq), BF16),
            jax.ShapeDtypeStruct((seq, qk_cols), BF16),
            jax.ShapeDtypeStruct((seq, vc), BF16),
        ),
        in_specs=[pl.BlockSpec(memory_space=pltpu.SMEM)] + [vm] * 4,
        out_specs=(vm, vm, vm),
        scratch_shapes=[
            pltpu.VMEM((qk_cols, seq), F32),
            pltpu.VMEM((vc, seq), BF16),
            pltpu.VMEM((vc, seq), BF16),
            pltpu.VMEM((vc, seq), F32),
            pltpu.VMEM((qk_cols // heads // 2, seq), F32),
        ],
        compiler_params=pltpu.CompilerParams(vmem_limit_bytes=60 * 1024 * 1024),
        name="attn",
    )(lam, cos, sin, qk, vog)


def sender(src, dst, ssem, rsem, device):
    return pltpu.make_async_remote_copy(
        src_ref=src, dst_ref=dst, send_sem=ssem, recv_sem=rsem,
        device_id=device, device_id_type=pl.DeviceIdType.MESH,
    )


def places(sp, dp):
    me, mine = lax.axis_index("sp"), lax.axis_index("dp")
    z, core = mine // 2, lax.rem(mine, 2)
    nz = dp // 2
    if sp == 4:
        peers = [me + 1 - 2 * lax.rem(me, 2), lax.rem(me + 2, 4), 3 - me]
        froms = peers
    else:
        peers = [lax.rem(me + d, sp) for d in range(1, sp)]
        froms = [lax.rem(me + sp - d, sp) for d in range(1, sp)]
    z_to = [lax.rem(z + i, nz) * 2 for i in range(1, nz)]
    z_from = [lax.rem(z + nz - i, nz) * 2 for i in range(1, nz)]
    return me, mine, z, core, peers, froms, z_to, z_from


def greet(me, mine, core, peers, z_to):
    barrier = pltpu.get_barrier_semaphore()
    where = [(p, mine) for p in peers] + [(me, zt + core) for zt in z_to] + [(me, mine + 1 - 2 * core)]
    for device in where:
        pl.semaphore_signal(barrier, inc=1, device_id=device, device_id_type=pl.DeviceIdType.MESH)
    pl.semaphore_wait(barrier, len(where))


def gather_kernel(sp, dp, tok_ref, v_ref, og_ref, wq_ref, wk_ref, tok_all, vog_all, w_all, qk_ref,
                  vog_ref, tok_ss, tok_rs, vog_ss, vog_rs, w_ss, w_rs, sib_ss, sib_rs):
    me, mine, z, core, peers, froms, z_to, z_from = places(sp, dp)
    rows, wr = tok_ref.shape[0], wq_ref.shape[0]
    sib = (me, mine + 1 - 2 * core)

    def trow(i, start=0, size=rows):
        return pl.ds(pl.multiple_of(i * rows + start, 16), size)

    def wrow(i):
        return pl.ds(pl.multiple_of(i * wr, wr), wr)

    vc, qc = v_ref.shape[1] // sp, wq_ref.shape[1] // sp
    for s in range(sp):
        vog_ref[s, 0] = v_ref[:, s * vc : (s + 1) * vc]
        vog_ref[s, 1] = og_ref[:, s * vc : (s + 1) * vc]

        @pl.when(me == s)
        def _():
            w_all[wrow(mine), :qc] = wq_ref[:, s * qc : (s + 1) * qc]
            w_all[wrow(mine), qc:] = wk_ref[:, s * qc : (s + 1) * qc]

    tok_all[trow(me), :] = tok_ref[...]
    greet(me, mine, core, peers, z_to)
    w_ref = w_all.at[wrow(mine)]
    sends = []

    def go(copy):
        copy.start()
        sends.append(copy)
        return copy

    wz = [go(sender(w_ref, w_all.at[wrow(mine)], w_ss.at[i], w_rs.at[i], (me, zt + core)))
          for i, zt in enumerate(z_to)]
    ws = [go(sender(w_ref, w_all.at[wrow(mine)], sib_ss.at[0], sib_rs.at[0], sib))]
    half = rows // 2
    if sp == 4:
        def piece(p, h, k):
            r = trow(me, h * half, half)
            return go(sender(tok_ref.at[pl.ds(h * half, half)], tok_all.at[r], tok_ss.at[k], tok_rs.at[k], (p, mine)))

        x0, y1 = piece(peers[0], 0, 0), piece(peers[1], 1, 1)
        x1, y0 = piece(peers[0], 1, 2), piece(peers[1], 0, 3)
    else:
        tk = [go(sender(tok_ref, tok_all.at[trow(me)], tok_ss.at[i], tok_rs.at[i], (p, mine)))
              for i, p in enumerate(peers)]
    vg = [go(sender(vog_ref.at[p], vog_all.at[:, trow(me)], vog_ss.at[i], vog_rs.at[i], (p, mine)))
          for i, p in enumerate(peers)]
    vog_all[:, trow(me), :] = vog_ref[me]
    if sp == 4:
        x0.wait_recv()
        f0 = trow(peers[0], 0, half)
        d0 = go(sender(tok_all.at[f0], tok_all.at[f0], tok_ss.at[4], tok_rs.at[4], (peers[1], mine)))
        y1.wait_recv()
        f1 = trow(peers[1], half, half)
        d1 = go(sender(tok_all.at[f1], tok_all.at[f1], tok_ss.at[5], tok_rs.at[5], (peers[0], mine)))
        arrivals = [[x1], [y0], [d0, d1]]
    else:
        arrivals = [[c] for c in tk]
    for i, zf in enumerate(z_from):
        wz[i].wait_recv()
        r = wrow(zf + core)
        ws.append(go(sender(w_all.at[r], w_all.at[r], sib_ss.at[i + 1], sib_rs.at[i + 1], sib)))
    for c in ws:
        c.wait_recv()
    qk_ref[trow(me), :] = dot(tok_ref[...], w_all[...])
    for f, copies in zip(froms, arrivals):
        for c in copies:
            c.wait_recv()
        qk_ref[trow(f), :] = dot(tok_all[trow(f), :], w_all[...])
    for c in vg:
        c.wait_recv()
    for c in sends:
        c.wait_send()


def gather(tok, v, og, wq, wk, sp, dp):
    rows, width = tok.shape
    vc, wr, cols = v.shape[1] // sp, wq.shape[0], 2 * wq.shape[1] // sp
    vm = pl.BlockSpec(memory_space=pltpu.VMEM)
    dma = pltpu.SemaphoreType.DMA
    nt = 6 if sp == 4 else sp - 1
    nz = dp // 2
    return pl.pallas_call(
        functools.partial(gather_kernel, sp, dp),
        out_shape=(
            jax.ShapeDtypeStruct((rows * sp, width), BF16),
            jax.ShapeDtypeStruct((2, rows * sp, vc), BF16),
            jax.ShapeDtypeStruct((wr * dp, cols), BF16),
            jax.ShapeDtypeStruct((rows * sp, cols), F32),
        ),
        in_specs=[vm] * 5,
        out_specs=(vm,) * 4,
        scratch_shapes=[pltpu.VMEM((sp, 2, rows, vc), BF16), dma((nt,)), dma((nt,)), dma((sp - 1,)), dma((sp - 1,)),
                        dma((nz - 1,)), dma((nz - 1,)), dma((nz,)), dma((nz,))],
        compiler_params=pltpu.CompilerParams(
            vmem_limit_bytes=60 * 1024 * 1024, collective_id=0, has_side_effects=True
        ),
        name="gather",
    )(tok, v, og, wq, wk)


def scatter_kernel(sp, dp, back_t, back_m, tok_all, w_all, dv, tg_out, dv_out, qg, kg,
                   tbuf, trecv, tacc, dvr, sib_s, sib_r, wz_s, wz_r, wacc, wg_s, wg_r,
                   t_ss, t_rs, d_ss, d_rs, s_ss, s_rs, z_ss, z_rs, g_ss, g_rs):
    me, mine, z, core, peers, froms, z_to, z_from = places(sp, dp)
    nz = dp // 2
    rows, wr = tg_out.shape[0], qg.shape[0]
    vc = dv.shape[1]
    qc = w_all.shape[1] // 2
    sib = (me, mine + 1 - 2 * core)
    greet(me, mine, core, peers, z_to)
    sends = []

    def go(copy):
        copy.start()
        sends.append(copy)
        return copy

    def trow(i):
        return pl.ds(pl.multiple_of(i * rows, 16), rows)

    def weight_part(owner):
        return dot(back_t[...], tok_all[:, pl.ds(pl.multiple_of(owner * wr, wr), wr)])

    def token_part(p):
        return dot(back_m[trow(p), :], w_all[...], 1, 1)

    def send_tokens(i):
        tbuf[i] = token_part(peers[i]).astype(BF16)
        return go(sender(tbuf.at[i], trecv.at[i], t_ss.at[i], t_rs.at[i], (peers[i], mine)))

    targets = z_to + [z * 2]
    half = rows // 2
    lo, hi = pl.ds(0, half), pl.ds(half, half)
    tg = []

    def hop(i, dst, part, k, to):
        return go(sender(tbuf.at[i, part], trecv.at[dst, part], t_ss.at[k], t_rs.at[k], (peers[to], mine)))

    if sp == 4:
        tbuf[2] = token_part(peers[2]).astype(BF16)
        via_x, via_y = hop(2, 2, lo, 0, 0), hop(2, 2, hi, 1, 1)
    else:
        tg.append(send_tokens(0))
    sb = []
    for i, zt in enumerate(targets):
        sib_s[i] = weight_part(zt + 1 - core).astype(BF16)
        sb.append(go(sender(sib_s.at[i], sib_r.at[i], s_ss.at[i], s_rs.at[i], sib)))
    zs = []
    for i, zt in enumerate(targets):
        part = weight_part(zt + core)
        sb[i].wait_recv()
        part = part + sib_r[i].astype(F32)
        if i < nz - 1:
            wz_s[i] = part.astype(BF16)
            zs.append(go(sender(wz_s.at[i], wz_r.at[i], z_ss.at[i], z_rs.at[i], (me, zt + core))))
        else:
            wacc[...] = part
    if sp == 4:
        part = token_part(peers[0])
        tbuf[0, lo] = part[:half].astype(BF16)
        x_lo = hop(0, 0, lo, 2, 0)
        tacc[hi] = part[half:]
        part = token_part(peers[1])
        tbuf[1, hi] = part[half:].astype(BF16)
        y_hi = hop(1, 1, hi, 3, 1)
        tacc[lo] = part[:half]
        via_x.wait_recv()
        tbuf[1, lo] = (tacc[lo] + trecv[2, lo].astype(F32)).astype(BF16)
        y_lo = hop(1, 1, lo, 4, 1)
        via_y.wait_recv()
        tbuf[0, hi] = (tacc[hi] + trecv[2, hi].astype(F32)).astype(BF16)
        x_hi = hop(0, 0, hi, 5, 0)
        tg = [x_lo, x_hi, y_lo, y_hi]
    else:
        for i in range(1, sp - 1):
            tg.append(send_tokens(i))
    dvc = [go(sender(dv.at[trow(p)], dvr.at[me], d_ss.at[i], d_rs.at[i], (p, mine)))
           for i, p in enumerate(peers)]
    dvr[me] = dv[trow(me), :]
    tacc[...] = token_part(me)
    for i in range(nz - 1):
        zs[i].wait_recv()
        wacc[...] += wz_r[i].astype(F32)
    total = wacc[...].T.astype(BF16)
    wg_s[...] = total
    wg_r[me] = total
    wh = wr // 2
    if sp == 4:
        def piece(p, h, k):
            r = pl.ds(h * wh, wh)
            return go(sender(wg_s.at[r], wg_r.at[me, r], g_ss.at[k], g_rs.at[k], (p, mine)))

        def forward(f, h, k, p):
            r = pl.ds(h * wh, wh)
            return go(sender(wg_r.at[f, r], wg_r.at[f, r], g_ss.at[k], g_rs.at[k], (p, mine)))

        gx0, gy1 = piece(peers[0], 0, 0), piece(peers[1], 1, 1)
        gx1, gy0 = piece(peers[0], 1, 2), piece(peers[1], 0, 3)
        gx0.wait_recv()
        gd0 = forward(peers[0], 0, 4, peers[1])
        gy1.wait_recv()
        gd1 = forward(peers[1], 1, 5, peers[0])
        gs = [gx1, gy0, gd0, gd1]
    else:
        gs = [go(sender(wg_s, wg_r.at[me], g_ss.at[i], g_rs.at[i], (p, mine))) for i, p in enumerate(peers)]
    for c in tg:
        c.wait_recv()
    for i in range(2 if sp == 4 else sp - 1):
        tacc[...] += trecv[i].astype(F32)
    tg_out[...] = tacc[...].astype(BF16)
    for c in dvc:
        c.wait_recv()
    for s in range(sp):
        dv_out[:, s * vc : (s + 1) * vc] = dvr[s]
    for c in gs:
        c.wait_recv()
    for s in range(sp):
        qg[:, s * qc : (s + 1) * qc] = wg_r[s, :, :qc]
        kg[:, s * qc : (s + 1) * qc] = wg_r[s, :, qc:]
    for c in sends:
        c.wait_send()


def scatter(back_t, back_m, tok_all, w_all, dv, sp, dp):
    seq, width = tok_all.shape
    rows, wr = seq // sp, width // dp
    cols = w_all.shape[1]
    vc = dv.shape[1]
    nz = dp // 2
    vm = pl.BlockSpec(memory_space=pltpu.VMEM)
    dma = pltpu.SemaphoreType.DMA
    nt = 6 if sp == 4 else sp - 1
    return pl.pallas_call(
        functools.partial(scatter_kernel, sp, dp),
        out_shape=(
            jax.ShapeDtypeStruct((rows, width), BF16),
            jax.ShapeDtypeStruct((rows, vc * sp), BF16),
            jax.ShapeDtypeStruct((wr, cols // 2 * sp), BF16),
            jax.ShapeDtypeStruct((wr, cols // 2 * sp), BF16),
        ),
        in_specs=[vm] * 5,
        out_specs=(vm,) * 4,
        scratch_shapes=[
            pltpu.VMEM((sp - 1, rows, width), BF16),
            pltpu.VMEM((sp - 1, rows, width), BF16),
            pltpu.VMEM((rows, width), F32),
            pltpu.VMEM((sp, rows, vc), BF16),
            pltpu.VMEM((nz, cols, wr), BF16),
            pltpu.VMEM((nz, cols, wr), BF16),
            pltpu.VMEM((nz - 1, cols, wr), BF16),
            pltpu.VMEM((nz - 1, cols, wr), BF16),
            pltpu.VMEM((cols, wr), F32),
            pltpu.VMEM((wr, cols), BF16),
            pltpu.VMEM((sp, wr, cols), BF16),
            dma((nt,)), dma((nt,)), dma((sp - 1,)), dma((sp - 1,)), dma((nz,)), dma((nz,)),
            dma((nz - 1,)), dma((nz - 1,)), dma((nt,)), dma((nt,)),
        ],
        compiler_params=pltpu.CompilerParams(
            vmem_limit_bytes=62 * 1024 * 1024, collective_id=1, has_side_effects=True
        ),
        name="scatter",
    )(back_t, back_m, tok_all, w_all, dv)


def position_tables(seq_length):
    half = DQK // 2
    freqs = np.exp(np.float32(-math.log(THETA)) * np.arange(half, dtype=np.float32) / np.float32(half)).astype(np.float32)
    angles = freqs[:, None] * np.arange(seq_length, dtype=np.float32)[None, :]
    wide = angles.astype(np.float64)
    return jnp.asarray(np.concatenate([np.cos(wide), np.sin(wide)]).astype(np.float32))


def head_scores(hh, cos, sin, q, k_in, qt_s, kt_s, p_s, lam):
    seq = cos.shape[1]
    scale = math.log2(math.e) / math.sqrt(DQK)
    step = 256
    zero_half = jnp.zeros((DQK, step), BF16)
    qt = rotate_rows(q, cos, sin).astype(BF16)
    kt = rotate_rows(k_in, cos, sin).astype(BF16)
    qt_s[hh] = qt
    kt_s[hh] = kt
    k = kt.T
    for t0 in range(0, seq, step):
        end = min(t0 + step, seq)
        tb = end - t0
        zh = zero_half[:, :tb]
        q_b = qt[:, t0:end]
        mask = lax.broadcasted_iota(jnp.int32, (tb, tb), 0) <= lax.broadcasted_iota(jnp.int32, (tb, tb), 1)
        for m in range(2):
            half_q = q_b[m * DQK : (m + 1) * DQK]
            rhs = jnp.concatenate([half_q, zh] if m == 0 else [zh, half_q], axis=0)
            s = dot(k[:end], rhs)
            diag = jnp.where(mask, s[t0:], -jnp.inf)
            s = jnp.concatenate([s[:t0], diag], axis=0) if t0 else diag
            e = jnp.exp2((s - jnp.max(s, axis=0, keepdims=True)) * scale)
            r = 1.0 / jnp.sum(e, axis=0, keepdims=True)
            p_s[hh, m, :end, t0:end] = e * (r if m == 0 else r * -lam)


def pair_back(h0, cos, sin, lams, qt_s, kt_s, p_s, vt_s, ogt_s, dvt_s, dk_s, bt_s):
    seq = cos.shape[1]
    hw = 2 * DQK
    ve = vt_s.shape[0] // 2
    inv_root = 1.0 / math.sqrt(DQK)
    step = 256
    cb, sb = cos * inv_root, sin * -inv_root
    work = [(hh, t0, min(t0 + step, seq)) for t0 in range(0, seq, step) for hh in range(2)]
    rows = [slice(hh * hw, (hh + 1) * hw) for hh in range(2)]
    vrows = [slice(hh * ve, (hh + 1) * ve) for hh in range(2)]
    vt = [vt_s[r, :] for r in vrows]
    v = [x.T for x in vt]
    mix, ho, ob, g1, g2 = {}, {}, {}, {}, {}
    for w in work:
        hh, t0, end = w
        mix[w] = (p_s[h0 + hh, 0, :end, t0:end] + p_s[h0 + hh, 1, :end, t0:end]).astype(BF16)
        ho[w] = dot(vt[hh][:, :end], mix[w])
    for w in work:
        hh, t0, end = w
        x = ho[w]
        inv = lax.rsqrt(jnp.mean(x * x, axis=0, keepdims=True) + NORM_EPS)
        og = ogt_s[vrows[hh], t0:end].astype(F32)
        ob[w] = (inv * og - inv * inv * inv * x * jnp.mean(og * x, axis=0, keepdims=True)).astype(BF16)
    for w in work:
        hh, t0, end = w
        mg = dot(v[hh][:end], ob[w])
        p1, p2 = p_s[h0 + hh, 0, :end, t0:end], p_s[h0 + hh, 1, :end, t0:end]
        g1[w] = (p1 * (mg - jnp.sum(mg * p1, axis=0, keepdims=True))).astype(BF16)
        g2[w] = (p2 * (mg + jnp.sum(mg * p2, axis=0, keepdims=True) * (1.0 / lams[hh]))).astype(BF16)
        q_b, kt = qt_s[h0 + hh, :, t0:end], kt_s[h0 + hh]
        dq = jnp.concatenate([dot(kt[:DQK, :end], g1[w]), dot(kt[DQK:, :end], g2[w])], axis=0)
        bt_s[rows[hh], t0:end] = rotate_rows(dq, cb[:, t0:end], sb[:, t0:end]).astype(BF16)
        dvd = dot(ob[w], mix[w], 1, 1)
        dkd = jnp.concatenate([dot(q_b[:DQK], g1[w], 1, 1), dot(q_b[DQK:], g2[w], 1, 1)], axis=0)
        if t0:
            dvd = jnp.concatenate([dvt_s[vrows[hh], :t0] + dvd[:, :t0], dvd[:, t0:]], axis=1)
            dkd = jnp.concatenate([dk_s[rows[hh], :t0] + dkd[:, :t0], dkd[:, t0:]], axis=1)
        dvt_s[vrows[hh], :end] = dvd
        dk_s[rows[hh], :end] = dkd
    for hh in range(2):
        bt_s[2 * hw + hh * hw : 2 * hw + (hh + 1) * hw, :] = rotate_rows(dk_s[rows[hh], :], cb, sb).astype(BF16)


def fused_kernel(sp, dp, pairs, lam_in, rot_in, tok_in, v_in, og_in, wq_in, wk_in,
                 tg_out, dvr, wg_r,
                 lam_ref, rot_ref, tok_all, w1, w2, qk_s, vog_src, vog_all, qt_s, kt_s, p_s,
                 vt_s, ogt_s, dvt_s, dk_s, bt_s, back_m, back_x,
                 dv_s, sib_s, sib_r, own_s, wz_s, wz_r, wz_m, tbuf, trecv, tacc,
                 pool, tok_rs, vog_rs, z_rs, s_rs, bx_rs, dv_rs, c_rs, g_rs, m_rs, ag_rs, ty_rs):
    me, mine, z, core, peers, froms, z_to, z_from = places(sp, dp)
    nz = dp // 2
    rows, wr = tok_in.shape[0], wq_in.shape[0]
    half = rows // 2
    pw = 128
    sib = (me, mine + 1 - 2 * core)
    xp, yp = (peers[0], mine), (peers[1], mine)

    def trow(i, start=0, size=rows):
        return pl.ds(pl.multiple_of(i * rows + start, 16), size)

    def wrow(zz, c):
        return pl.ds(pl.multiple_of((c * nz + zz) * wr, wr), wr)

    def lanes(i, size):
        return pl.ds(pl.multiple_of(i * size, size), size)

    sends = []
    free = list(range(pool.shape[0]))

    def remote(src, dst, rsem, device):
        return lambda ssem: sender(src, dst, ssem, rsem, device)

    def arrive(link):
        link(pool.at[0]).wait_recv()

    def ready(link, cond=None):
        slot = free.pop(0)
        copy = link(pool.at[slot])
        sends.append((copy, cond, slot))
        return copy

    def go(link, cond=None):
        copy = ready(link, cond)
        if cond is None:
            copy.start()
        else:
            pl.when(cond)(copy.start)
        return link

    def flush(count):
        for c, cond, slot in sends[:count]:
            if cond is None:
                c.wait_send()
            else:
                pl.when(cond)(c.wait_send)
            free.append(slot)
        del sends[:count]

    barrier = pltpu.get_barrier_semaphore()
    where = [(p, mine) for p in peers] + [(me, zt + core) for zt in z_to] + [sib]
    for device in where:
        pl.semaphore_signal(barrier, inc=1, device_id=device, device_id_type=pl.DeviceIdType.MESH)

    def load(src, dst):
        slot = free.pop(0)
        c = pltpu.make_async_copy(src, dst, pool.at[slot])
        c.start()
        return c, slot

    def loaded(copies):
        for c, slot in copies:
            c.wait()
            free.append(slot)

    def load_weights(w, who):
        out = []
        for j in range(pairs):
            src = lanes(who * pairs + j, pw)
            out.append(load(wq_in.at[:, src], w.at[wrow(z, core), 2 * j * pw : (2 * j + 1) * pw]))
            out.append(load(wk_in.at[:, src], w.at[wrow(z, core), (2 * j + 1) * pw : (2 * j + 2) * pw]))
        return out

    l_tok = []
    for c in range(2):
        for zz in range(nz):
            n = slice((c * nz + zz) * wr, (c * nz + zz + 1) * wr)
            l_tok.append(load(tok_in.at[:, (2 * zz + c) * wr : (2 * zz + c + 1) * wr], tok_all.at[trow(me), n]))
    l_w1 = load_weights(w1, me)
    far = lax.rem(z + 2, nz)
    order = [far, z + 1 - 2 * lax.rem(z, 2), nz - 1 - z]
    inner = jnp.logical_and(z > 0, z < nz - 1)
    outer = jnp.logical_not(inner)

    def z_copy(w, k, n, src, to):
        r = w.at[wrow(src, core)]
        return remote(r, r, z_rs.at[k, src], (me, 2 * to + core))

    def s_copy(w, k, src):
        r = w.at[wrow(src, core)]
        return remote(r, r, s_rs.at[k, src], sib)

    def z_start():
        go(z_copy(w1, 0, 0, z, far))
        go(z_copy(w1, 0, 1, z, order[1]))
        go(z_copy(w1, 0, 2, z, order[2]), inner)
        go(s_copy(w1, 0, z))

    def z_step(i):
        arrive(z_copy(w1, 0, 0, order[i], z))
        go(s_copy(w1, 0, order[i]))
        if i == 0:
            go(z_copy(w1, 0, 3, far, order[1]), inner)

    aside = (1 - z // 2) * (nz - 1)
    near = [order[1], jnp.where(inner, order[2], far)]

    def other_start():
        go(z_copy(w2, 1, 0, z, far), inner)
        go(z_copy(w2, 1, 1, z, order[1]))
        go(z_copy(w2, 1, 2, z, order[2]), inner)
        go(s_copy(w2, 1, z))

    def other_aside():
        r = wrow(aside, core)
        to = (jnp.where(core == 0, peers[0], peers[1]), mine)
        return remote(w1.at[r], w2.at[r], z_rs.at[1, aside], to)

    def other_step(src):
        arrive(z_copy(w2, 1, 0, src, z))
        go(s_copy(w2, 1, src))

    def z_sib(w, k):
        for src in [z] + order:
            r = w.at[wrow(src, 1 - core)]
            arrive(remote(r, r, s_rs.at[k, src], sib))

    def piece(p, h, k):
        r = trow(me, h * half, half)
        return go(remote(tok_all.at[r], tok_all.at[r], tok_rs.at[k], p))

    loaded(l_tok)
    pl.semaphore_wait(barrier, len(where))
    x0, y1 = piece(xp, 0, 0), piece(yp, 1, 1)
    x1, y0 = piece(xp, 1, 2), piece(yp, 0, 3)
    loaded(l_w1)
    z_start()
    l_vog = []
    for n, src in enumerate((v_in, og_in)):
        for i, p in enumerate(peers):
            l_vog.append(load(src.at[:, lanes(p, pairs * pw)], vog_src.at[i, n]))
        l_vog.append(load(src.at[:, lanes(me, pairs * pw)], vog_all.at[n, trow(me)]))
    l_w2 = load_weights(w2, jnp.where(core == 0, peers[0], peers[1]))
    l_rot = [load(rot_in, rot_ref), load(lam_in, lam_ref)]
    loaded(l_w2 + l_vog + l_rot)
    arrive(x0)
    f0 = trow(peers[0], 0, half)
    d0 = go(remote(tok_all.at[f0], tok_all.at[f0], tok_rs.at[4], yp))
    arrive(y1)
    f1 = trow(peers[1], half, half)
    d1 = go(remote(tok_all.at[f1], tok_all.at[f1], tok_rs.at[5], xp))

    def vog_start(j):
        for i in range(sp - 1):
            n = slice(j * pw, (j + 1) * pw)
            dst = vog_all.at[:, trow(me), n]
            go(remote(vog_src.at[i, :, :, n], dst, vog_rs.at[j, i], (peers[i], mine)))

    vog_start(0)
    z_step(0)
    z_step(1)
    z_step(2)
    other_start()
    z_sib(w1, 0)
    qk_s[trow(me), :] = dot(tok_all[trow(me), :], w1[...])
    for f, copies in zip(froms, [[x1], [y0], [d0, d1]]):
        for c in copies:
            arrive(c)
        qk_s[trow(f), :] = dot(tok_all[trow(f), :], w1[...])

    n16 = DQK // 2
    cos, sin = rot_ref[:n16, :], rot_ref[n16:, :]
    hw = 2 * DQK

    lams = [lam_ref[me * pairs * 2 + h] for h in range(2 * pairs)]
    def scores(j):
        qk = [qk_s[:, (2 * j + n) * pw : (2 * j + n + 1) * pw].T for n in range(2)]
        for hh in range(2):
            r = slice(hh * hw, (hh + 1) * hw)
            h = 2 * j + hh
            head_scores(h, cos, sin, qk[0][r], qk[1][r], qt_s, kt_s, p_s, lams[h])

    def values_start(j):
        for i, p in enumerate(peers):
            go(remote(dv_s.at[j, trow(p)], dvr.at[me, j], dv_rs.at[j, i], (p, mine)))
        dvr[me, j] = dv_s[j, trow(me), :]

    def one_pair(j):
        for i, p in enumerate(peers):
            r = vog_all.at[:, trow(p), j * pw : (j + 1) * pw]
            arrive(remote(r, r, vog_rs.at[j, i], (p, mine)))
        if j == 0:
            go(other_aside())
        vt_s[...] = vog_all[0, :, j * pw : (j + 1) * pw].T
        ogt_s[...] = vog_all[1, :, j * pw : (j + 1) * pw].T
        pair_back(2 * j, cos, sin, lams[2 * j : 2 * j + 2], qt_s, kt_s, p_s, vt_s, ogt_s, dvt_s, dk_s, bt_s)
        back_m[j] = bt_s[...].T
        for a, to in enumerate((0, 1)):
            for b, p in enumerate((peers[to], peers[2])):
                go(remote(back_m.at[j, trow(p)], back_x.at[a, j, b], bx_rs.at[a, j, b], (xp, yp)[to]))

        if j:
            merge(j - 1)

        def weight_part(c):
            return dot(bt_s[...], tok_all[:, lanes(c, nz * wr)])

        part = weight_part(1 - core)
        for zz in range(nz):
            sib_s[j, zz] = part[:, zz * wr : (zz + 1) * wr].astype(BF16)
        go(remote(sib_s.at[j], sib_r.at[j], c_rs.at[j], sib))
        part = weight_part(core)
        for zz in range(nz):
            own_s[j, zz] = part[:, zz * wr : (zz + 1) * wr]
        dv_s[j] = dvt_s[...].T.astype(BF16)
        values_start(j)

    def shares(j):
        arrive(remote(sib_s.at[j], sib_r.at[j], c_rs.at[j], sib))
        for i in range(nz):
            own_s[j, i] = own_s[j, i] + sib_r[j, i].astype(F32)
        for i in range(nz - 1):
            wz_s[j, i] = own_s[j, order[i]].astype(BF16)
        go(remote(wz_s.at[j, 2], wz_m.at[j], m_rs.at[j], (me, 2 * order[1] + core)), outer)
        go(z_share(j, 0), outer)
        go(z_share(j, 2), inner)
        go(z_share(j, 1))

    def z_share(j, i):
        return remote(wz_s.at[j, i], wz_r.at[j, i], g_rs.at[j, i], (me, 2 * order[i] + core))

    def merge(j):
        copy = ready(z_share(j, 0), inner)

        @pl.when(inner)
        def _():
            arrive(remote(wz_m.at[j], wz_m.at[j], m_rs.at[j], sib))
            wz_s[j, 0] = (own_s[j, far] + wz_m[j].astype(F32)).astype(BF16)
            copy.start()

    scores(0)
    flush(10)
    for j in range(1, pairs):
        vog_start(j)
        scores(j)
    for j in range(pairs):
        one_pair(j)
        if j == 0:
            done = len(sends)
        shares(j)
        if j == 0:
            other_step(near[0])

    def back_wait(a, j, b):
        r = back_x.at[a, j, b]
        arrive(remote(r, r, bx_rs.at[a, j, b], sib))

    def token_part(who, a, b, parts):
        n = slice(a * nz * wr, (a + 1) * nz * wr)
        out = None
        for j, own in parts:
            k = slice(2 * j * pw, (2 * j + 2) * pw)
            part = dot(back_m[j, trow(who), :], w1[n, k], 1, 1) if own else dot(back_x[a, j, b], w2[n, k], 1, 1)
            out = part if out is None else out + part
        return out

    early = [(j, True) for j in range(pairs)] + [(j, False) for j in range(pairs - 1)]
    late = [(pairs - 1, False)]
    other_step(near[1])
    other_step(aside)
    z_sib(w2, 1)
    for a in range(2):
        for b in range(2):
            for j in range(pairs - 1):
                back_wait(a, j, b)
    for a in range(2):
        tacc[a] = token_part(peers[1 - a], a, 1, early)
    flush(done)
    ty = {}
    for a in range(2):
        back_wait(a, pairs - 1, 1)
        tbuf[a] = (tacc[a] + token_part(peers[1 - a], a, 1, late)).astype(BF16)
        for h in range(2):
            r = pl.ds(h * half, half)
            ty[a, h] = go(remote(tbuf.at[a, r], trecv.at[a, r], ty_rs.at[a, h], (yp, xp)[a]))

    def weights_end(j):
        @pl.when(inner)
        def _():
            arrive(z_share(j, 2))
            own_s[j, z] = own_s[j, z] + wz_r[j, 2].astype(F32)

        arrive(z_share(j, 0))
        arrive(z_share(j, 1))
        total = own_s[j, z] + wz_r[j, 0].astype(F32) + wz_r[j, 1].astype(F32)
        wg_r[me, j] = total.T.astype(BF16)
        for h, k, to in ((0, 0, xp), (1, 1, yp), (1, 2, xp), (0, 3, yp)):
            go(ag(me, j, h, k, to))

    wh = wr // 2

    def ag(owner, j, h, k, to):
        r = wg_r.at[owner, j, pl.ds(h * wh, wh)]
        return remote(r, r, ag_rs.at[j, k], to)

    def weights_relay(j):
        arrive(ag(peers[0], j, 0, 0, xp))
        go(ag(peers[0], j, 0, 4, yp))
        arrive(ag(peers[1], j, 1, 1, yp))
        go(ag(peers[1], j, 1, 5, xp))

    merge(pairs - 1)
    weights_end(0)
    for a in range(2):
        back_wait(a, pairs - 1, 0)
    for a in range(2):
        tacc[a] = token_part(me, a, 0, early + late)
    for j in range(1, pairs):
        weights_end(j)
    for h in range(2):
        for a in range(2):
            arrive(ty[a, h])
            if h == 1 and a == 1:
                flush(len(sends) - 4 * pairs)
            r = slice(h * half, (h + 1) * half)
            total = (tacc[a, r] + trecv[a, r].astype(F32)).astype(BF16)
            for zz in range(nz):
                tg_out[r, (2 * zz + a) * wr : (2 * zz + a + 1) * wr] = total[:, zz * wr : (zz + 1) * wr]
    for j in range(pairs):
        weights_relay(j)
    for j in range(pairs):
        for i, p in enumerate(peers):
            r = dvr.at[p, j]
            arrive(remote(r, r, dv_rs.at[j, i], xp))
        for owner, h, k in ((peers[0], 1, 2), (peers[1], 0, 3), (peers[2], 0, 4), (peers[2], 1, 5)):
            arrive(ag(owner, j, h, k, xp))
    flush(len(sends))


def finish_kernel(factor, tg, dvr, wg, tg_out, dv_out, qg_out, kg_out, dv_s, qg, kg, sem):
    sp, pairs, wr, cols = wg.shape
    pw = cols // 2
    copies = [pltpu.make_async_copy(tg, tg_out, sem.at[0])]
    copies[0].start()
    for s in range(sp):
        for j in range(pairs):
            n = slice((s * pairs + j) * pw, (s * pairs + j + 1) * pw)
            qg[:, n] = wg[s, j, :, :pw].astype(F32) * factor
    copies.append(pltpu.make_async_copy(qg, qg_out, sem.at[1]))
    copies[1].start()
    for s in range(sp):
        for j in range(pairs):
            n = slice((s * pairs + j) * pw, (s * pairs + j + 1) * pw)
            kg[:, n] = wg[s, j, :, pw:].astype(F32) * factor
    copies.append(pltpu.make_async_copy(kg, kg_out, sem.at[2]))
    copies[2].start()
    for s in range(sp):
        for j in range(pairs):
            n = slice((s * pairs + j) * pw, (s * pairs + j + 1) * pw)
            dv_s[:, n] = dvr[s, j]
    copies.append(pltpu.make_async_copy(dv_s, dv_out, sem.at[3]))
    copies[3].start()
    for c in copies:
        c.wait()


def fused(tok, v, og, wq, wk, lam, rot, sp, dp):
    rows, width = tok.shape
    seq = rows * sp
    wr = wq.shape[0]
    nz = dp // 2
    pw = 128
    pairs = v.shape[1] // (sp * pw)
    factor = 1.0 / math.sqrt(dp * seq)
    vm = pl.BlockSpec(memory_space=pltpu.VMEM)
    anywhere = pl.BlockSpec(memory_space=pl.ANY)
    dma = pltpu.SemaphoreType.DMA
    V = pltpu.VMEM
    tg, dvr, wg = pl.pallas_call(
        functools.partial(fused_kernel, sp, dp, pairs),
        out_shape=(
            V((rows, width), BF16),
            V((sp, pairs, rows, pw), BF16),
            V((sp, pairs, wr, 2 * pw), BF16),
        ),
        in_specs=[anywhere] * 7,
        out_specs=(vm,) * 3,
        scratch_shapes=[
            pltpu.SMEM(lam.shape, F32), V(rot.shape, F32),
            V((seq, width), BF16), V((width, 2 * pairs * pw), BF16), V((width, 2 * pairs * pw), BF16),
            V((seq, 2 * pairs * pw), F32), V((sp - 1, 2, rows, pairs * pw), BF16), V((2, seq, pairs * pw), BF16),
            V((2 * pairs, 2 * DQK, seq), BF16), V((2 * pairs, 2 * DQK, seq), BF16), V((2 * pairs, 2, seq, seq), F32),
            V((pw, seq), BF16), V((pw, seq), BF16), V((pw, seq), F32), V((pw, seq), F32), V((2 * pw, seq), BF16),
            V((pairs, seq, 2 * pw), BF16), V((2, pairs, 2, rows, 2 * pw), BF16),
            V((pairs, seq, pw), BF16),
            V((pairs, nz, 2 * pw, wr), BF16), V((pairs, nz, 2 * pw, wr), BF16), V((pairs, nz, 2 * pw, wr), F32),
            V((pairs, nz - 1, 2 * pw, wr), BF16), V((pairs, nz - 1, 2 * pw, wr), BF16), V((pairs, 2 * pw, wr), BF16),
            V((2, rows, nz * wr), BF16), V((2, rows, nz * wr), BF16), V((2, rows, nz * wr), F32),
            dma((44,)), dma((6,)), dma((pairs, sp - 1)), dma((2, nz)), dma((2, nz)), dma((2, pairs, 2)),
            dma((pairs, sp - 1)), dma((pairs,)), dma((pairs, nz - 1)), dma((pairs,)), dma((pairs, 6)), dma((2, 2)),
        ],
        compiler_params=pltpu.CompilerParams(
            vmem_limit_bytes=56 * 1024 * 1024, collective_id=2, has_side_effects=True
        ),
        name="fused",
    )(lam, rot, tok, v, og, wq, wk)
    return pl.pallas_call(
        functools.partial(finish_kernel, factor),
        out_shape=(
            jax.ShapeDtypeStruct((rows, width), BF16),
            jax.ShapeDtypeStruct((rows, v.shape[1]), BF16),
            jax.ShapeDtypeStruct((wr, wq.shape[1]), F32),
            jax.ShapeDtypeStruct((wr, wq.shape[1]), F32),
        ),
        in_specs=[vm] * 3,
        out_specs=(anywhere,) * 4,
        scratch_shapes=[V((rows, v.shape[1]), BF16), V((wr, wq.shape[1]), F32), V((wr, wq.shape[1]), F32), dma((4,))],
        compiler_params=pltpu.CompilerParams(vmem_limit_bytes=16 * 1024 * 1024),
        name="finish",
    )(tg, dvr, wg)


def body(tokens, query_weight, key_weight, values, lambdas, out_grad):
    sp = lax.axis_size("sp")
    dp = lax.axis_size("dp")
    rows = tokens.shape[1]
    heads = lambdas.shape[0] // sp
    head_vec = values.shape[2] // lambdas.shape[0]
    if sp == 4 and dp == 8 and heads % 2 == 0 and head_vec == 64 and rows * sp <= 640:
        tg, dv, qg, kg = fused(
            tokens[0], values[0], out_grad[0], query_weight, key_weight, lambdas,
            position_tables(rows * sp), sp, dp,
        )
        return tg[None], dv[None], qg, kg
    cos, sin = rotation_tables(rows * sp)
    tok_all, vog_all, w_all, qk = gather(
        tokens[0], values[0], out_grad[0], query_weight, key_weight, sp, dp
    )
    back_t, back_m, dv = attention(qk, vog_all, lambdas, cos, sin, heads)
    tokens_grad, values_grad, qg, kg = scatter(back_t, back_m, tok_all, w_all, dv, sp, dp)
    factor = 1.0 / math.sqrt(dp * rows * sp)
    return tokens_grad[None], values_grad[None], qg.astype(F32) * factor, kg.astype(F32) * factor


def solution(mesh):
    x = P("dp", "sp", None)
    w = P("dp", None)
    return jax.shard_map(
        body, mesh=mesh, in_specs=(x, w, w, x, P(), x), out_specs=(x, x, w, w), check_vma=False
    )
```

```python
import functools
import math

import jax
import jax.numpy as jnp
import numpy as np
from jax import lax
from jax.experimental import pallas as pl
from jax.experimental.pallas import tpu as pltpu
from jax.sharding import PartitionSpec as P

DQK = 32
NORM_EPS = 0.1
THETA = 10000.0
F32 = jnp.float32
BF16 = jnp.bfloat16


def dot(a, b, ca=1, cb=0):
    return lax.dot_general(a, b, (((ca,), (cb,)), ((), ())), preferred_element_type=F32)


def rotation_tables(seq_length):
    half = DQK // 2
    freqs = jnp.exp(-math.log(THETA) * jnp.arange(half, dtype=F32) / half)
    angles = freqs[:, None] * jnp.arange(seq_length, dtype=jnp.int32).astype(F32)[None, :]
    return jnp.cos(angles), jnp.sin(angles)


def rotate_rows(x, cos, sin):
    half = DQK // 2
    parts = []
    for g in range(x.shape[0] // DQK):
        a = x[g * DQK : g * DQK + half]
        b = x[g * DQK + half : (g + 1) * DQK]
        parts += [a * cos - b * sin, b * cos + a * sin]
    return jnp.concatenate(parts, axis=0)


def attention_kernel(heads, lam_ref, cos_ref, sin_ref, qk_in, vog_ref, back_ref, rows_ref, dv_ref,
                     qk_ref, vt_s, ogt_s, dvt_s, dk_s):
    seq = cos_ref.shape[1]
    qc = qk_ref.shape[0] // 2
    hw = qc // heads
    ve = vog_ref.shape[2] // heads
    qk_ref[...] = qk_in[...].T
    inv_root = 1.0 / math.sqrt(DQK)
    vt_s[...] = vog_ref[0].T
    ogt_s[...] = vog_ref[1].T
    step = 256

    def one_head(h, _):
        lam = lam_ref[lax.axis_index("sp") * heads + h]
        cos, sin = cos_ref[...], sin_ref[...]
        qrow = pl.multiple_of(h * hw, hw)
        vrow = pl.multiple_of(h * ve, ve)
        qt = rotate_rows(qk_ref[pl.ds(qrow, hw), :], cos, sin).astype(BF16)
        kt = rotate_rows(qk_ref[pl.ds(qc + qrow, hw), :], cos, sin).astype(BF16)
        k = kt.T
        vt = vt_s[pl.ds(vrow, ve), :]
        v = vt.T
        zero_half = jnp.zeros((DQK, step), BF16)
        dk_s[...] = jnp.zeros_like(dk_s)
        dvt_s[pl.ds(vrow, ve), :] = jnp.zeros((ve, seq), F32)
        for t0 in range(0, seq, step):
            end = min(t0 + step, seq)
            tb = end - t0
            zh = zero_half[:, :tb]
            q_b = qt[:, t0:end]
            mask = lax.broadcasted_iota(jnp.int32, (tb, tb), 0) <= lax.broadcasted_iota(
                jnp.int32, (tb, tb), 1
            )
            probs = []
            for m in range(2):
                half_q = q_b[m * DQK : (m + 1) * DQK]
                rhs = jnp.concatenate([half_q, zh] if m == 0 else [zh, half_q], axis=0)
                s = dot(k[:end], rhs) * inv_root
                diag = jnp.where(mask, s[t0:], -jnp.inf)
                s = jnp.concatenate([s[:t0], diag], axis=0) if t0 else diag
                e = jnp.exp(s - jnp.max(s, axis=0, keepdims=True))
                probs.append(e * (1.0 / jnp.sum(e, axis=0, keepdims=True)))
            p1, p2 = probs
            mix = (p1 - lam * p2).astype(BF16)
            ho = dot(vt[:, :end], mix)
            inv = lax.rsqrt(jnp.mean(ho * ho, axis=0, keepdims=True) + NORM_EPS)
            og = ogt_s[pl.ds(vrow, ve), t0:end].astype(F32)
            ob = (inv * og - inv * inv * inv * ho * jnp.mean(og * ho, axis=0, keepdims=True)).astype(BF16)
            mg = dot(v[:end], ob) * inv_root
            g1 = (p1 * (mg - jnp.sum(mg * p1, axis=0, keepdims=True))).astype(BF16)
            g2 = ((-lam * p2) * (mg - jnp.sum(mg * p2, axis=0, keepdims=True))).astype(BF16)
            dvt_s[pl.ds(vrow, ve), :end] += dot(ob, mix, 1, 1)
            dq = jnp.concatenate([dot(kt[:DQK, :end], g1), dot(kt[DQK:, :end], g2)], axis=0)
            back_ref[pl.ds(qrow, hw), t0:end] = rotate_rows(dq, cos[:, t0:end], -sin[:, t0:end]).astype(BF16)
            dk_s[:DQK, :end] += dot(q_b[:DQK], g1, 1, 1)
            dk_s[DQK:, :end] += dot(q_b[DQK:], g2, 1, 1)
        back_ref[pl.ds(qc + qrow, hw), :] = rotate_rows(dk_s[...], cos, -sin).astype(BF16)
        return 0

    lax.fori_loop(0, heads, one_head, 0)
    dv_ref[...] = dvt_s[...].T.astype(BF16)
    rows_ref[...] = back_ref[...].T


def attention(qk, vog, lam, cos, sin, heads):
    seq, qk_cols = qk.shape
    vc = vog.shape[2]
    vm = pl.BlockSpec(memory_space=pltpu.VMEM)
    return pl.pallas_call(
        functools.partial(attention_kernel, heads),
        out_shape=(
            jax.ShapeDtypeStruct((qk_cols, seq), BF16),
            jax.ShapeDtypeStruct((seq, qk_cols), BF16),
            jax.ShapeDtypeStruct((seq, vc), BF16),
        ),
        in_specs=[pl.BlockSpec(memory_space=pltpu.SMEM)] + [vm] * 4,
        out_specs=(vm, vm, vm),
        scratch_shapes=[
            pltpu.VMEM((qk_cols, seq), F32),
            pltpu.VMEM((vc, seq), BF16),
            pltpu.VMEM((vc, seq), BF16),
            pltpu.VMEM((vc, seq), F32),
            pltpu.VMEM((qk_cols // heads // 2, seq), F32),
        ],
        compiler_params=pltpu.CompilerParams(vmem_limit_bytes=60 * 1024 * 1024),
        name="attn",
    )(lam, cos, sin, qk, vog)


def sender(src, dst, ssem, rsem, device):
    return pltpu.make_async_remote_copy(
        src_ref=src, dst_ref=dst, send_sem=ssem, recv_sem=rsem,
        device_id=device, device_id_type=pl.DeviceIdType.MESH,
    )


def places(sp, dp):
    me, mine = lax.axis_index("sp"), lax.axis_index("dp")
    z, core = mine // 2, lax.rem(mine, 2)
    nz = dp // 2
    if sp == 4:
        peers = [me + 1 - 2 * lax.rem(me, 2), lax.rem(me + 2, 4), 3 - me]
        froms = peers
    else:
        peers = [lax.rem(me + d, sp) for d in range(1, sp)]
        froms = [lax.rem(me + sp - d, sp) for d in range(1, sp)]
    z_to = [lax.rem(z + i, nz) * 2 for i in range(1, nz)]
    z_from = [lax.rem(z + nz - i, nz) * 2 for i in range(1, nz)]
    return me, mine, z, core, peers, froms, z_to, z_from


def greet(me, mine, core, peers, z_to):
    barrier = pltpu.get_barrier_semaphore()
    where = [(p, mine) for p in peers] + [(me, zt + core) for zt in z_to] + [(me, mine + 1 - 2 * core)]
    for device in where:
        pl.semaphore_signal(barrier, inc=1, device_id=device, device_id_type=pl.DeviceIdType.MESH)
    pl.semaphore_wait(barrier, len(where))


def gather_kernel(sp, dp, tok_ref, v_ref, og_ref, wq_ref, wk_ref, tok_all, vog_all, w_all, qk_ref,
                  vog_ref, tok_ss, tok_rs, vog_ss, vog_rs, w_ss, w_rs, sib_ss, sib_rs):
    me, mine, z, core, peers, froms, z_to, z_from = places(sp, dp)
    rows, wr = tok_ref.shape[0], wq_ref.shape[0]
    sib = (me, mine + 1 - 2 * core)

    def trow(i, start=0, size=rows):
        return pl.ds(pl.multiple_of(i * rows + start, 16), size)

    def wrow(i):
        return pl.ds(pl.multiple_of(i * wr, wr), wr)

    vc, qc = v_ref.shape[1] // sp, wq_ref.shape[1] // sp
    for s in range(sp):
        vog_ref[s, 0] = v_ref[:, s * vc : (s + 1) * vc]
        vog_ref[s, 1] = og_ref[:, s * vc : (s + 1) * vc]

        @pl.when(me == s)
        def _():
            w_all[wrow(mine), :qc] = wq_ref[:, s * qc : (s + 1) * qc]
            w_all[wrow(mine), qc:] = wk_ref[:, s * qc : (s + 1) * qc]

    tok_all[trow(me), :] = tok_ref[...]
    greet(me, mine, core, peers, z_to)
    w_ref = w_all.at[wrow(mine)]
    sends = []

    def go(copy):
        copy.start()
        sends.append(copy)
        return copy

    wz = [go(sender(w_ref, w_all.at[wrow(mine)], w_ss.at[i], w_rs.at[i], (me, zt + core)))
          for i, zt in enumerate(z_to)]
    ws = [go(sender(w_ref, w_all.at[wrow(mine)], sib_ss.at[0], sib_rs.at[0], sib))]
    half = rows // 2
    if sp == 4:
        def piece(p, h, k):
            r = trow(me, h * half, half)
            return go(sender(tok_ref.at[pl.ds(h * half, half)], tok_all.at[r], tok_ss.at[k], tok_rs.at[k], (p, mine)))

        x0, y1 = piece(peers[0], 0, 0), piece(peers[1], 1, 1)
        x1, y0 = piece(peers[0], 1, 2), piece(peers[1], 0, 3)
    else:
        tk = [go(sender(tok_ref, tok_all.at[trow(me)], tok_ss.at[i], tok_rs.at[i], (p, mine)))
              for i, p in enumerate(peers)]
    vg = [go(sender(vog_ref.at[p], vog_all.at[:, trow(me)], vog_ss.at[i], vog_rs.at[i], (p, mine)))
          for i, p in enumerate(peers)]
    vog_all[:, trow(me), :] = vog_ref[me]
    if sp == 4:
        x0.wait_recv()
        f0 = trow(peers[0], 0, half)
        d0 = go(sender(tok_all.at[f0], tok_all.at[f0], tok_ss.at[4], tok_rs.at[4], (peers[1], mine)))
        y1.wait_recv()
        f1 = trow(peers[1], half, half)
        d1 = go(sender(tok_all.at[f1], tok_all.at[f1], tok_ss.at[5], tok_rs.at[5], (peers[0], mine)))
        arrivals = [[x1], [y0], [d0, d1]]
    else:
        arrivals = [[c] for c in tk]
    for i, zf in enumerate(z_from):
        wz[i].wait_recv()
        r = wrow(zf + core)
        ws.append(go(sender(w_all.at[r], w_all.at[r], sib_ss.at[i + 1], sib_rs.at[i + 1], sib)))
    for c in ws:
        c.wait_recv()
    qk_ref[trow(me), :] = dot(tok_ref[...], w_all[...])
    for f, copies in zip(froms, arrivals):
        for c in copies:
            c.wait_recv()
        qk_ref[trow(f), :] = dot(tok_all[trow(f), :], w_all[...])
    for c in vg:
        c.wait_recv()
    for c in sends:
        c.wait_send()


def gather(tok, v, og, wq, wk, sp, dp):
    rows, width = tok.shape
    vc, wr, cols = v.shape[1] // sp, wq.shape[0], 2 * wq.shape[1] // sp
    vm = pl.BlockSpec(memory_space=pltpu.VMEM)
    dma = pltpu.SemaphoreType.DMA
    nt = 6 if sp == 4 else sp - 1
    nz = dp // 2
    return pl.pallas_call(
        functools.partial(gather_kernel, sp, dp),
        out_shape=(
            jax.ShapeDtypeStruct((rows * sp, width), BF16),
            jax.ShapeDtypeStruct((2, rows * sp, vc), BF16),
            jax.ShapeDtypeStruct((wr * dp, cols), BF16),
            jax.ShapeDtypeStruct((rows * sp, cols), F32),
        ),
        in_specs=[vm] * 5,
        out_specs=(vm,) * 4,
        scratch_shapes=[pltpu.VMEM((sp, 2, rows, vc), BF16), dma((nt,)), dma((nt,)), dma((sp - 1,)), dma((sp - 1,)),
                        dma((nz - 1,)), dma((nz - 1,)), dma((nz,)), dma((nz,))],
        compiler_params=pltpu.CompilerParams(
            vmem_limit_bytes=60 * 1024 * 1024, collective_id=0, has_side_effects=True
        ),
        name="gather",
    )(tok, v, og, wq, wk)


def scatter_kernel(sp, dp, back_t, back_m, tok_all, w_all, dv, tg_out, dv_out, qg, kg,
                   tbuf, trecv, tacc, dvr, sib_s, sib_r, wz_s, wz_r, wacc, wg_s, wg_r,
                   t_ss, t_rs, d_ss, d_rs, s_ss, s_rs, z_ss, z_rs, g_ss, g_rs):
    me, mine, z, core, peers, froms, z_to, z_from = places(sp, dp)
    nz = dp // 2
    rows, wr = tg_out.shape[0], qg.shape[0]
    vc = dv.shape[1]
    qc = w_all.shape[1] // 2
    sib = (me, mine + 1 - 2 * core)
    greet(me, mine, core, peers, z_to)
    sends = []

    def go(copy):
        copy.start()
        sends.append(copy)
        return copy

    def trow(i):
        return pl.ds(pl.multiple_of(i * rows, 16), rows)

    def weight_part(owner):
        return dot(back_t[...], tok_all[:, pl.ds(pl.multiple_of(owner * wr, wr), wr)])

    def token_part(p):
        return dot(back_m[trow(p), :], w_all[...], 1, 1)

    def send_tokens(i):
        tbuf[i] = token_part(peers[i]).astype(BF16)
        return go(sender(tbuf.at[i], trecv.at[i], t_ss.at[i], t_rs.at[i], (peers[i], mine)))

    targets = z_to + [z * 2]
    half = rows // 2
    lo, hi = pl.ds(0, half), pl.ds(half, half)
    tg = []

    def hop(i, dst, part, k, to):
        return go(sender(tbuf.at[i, part], trecv.at[dst, part], t_ss.at[k], t_rs.at[k], (peers[to], mine)))

    if sp == 4:
        tbuf[2] = token_part(peers[2]).astype(BF16)
        via_x, via_y = hop(2, 2, lo, 0, 0), hop(2, 2, hi, 1, 1)
    else:
        tg.append(send_tokens(0))
    sb = []
    for i, zt in enumerate(targets):
        sib_s[i] = weight_part(zt + 1 - core).astype(BF16)
        sb.append(go(sender(sib_s.at[i], sib_r.at[i], s_ss.at[i], s_rs.at[i], sib)))
    zs = []
    for i, zt in enumerate(targets):
        part = weight_part(zt + core)
        sb[i].wait_recv()
        part = part + sib_r[i].astype(F32)
        if i < nz - 1:
            wz_s[i] = part.astype(BF16)
            zs.append(go(sender(wz_s.at[i], wz_r.at[i], z_ss.at[i], z_rs.at[i], (me, zt + core))))
        else:
            wacc[...] = part
    if sp == 4:
        part = token_part(peers[0])
        tbuf[0, lo] = part[:half].astype(BF16)
        x_lo = hop(0, 0, lo, 2, 0)
        tacc[hi] = part[half:]
        part = token_part(peers[1])
        tbuf[1, hi] = part[half:].astype(BF16)
        y_hi = hop(1, 1, hi, 3, 1)
        tacc[lo] = part[:half]
        via_x.wait_recv()
        tbuf[1, lo] = (tacc[lo] + trecv[2, lo].astype(F32)).astype(BF16)
        y_lo = hop(1, 1, lo, 4, 1)
        via_y.wait_recv()
        tbuf[0, hi] = (tacc[hi] + trecv[2, hi].astype(F32)).astype(BF16)
        x_hi = hop(0, 0, hi, 5, 0)
        tg = [x_lo, x_hi, y_lo, y_hi]
    else:
        for i in range(1, sp - 1):
            tg.append(send_tokens(i))
    dvc = [go(sender(dv.at[trow(p)], dvr.at[me], d_ss.at[i], d_rs.at[i], (p, mine)))
           for i, p in enumerate(peers)]
    dvr[me] = dv[trow(me), :]
    tacc[...] = token_part(me)
    for i in range(nz - 1):
        zs[i].wait_recv()
        wacc[...] += wz_r[i].astype(F32)
    total = wacc[...].T.astype(BF16)
    wg_s[...] = total
    wg_r[me] = total
    wh = wr // 2
    if sp == 4:
        def piece(p, h, k):
            r = pl.ds(h * wh, wh)
            return go(sender(wg_s.at[r], wg_r.at[me, r], g_ss.at[k], g_rs.at[k], (p, mine)))

        def forward(f, h, k, p):
            r = pl.ds(h * wh, wh)
            return go(sender(wg_r.at[f, r], wg_r.at[f, r], g_ss.at[k], g_rs.at[k], (p, mine)))

        gx0, gy1 = piece(peers[0], 0, 0), piece(peers[1], 1, 1)
        gx1, gy0 = piece(peers[0], 1, 2), piece(peers[1], 0, 3)
        gx0.wait_recv()
        gd0 = forward(peers[0], 0, 4, peers[1])
        gy1.wait_recv()
        gd1 = forward(peers[1], 1, 5, peers[0])
        gs = [gx1, gy0, gd0, gd1]
    else:
        gs = [go(sender(wg_s, wg_r.at[me], g_ss.at[i], g_rs.at[i], (p, mine))) for i, p in enumerate(peers)]
    for c in tg:
        c.wait_recv()
    for i in range(2 if sp == 4 else sp - 1):
        tacc[...] += trecv[i].astype(F32)
    tg_out[...] = tacc[...].astype(BF16)
    for c in dvc:
        c.wait_recv()
    for s in range(sp):
        dv_out[:, s * vc : (s + 1) * vc] = dvr[s]
    for c in gs:
        c.wait_recv()
    for s in range(sp):
        qg[:, s * qc : (s + 1) * qc] = wg_r[s, :, :qc]
        kg[:, s * qc : (s + 1) * qc] = wg_r[s, :, qc:]
    for c in sends:
        c.wait_send()


def scatter(back_t, back_m, tok_all, w_all, dv, sp, dp):
    seq, width = tok_all.shape
    rows, wr = seq // sp, width // dp
    cols = w_all.shape[1]
    vc = dv.shape[1]
    nz = dp // 2
    vm = pl.BlockSpec(memory_space=pltpu.VMEM)
    dma = pltpu.SemaphoreType.DMA
    nt = 6 if sp == 4 else sp - 1
    return pl.pallas_call(
        functools.partial(scatter_kernel, sp, dp),
        out_shape=(
            jax.ShapeDtypeStruct((rows, width), BF16),
            jax.ShapeDtypeStruct((rows, vc * sp), BF16),
            jax.ShapeDtypeStruct((wr, cols // 2 * sp), BF16),
            jax.ShapeDtypeStruct((wr, cols // 2 * sp), BF16),
        ),
        in_specs=[vm] * 5,
        out_specs=(vm,) * 4,
        scratch_shapes=[
            pltpu.VMEM((sp - 1, rows, width), BF16),
            pltpu.VMEM((sp - 1, rows, width), BF16),
            pltpu.VMEM((rows, width), F32),
            pltpu.VMEM((sp, rows, vc), BF16),
            pltpu.VMEM((nz, cols, wr), BF16),
            pltpu.VMEM((nz, cols, wr), BF16),
            pltpu.VMEM((nz - 1, cols, wr), BF16),
            pltpu.VMEM((nz - 1, cols, wr), BF16),
            pltpu.VMEM((cols, wr), F32),
            pltpu.VMEM((wr, cols), BF16),
            pltpu.VMEM((sp, wr, cols), BF16),
            dma((nt,)), dma((nt,)), dma((sp - 1,)), dma((sp - 1,)), dma((nz,)), dma((nz,)),
            dma((nz - 1,)), dma((nz - 1,)), dma((nt,)), dma((nt,)),
        ],
        compiler_params=pltpu.CompilerParams(
            vmem_limit_bytes=62 * 1024 * 1024, collective_id=1, has_side_effects=True
        ),
        name="scatter",
    )(back_t, back_m, tok_all, w_all, dv)


def position_tables(seq_length):
    half = DQK // 2
    freqs = np.exp(np.float32(-math.log(THETA)) * np.arange(half, dtype=np.float32) / np.float32(half)).astype(np.float32)
    angles = freqs[:, None] * np.arange(seq_length, dtype=np.float32)[None, :]
    wide = angles.astype(np.float64)
    return jnp.asarray(np.concatenate([np.cos(wide), np.sin(wide)]).astype(np.float32))


def head_scores(hh, cos, sin, q, k_in, qt_s, kt_s, p_s, r_s, lam):
    seq = cos.shape[1]
    scale = math.log2(math.e) / math.sqrt(DQK)
    step = 256
    zero_half = jnp.zeros((DQK, step), BF16)
    qt = rotate_rows(q, cos, sin).astype(BF16)
    kt = rotate_rows(k_in, cos, sin).astype(BF16)
    qt_s[hh] = qt
    kt_s[hh] = kt
    k = kt.T
    for t0 in range(0, seq, step):
        end = min(t0 + step, seq)
        tb = end - t0
        zh = zero_half[:, :tb]
        q_b = qt[:, t0:end]
        mask = lax.broadcasted_iota(jnp.int32, (tb, tb), 0) <= lax.broadcasted_iota(jnp.int32, (tb, tb), 1)
        for m in range(2):
            half_q = q_b[m * DQK : (m + 1) * DQK]
            rhs = jnp.concatenate([half_q, zh] if m == 0 else [zh, half_q], axis=0)
            s = dot(k[:end], rhs)
            diag = jnp.where(mask, s[t0:], -jnp.inf)
            s = jnp.concatenate([s[:t0], diag], axis=0) if t0 else diag
            e = jnp.exp2((s - jnp.max(s, axis=0, keepdims=True)) * scale)
            r = 1.0 / jnp.sum(e, axis=0, keepdims=True)
            p_s[hh, m, :end, t0:end] = e
            r_s[hh, m : m + 1, t0:end] = r if m == 0 else r * -lam


def pair_back(h0, cos, sin, lams, qt_s, kt_s, p_s, r_s, vt_s, ogt_s, dvt_s, dk_s, bt_s):
    seq = cos.shape[1]
    hw = 2 * DQK
    ve = vt_s.shape[0] // 2
    inv_root = 1.0 / math.sqrt(DQK)
    step = 256
    cb, sb = cos * inv_root, sin * -inv_root
    work = [(hh, t0, min(t0 + step, seq)) for t0 in range(0, seq, step) for hh in range(2)]
    rows = [slice(hh * hw, (hh + 1) * hw) for hh in range(2)]
    vrows = [slice(hh * ve, (hh + 1) * ve) for hh in range(2)]
    vt = [vt_s[r, :] for r in vrows]
    v = [x.T for x in vt]
    mix, ho, ob, g1, g2 = {}, {}, {}, {}, {}
    for w in work:
        hh, t0, end = w
        r1, r2 = r_s[h0 + hh, 0:1, t0:end], r_s[h0 + hh, 1:2, t0:end]
        mix[w] = (p_s[h0 + hh, 0, :end, t0:end] * r1 + p_s[h0 + hh, 1, :end, t0:end] * r2).astype(BF16)
        ho[w] = dot(vt[hh][:, :end], mix[w])
    for w in work:
        hh, t0, end = w
        x = ho[w]
        inv = lax.rsqrt(jnp.mean(x * x, axis=0, keepdims=True) + NORM_EPS)
        og = ogt_s[vrows[hh], t0:end].astype(F32)
        ob[w] = (inv * og - inv * inv * inv * x * jnp.mean(og * x, axis=0, keepdims=True)).astype(BF16)
    for w in work:
        hh, t0, end = w
        mg = dot(v[hh][:end], ob[w])
        p1, p2 = p_s[h0 + hh, 0, :end, t0:end], p_s[h0 + hh, 1, :end, t0:end]
        r1, r2 = r_s[h0 + hh, 0:1, t0:end], r_s[h0 + hh, 1:2, t0:end]
        m1, m2 = mg * r1, mg * r2
        g1[w] = (p1 * (m1 - jnp.sum(m1 * p1, axis=0, keepdims=True) * r1)).astype(BF16)
        g2[w] = (p2 * (m2 + jnp.sum(m2 * p2, axis=0, keepdims=True) * (r2 / lams[hh]))).astype(BF16)
        q_b, kt = qt_s[h0 + hh, :, t0:end], kt_s[h0 + hh]
        dq = jnp.concatenate([dot(kt[:DQK, :end], g1[w]), dot(kt[DQK:, :end], g2[w])], axis=0)
        bt_s[rows[hh], t0:end] = rotate_rows(dq, cb[:, t0:end], sb[:, t0:end]).astype(BF16)
        dvd = dot(ob[w], mix[w], 1, 1)
        dkd = jnp.concatenate([dot(q_b[:DQK], g1[w], 1, 1), dot(q_b[DQK:], g2[w], 1, 1)], axis=0)
        if t0:
            dvd = jnp.concatenate([dvt_s[vrows[hh], :t0] + dvd[:, :t0], dvd[:, t0:]], axis=1)
            dkd = jnp.concatenate([dk_s[rows[hh], :t0] + dkd[:, :t0], dkd[:, t0:]], axis=1)
        dvt_s[vrows[hh], :end] = dvd
        dk_s[rows[hh], :end] = dkd
    for hh in range(2):
        bt_s[2 * hw + hh * hw : 2 * hw + (hh + 1) * hw, :] = rotate_rows(dk_s[rows[hh], :], cb, sb).astype(BF16)


def fused_kernel(sp, dp, pairs, lam_in, rot_in, tok_in, v_in, og_in, wq_in, wk_in,
                 tg_out, dvr, wg_r,
                 lam_ref, rot_ref, tok_all, w1, w2, qk_s, vog_src, vog_all, qt_s, kt_s, p_s, r_s,
                 vt_s, ogt_s, dvt_s, dk_s, bt_s, back_m, back_x,
                 dv_s, sib_s, sib_r, own_s, wz_s, wz_r, wz_m, tbuf, trecv, tacc,
                 pool, tok_rs, vog_rs, z_rs, s_rs, bx_rs, dv_rs, c_rs, g_rs, m_rs, ag_rs, ty_rs):
    me, mine, z, core, peers, froms, z_to, z_from = places(sp, dp)
    nz = dp // 2
    rows, wr = tok_in.shape[0], wq_in.shape[0]
    half = rows // 2
    pw = 128
    sib = (me, mine + 1 - 2 * core)
    xp, yp = (peers[0], mine), (peers[1], mine)

    def trow(i, start=0, size=rows):
        return pl.ds(pl.multiple_of(i * rows + start, 16), size)

    def wrow(zz, c):
        return pl.ds(pl.multiple_of((c * nz + zz) * wr, wr), wr)

    def lanes(i, size):
        return pl.ds(pl.multiple_of(i * size, size), size)

    sends = []
    free = list(range(pool.shape[0]))

    def remote(src, dst, rsem, device):
        return lambda ssem: sender(src, dst, ssem, rsem, device)

    def arrive(link):
        link(pool.at[0]).wait_recv()

    def ready(link, cond=None):
        slot = free.pop(0)
        copy = link(pool.at[slot])
        sends.append((copy, cond, slot))
        return copy

    def go(link, cond=None):
        copy = ready(link, cond)
        if cond is None:
            copy.start()
        else:
            pl.when(cond)(copy.start)
        return link

    def flush(count):
        for c, cond, slot in sends[:count]:
            if cond is None:
                c.wait_send()
            else:
                pl.when(cond)(c.wait_send)
            free.append(slot)
        del sends[:count]

    barrier = pltpu.get_barrier_semaphore()
    where = [(p, mine) for p in peers] + [(me, zt + core) for zt in z_to] + [sib]
    for device in where:
        pl.semaphore_signal(barrier, inc=1, device_id=device, device_id_type=pl.DeviceIdType.MESH)

    def load(src, dst):
        slot = free.pop(0)
        c = pltpu.make_async_copy(src, dst, pool.at[slot])
        c.start()
        return c, slot

    def loaded(copies):
        for c, slot in copies:
            c.wait()
            free.append(slot)

    def load_weights(w, who):
        out = []
        for j in range(pairs):
            src = lanes(who * pairs + j, pw)
            out.append(load(wq_in.at[:, src], w.at[wrow(z, core), 2 * j * pw : (2 * j + 1) * pw]))
            out.append(load(wk_in.at[:, src], w.at[wrow(z, core), (2 * j + 1) * pw : (2 * j + 2) * pw]))
        return out

    l_tok = []
    for c in range(2):
        for zz in range(nz):
            n = slice((c * nz + zz) * wr, (c * nz + zz + 1) * wr)
            l_tok.append(load(tok_in.at[:, (2 * zz + c) * wr : (2 * zz + c + 1) * wr], tok_all.at[trow(me), n]))
    l_w1 = load_weights(w1, me)
    far = lax.rem(z + 2, nz)
    order = [far, z + 1 - 2 * lax.rem(z, 2), nz - 1 - z]
    inner = jnp.logical_and(z > 0, z < nz - 1)
    outer = jnp.logical_not(inner)

    def z_copy(w, k, n, src, to):
        r = w.at[wrow(src, core)]
        return remote(r, r, z_rs.at[k, src], (me, 2 * to + core))

    def s_copy(w, k, src):
        r = w.at[wrow(src, core)]
        return remote(r, r, s_rs.at[k, src], sib)

    def z_start():
        go(z_copy(w1, 0, 0, z, far))
        go(z_copy(w1, 0, 1, z, order[1]))
        go(z_copy(w1, 0, 2, z, order[2]), inner)
        go(s_copy(w1, 0, z))

    def z_step(i):
        arrive(z_copy(w1, 0, 0, order[i], z))
        go(s_copy(w1, 0, order[i]))
        if i == 0:
            go(z_copy(w1, 0, 3, far, order[1]), inner)

    aside = (1 - z // 2) * (nz - 1)
    near = [order[1], jnp.where(inner, order[2], far)]

    def other_start():
        go(z_copy(w2, 1, 0, z, far), inner)
        go(z_copy(w2, 1, 1, z, order[1]))
        go(z_copy(w2, 1, 2, z, order[2]), inner)
        go(s_copy(w2, 1, z))

    def other_aside():
        r = wrow(aside, core)
        to = (jnp.where(core == 0, peers[0], peers[1]), mine)
        return remote(w1.at[r], w2.at[r], z_rs.at[1, aside], to)

    def other_step(src):
        arrive(z_copy(w2, 1, 0, src, z))
        go(s_copy(w2, 1, src))

    def z_sib(w, k):
        for src in [z] + order:
            r = w.at[wrow(src, 1 - core)]
            arrive(remote(r, r, s_rs.at[k, src], sib))

    def piece(p, h, k):
        r = trow(me, h * half, half)
        return go(remote(tok_all.at[r], tok_all.at[r], tok_rs.at[k], p))

    loaded(l_tok)
    pl.semaphore_wait(barrier, len(where))
    x0, y1 = piece(xp, 0, 0), piece(yp, 1, 1)
    x1, y0 = piece(xp, 1, 2), piece(yp, 0, 3)
    loaded(l_w1)
    z_start()
    l_vog = []
    for j in range(pairs):
        for n, src in enumerate((v_in, og_in)):
            for i, p in enumerate(peers):
                l_vog.append(load(src.at[:, lanes(p * pairs + j, pw)], vog_src.at[i, j, n]))
            l_vog.append(load(src.at[:, lanes(me * pairs + j, pw)], vog_all.at[j, n, trow(me)]))
    l_w2 = load_weights(w2, jnp.where(core == 0, peers[0], peers[1]))
    l_rot = [load(rot_in, rot_ref), load(lam_in, lam_ref)]
    loaded(l_w2 + l_vog + l_rot)
    arrive(x0)
    f0 = trow(peers[0], 0, half)
    d0 = go(remote(tok_all.at[f0], tok_all.at[f0], tok_rs.at[4], yp))
    arrive(y1)
    f1 = trow(peers[1], half, half)
    d1 = go(remote(tok_all.at[f1], tok_all.at[f1], tok_rs.at[5], xp))

    def vog_start(j):
        for i in range(sp - 1):
            go(remote(vog_src.at[i, j], vog_all.at[j, :, trow(me)], vog_rs.at[j, i], (peers[i], mine)))

    vog_start(0)
    z_step(0)
    z_step(1)
    z_step(2)
    other_start()
    z_sib(w1, 0)
    qk_s[trow(me), :] = dot(tok_all[trow(me), :], w1[...])
    for f, copies in zip(froms, [[x1], [y0], [d0, d1]]):
        for c in copies:
            arrive(c)
        qk_s[trow(f), :] = dot(tok_all[trow(f), :], w1[...])

    n16 = DQK // 2
    cos, sin = rot_ref[:n16, :], rot_ref[n16:, :]
    hw = 2 * DQK

    lams = [lam_ref[me * pairs * 2 + h] for h in range(2 * pairs)]
    def scores(j):
        qk = [qk_s[:, (2 * j + n) * pw : (2 * j + n + 1) * pw].T for n in range(2)]
        for hh in range(2):
            r = slice(hh * hw, (hh + 1) * hw)
            h = 2 * j + hh
            head_scores(h, cos, sin, qk[0][r], qk[1][r], qt_s, kt_s, p_s, r_s, lams[h])

    def values_start(j):
        for i, p in enumerate(peers):
            go(remote(dv_s.at[j, trow(p)], dvr.at[me, j], dv_rs.at[j, i], (p, mine)))
        dvr[me, j] = dv_s[j, trow(me), :]

    def one_pair(j):
        for i, p in enumerate(peers):
            r = vog_all.at[j, :, trow(p)]
            arrive(remote(r, r, vog_rs.at[j, i], (p, mine)))
        if j == 0:
            go(other_aside())
        vt_s[...] = vog_all[j, 0].T
        ogt_s[...] = vog_all[j, 1].T
        pair_back(2 * j, cos, sin, lams[2 * j : 2 * j + 2], qt_s, kt_s, p_s, r_s, vt_s, ogt_s, dvt_s, dk_s, bt_s)
        back_m[j] = bt_s[...].T
        for a, to in enumerate((0, 1)):
            for b, p in enumerate((peers[to], peers[2])):
                go(remote(back_m.at[j, trow(p)], back_x.at[a, j, b], bx_rs.at[a, j, b], (xp, yp)[to]))

        if j:
            merge(j - 1)

        def weight_part(c):
            return dot(bt_s[...], tok_all[:, lanes(c, nz * wr)])

        part = weight_part(1 - core)
        for zz in range(nz):
            sib_s[j, zz] = part[:, zz * wr : (zz + 1) * wr].astype(BF16)
        go(remote(sib_s.at[j], sib_r.at[j], c_rs.at[j], sib))
        part = weight_part(core)
        for zz in range(nz):
            own_s[j, zz] = part[:, zz * wr : (zz + 1) * wr]
        dv_s[j] = dvt_s[...].T.astype(BF16)
        values_start(j)

    def shares(j):
        arrive(remote(sib_s.at[j], sib_r.at[j], c_rs.at[j], sib))
        for i in range(nz):
            own_s[j, i] = own_s[j, i] + sib_r[j, i].astype(F32)
        for i in range(nz - 1):
            wz_s[j, i] = own_s[j, order[i]].astype(BF16)
        go(remote(wz_s.at[j, 2], wz_m.at[j], m_rs.at[j], (me, 2 * order[1] + core)), outer)
        go(z_share(j, 0), outer)
        go(z_share(j, 2), inner)
        go(z_share(j, 1))

    def z_share(j, i):
        return remote(wz_s.at[j, i], wz_r.at[j, i], g_rs.at[j, i], (me, 2 * order[i] + core))

    def merge(j):
        copy = ready(z_share(j, 0), inner)

        @pl.when(inner)
        def _():
            arrive(remote(wz_m.at[j], wz_m.at[j], m_rs.at[j], sib))
            wz_s[j, 0] = (own_s[j, far] + wz_m[j].astype(F32)).astype(BF16)
            copy.start()

    scores(0)
    flush(10)
    for j in range(1, pairs):
        vog_start(j)
        scores(j)
    for j in range(pairs):
        one_pair(j)
        if j == 0:
            done = len(sends)
        shares(j)
        if j == 0:
            other_step(near[0])

    def back_wait(a, j, b):
        r = back_x.at[a, j, b]
        arrive(remote(r, r, bx_rs.at[a, j, b], sib))

    def token_part(who, a, b, parts):
        n = slice(a * nz * wr, (a + 1) * nz * wr)
        out = None
        for j, own in parts:
            k = slice(2 * j * pw, (2 * j + 2) * pw)
            part = dot(back_m[j, trow(who), :], w1[n, k], 1, 1) if own else dot(back_x[a, j, b], w2[n, k], 1, 1)
            out = part if out is None else out + part
        return out

    early = [(j, True) for j in range(pairs)] + [(j, False) for j in range(pairs - 1)]
    late = [(pairs - 1, False)]
    other_step(near[1])
    other_step(aside)
    z_sib(w2, 1)
    for a in range(2):
        for b in range(2):
            for j in range(pairs - 1):
                back_wait(a, j, b)
    for a in range(2):
        tacc[a] = token_part(peers[1 - a], a, 1, early)
    flush(done)
    ty = {}
    for a in range(2):
        back_wait(a, pairs - 1, 1)
        tbuf[a] = (tacc[a] + token_part(peers[1 - a], a, 1, late)).astype(BF16)
        for h in range(2):
            r = pl.ds(h * half, half)
            ty[a, h] = go(remote(tbuf.at[a, r], trecv.at[a, r], ty_rs.at[a, h], (yp, xp)[a]))

    def weights_end(j):
        @pl.when(inner)
        def _():
            arrive(z_share(j, 2))
            own_s[j, z] = own_s[j, z] + wz_r[j, 2].astype(F32)

        arrive(z_share(j, 0))
        arrive(z_share(j, 1))
        total = own_s[j, z] + wz_r[j, 0].astype(F32) + wz_r[j, 1].astype(F32)
        wg_r[me, j] = total.T.astype(BF16)
        for h, k, to in ((0, 0, xp), (1, 1, yp), (1, 2, xp), (0, 3, yp)):
            go(ag(me, j, h, k, to))

    wh = wr // 2

    def ag(owner, j, h, k, to):
        r = wg_r.at[owner, j, pl.ds(h * wh, wh)]
        return remote(r, r, ag_rs.at[j, k], to)

    def weights_relay(j):
        arrive(ag(peers[0], j, 0, 0, xp))
        go(ag(peers[0], j, 0, 4, yp))
        arrive(ag(peers[1], j, 1, 1, yp))
        go(ag(peers[1], j, 1, 5, xp))

    merge(pairs - 1)
    weights_end(0)
    for a in range(2):
        back_wait(a, pairs - 1, 0)
    for a in range(2):
        tacc[a] = token_part(me, a, 0, early + late)
    for j in range(1, pairs):
        weights_end(j)
    for h in range(2):
        for a in range(2):
            arrive(ty[a, h])
            if h == 1 and a == 1:
                flush(len(sends) - 4 * pairs)
            r = slice(h * half, (h + 1) * half)
            total = (tacc[a, r] + trecv[a, r].astype(F32)).astype(BF16)
            for zz in range(nz):
                tg_out[r, (2 * zz + a) * wr : (2 * zz + a + 1) * wr] = total[:, zz * wr : (zz + 1) * wr]
    for j in range(pairs):
        weights_relay(j)
    for j in range(pairs):
        for i, p in enumerate(peers):
            r = dvr.at[p, j]
            arrive(remote(r, r, dv_rs.at[j, i], xp))
        for owner, h, k in ((peers[0], 1, 2), (peers[1], 0, 3), (peers[2], 0, 4), (peers[2], 1, 5)):
            arrive(ag(owner, j, h, k, xp))
    flush(len(sends))


def finish_kernel(factor, tg, dvr, wg, tg_out, dv_out, qg_out, kg_out, dv_s, qg, kg, sem):
    sp, pairs, wr, cols = wg.shape
    pw = cols // 2
    copies = [pltpu.make_async_copy(tg, tg_out, sem.at[0])]
    copies[0].start()
    for s in range(sp):
        for j in range(pairs):
            n = slice((s * pairs + j) * pw, (s * pairs + j + 1) * pw)
            qg[:, n] = wg[s, j, :, :pw].astype(F32) * factor
    copies.append(pltpu.make_async_copy(qg, qg_out, sem.at[1]))
    copies[1].start()
    for s in range(sp):
        for j in range(pairs):
            n = slice((s * pairs + j) * pw, (s * pairs + j + 1) * pw)
            kg[:, n] = wg[s, j, :, pw:].astype(F32) * factor
    copies.append(pltpu.make_async_copy(kg, kg_out, sem.at[2]))
    copies[2].start()
    for s in range(sp):
        for j in range(pairs):
            n = slice((s * pairs + j) * pw, (s * pairs + j + 1) * pw)
            dv_s[:, n] = dvr[s, j]
    copies.append(pltpu.make_async_copy(dv_s, dv_out, sem.at[3]))
    copies[3].start()
    for c in copies:
        c.wait()


def fused(tok, v, og, wq, wk, lam, rot, sp, dp):
    rows, width = tok.shape
    seq = rows * sp
    wr = wq.shape[0]
    nz = dp // 2
    pw = 128
    pairs = v.shape[1] // (sp * pw)
    factor = 1.0 / math.sqrt(dp * seq)
    vm = pl.BlockSpec(memory_space=pltpu.VMEM)
    anywhere = pl.BlockSpec(memory_space=pl.ANY)
    dma = pltpu.SemaphoreType.DMA
    V = pltpu.VMEM
    tg, dvr, wg = pl.pallas_call(
        functools.partial(fused_kernel, sp, dp, pairs),
        out_shape=(
            V((rows, width), BF16),
            V((sp, pairs, rows, pw), BF16),
            V((sp, pairs, wr, 2 * pw), BF16),
        ),
        in_specs=[anywhere] * 7,
        out_specs=(vm,) * 3,
        scratch_shapes=[
            pltpu.SMEM(lam.shape, F32), V(rot.shape, F32),
            V((seq, width), BF16), V((width, 2 * pairs * pw), BF16), V((width, 2 * pairs * pw), BF16),
            V((seq, 2 * pairs * pw), F32), V((sp - 1, pairs, 2, rows, pw), BF16), V((pairs, 2, seq, pw), BF16),
            V((2 * pairs, 2 * DQK, seq), BF16), V((2 * pairs, 2 * DQK, seq), BF16), V((2 * pairs, 2, seq, seq), F32), V((2 * pairs, 2, seq), F32),
            V((pw, seq), BF16), V((pw, seq), BF16), V((pw, seq), F32), V((pw, seq), F32), V((2 * pw, seq), BF16),
            V((pairs, seq, 2 * pw), BF16), V((2, pairs, 2, rows, 2 * pw), BF16),
            V((pairs, seq, pw), BF16),
            V((pairs, nz, 2 * pw, wr), BF16), V((pairs, nz, 2 * pw, wr), BF16), V((pairs, nz, 2 * pw, wr), F32),
            V((pairs, nz - 1, 2 * pw, wr), BF16), V((pairs, nz - 1, 2 * pw, wr), BF16), V((pairs, 2 * pw, wr), BF16),
            V((2, rows, nz * wr), BF16), V((2, rows, nz * wr), BF16), V((2, rows, nz * wr), F32),
            dma((44,)), dma((6,)), dma((pairs, sp - 1)), dma((2, nz)), dma((2, nz)), dma((2, pairs, 2)),
            dma((pairs, sp - 1)), dma((pairs,)), dma((pairs, nz - 1)), dma((pairs,)), dma((pairs, 6)), dma((2, 2)),
        ],
        compiler_params=pltpu.CompilerParams(
            vmem_limit_bytes=56 * 1024 * 1024, collective_id=2, has_side_effects=True
        ),
        name="fused",
    )(lam, rot, tok, v, og, wq, wk)
    return pl.pallas_call(
        functools.partial(finish_kernel, factor),
        out_shape=(
            jax.ShapeDtypeStruct((rows, width), BF16),
            jax.ShapeDtypeStruct((rows, v.shape[1]), BF16),
            jax.ShapeDtypeStruct((wr, wq.shape[1]), F32),
            jax.ShapeDtypeStruct((wr, wq.shape[1]), F32),
        ),
        in_specs=[vm] * 3,
        out_specs=(anywhere,) * 4,
        scratch_shapes=[V((rows, v.shape[1]), BF16), V((wr, wq.shape[1]), F32), V((wr, wq.shape[1]), F32), dma((4,))],
        compiler_params=pltpu.CompilerParams(vmem_limit_bytes=16 * 1024 * 1024),
        name="finish",
    )(tg, dvr, wg)


def body(tokens, query_weight, key_weight, values, lambdas, out_grad):
    sp = lax.axis_size("sp")
    dp = lax.axis_size("dp")
    rows = tokens.shape[1]
    heads = lambdas.shape[0] // sp
    head_vec = values.shape[2] // lambdas.shape[0]
    if sp == 4 and dp == 8 and heads % 2 == 0 and head_vec == 64 and rows * sp <= 640:
        tg, dv, qg, kg = fused(
            tokens[0], values[0], out_grad[0], query_weight, key_weight, lambdas,
            position_tables(rows * sp), sp, dp,
        )
        return tg[None], dv[None], qg, kg
    cos, sin = rotation_tables(rows * sp)
    tok_all, vog_all, w_all, qk = gather(
        tokens[0], values[0], out_grad[0], query_weight, key_weight, sp, dp
    )
    back_t, back_m, dv = attention(qk, vog_all, lambdas, cos, sin, heads)
    tokens_grad, values_grad, qg, kg = scatter(back_t, back_m, tok_all, w_all, dv, sp, dp)
    factor = 1.0 / math.sqrt(dp * rows * sp)
    return tokens_grad[None], values_grad[None], qg.astype(F32) * factor, kg.astype(F32) * factor


def solution(mesh):
    x = P("dp", "sp", None)
    w = P("dp", None)
    return jax.shard_map(
        body, mesh=mesh, in_specs=(x, w, w, x, P(), x), out_specs=(x, x, w, w), check_vma=False
    )
```
